32 devices in a mesh: sp: 8 (over z, x), tp: 4 (over y, core).
Axes of the slice: x: 2, y: 2, z: 4, core: 2. Of those that a mesh axis runs over, the one named last changes fastest.
Arguments:
- queries: bfloat16 [1536, 1536], P('sp', 'tp'), may hold values from -64 to 64
- latents: bfloat16 [1536, 512], P('sp'), may hold values from -6 to 6
- rope_key: bfloat16 [1536, 32], P('sp'), may hold values from -64 to 64
- w_key: bfloat16 [512, 1024], P(None, 'tp'), may hold values from -0.25 to 0.25
- w_value: bfloat16 [512, 1024], P(None, 'tp'), may hold values from -0.25 to 0.25
- w_out: bfloat16 [1024, 2048], P('tp'), may hold values from -0.59765625 to 0.59765625
- resid: bfloat16 [1536, 2048], P('sp', 'tp'), may hold values from -12 to 12
- gain_mix: float32 [2048], P('tp'), may hold values from 0.1 to 1.9
- w_gate: bfloat16 [2048, 3072], P('sp', 'tp'), may hold values from -0.125 to 0.125
- w_up: bfloat16 [2048, 3072], P('sp', 'tp'), may hold values from -0.125 to 0.125
- w_down: bfloat16 [3072, 2048], P('tp', 'sp'), may hold values from -0.41992188 to 0.41992188
- gain_out: float32 [2048], P('tp'), may hold values from 0.1 to 1.9
Outputs:
- layer_out: bfloat16 [1536, 2048], P('sp', 'tp')
The draws below stay inside these ranges and needn't reach their ends.
All inputs are finite; a program needn't handle non-finite values.
Results may differ from the reference program's by a relative error of at most 0.014.
Values may be sent and summed in bfloat16 or wider, within the bound.
A program may use at most 128 MiB of HBM per device.

```python
import math
import jax
import jax.numpy as jnp
from jax import lax

D = 2048
HEADS = 16
NOPE = 64
ROPE = 32
VDIM = 64
KV_RANK = 512
FF = 3072
GRID_W = 64
TOKENS = 1536
N_TP = 4


def drawn_pair(key):
    query_seed = jax.random.fold_in(key, 11)
    rotary_seed = jax.random.fold_in(key, 12)
    width_total = HEADS * (NOPE + ROPE)
    queries = jnp.clip(jax.random.normal(query_seed, (TOKENS, width_total), jnp.float32) * 2.5, -15.0, 15.0)
    rotary = jnp.clip(jax.random.normal(rotary_seed, (TOKENS, ROPE), jnp.float32), -6.0, 6.0)
    return (queries, rotary)


def draw_queries(key, part):
    return drawn_pair(key)[0].astype(jnp.bfloat16)


def draw_rope_key(key, part):
    return drawn_pair(key)[1].astype(jnp.bfloat16)


def draw_resid(key, part):
    row_seed = jax.random.fold_in(key, 21)
    value_seed = jax.random.fold_in(key, 22)
    column_scale = 0.6 * 10.0 ** (jnp.arange(D, dtype=jnp.float32) / (D - 1) - 0.5)
    row_scale = 10.0 ** jax.random.uniform(row_seed, (TOKENS, 1), jnp.float32, -0.5, 0.5)
    values_out = jax.random.normal(value_seed, (TOKENS, D), jnp.float32) * row_scale * column_scale
    return jnp.clip(values_out, -12.0, 12.0).astype(jnp.bfloat16)


def steps_of(key, shape, cuts, low, largest):
    gain, own = 1.0, jax.random.fold_in(key, 6)
    for axis_at, shards_of in cuts:
        draws = jnp.exp(jax.random.uniform(jax.random.fold_in(own, axis_at), (shards_of,), jnp.float32, low / len(cuts), largest / len(cuts)))
        gain = gain * jnp.repeat(draws, shape[axis_at] // shards_of).reshape([-1 if axis == axis_at else 1 for axis in range(len(shape))])
    return gain


def gaussian(stream_key, shape, spread, limit, pieces=(), kind=jnp.bfloat16):
    result = jax.random.normal(stream_key, shape, jnp.float32) * spread
    if len(pieces) > 0:
        result = steps_of(stream_key, shape, pieces, -0.22, 0.18) * result
    return jnp.clip(result, min=-limit, max=limit).astype(kind)


def setup_inputs(seed: int = 0) -> dict:
    keys = jax.random.split(jax.random.key(seed), 13)
    queries = draw_queries(jax.random.fold_in(keys[12], 71), 0)
    latents = gaussian(keys[1], (TOKENS, KV_RANK), 1.0, 6.0, ((0, 8),))
    rope_key = draw_rope_key(jax.random.fold_in(keys[12], 71), 0)
    w_key = gaussian(keys[3], (KV_RANK, HEADS * NOPE), KV_RANK ** -0.5, 0.25, ((1, 4),))
    w_value = gaussian(keys[4], (KV_RANK, HEADS * VDIM), KV_RANK ** -0.5, 0.25, ((1, 4),))
    w_out = gaussian(keys[5], (HEADS * VDIM, D), 0.1, 0.59765625, ((0, 4),))
    resid = draw_resid(jax.random.fold_in(keys[12], 71), 0)
    gain_mix = jnp.clip(1.0 + 0.18 * jax.random.normal(keys[7], (D,), jnp.float32), 0.1, 1.9)
    w_gate = gaussian(keys[8], (D, FF), D ** -0.5, 0.125, ((0, 8), (1, 4)))
    w_up = gaussian(keys[9], (D, FF), D ** -0.5, 0.125, ((0, 8), (1, 4)))
    w_down = gaussian(keys[10], (FF, D), 0.07, 0.41992188, ((0, 4), (1, 8)))
    gain_out = jnp.clip(1.0 + 0.18 * jax.random.normal(keys[11], (D,), jnp.float32), 0.1, 1.9)
    return {"queries": queries, "latents": latents, "rope_key": rope_key, "w_key": w_key, "w_value": w_value, "w_out": w_out, "resid": resid, "gain_mix": gain_mix, "w_gate": w_gate, "w_up": w_up, "w_down": w_down, "gain_out": gain_out}


ROTARY_BASE = 10000.0
NORM_EPSILON = 1e-06
DEEP_ALPHA = 8.0 ** 0.25
HALF_STEP = 0.5

def rotary_tables(positions, rotary_width, grid_width):
    grid_rows = (positions // grid_width).astype(jnp.float32)
    grid_cols = (positions % grid_width).astype(jnp.float32)
    freq_count = rotary_width // 4
    inverse = ROTARY_BASE ** (-jnp.arange(freq_count, dtype=jnp.float32) / freq_count)
    angle_table = jnp.concatenate([grid_rows[:, None] * inverse, grid_cols[:, None] * inverse], axis=-1)
    return (jnp.cos(angle_table), jnp.sin(angle_table))

def rotate(vectors, cosine, sine):
    half_width = vectors.shape[-1] // 2
    leading = vectors[..., :half_width].astype(jnp.float32)
    trailing = vectors[..., half_width:].astype(jnp.float32)
    return jnp.concatenate([leading * cosine - trailing * sine, leading * sine + trailing * cosine], axis=-1).astype(jnp.bfloat16)

def widened(tensor):
    return lax.optimization_barrier(tensor.astype(jnp.bfloat16)).astype(jnp.float32)

def layer_norm(rows_in, gain_row):
    row_mean = lax.optimization_barrier(jnp.mean(rows_in, axis=1, keepdims=True))
    variance = lax.optimization_barrier(jnp.mean(rows_in * rows_in, axis=1, keepdims=True)) - row_mean * row_mean
    return ((rows_in - row_mean) * lax.rsqrt(variance + NORM_EPSILON) * gain_row.astype(jnp.float32)).astype(jnp.bfloat16)

def group_sum(left, right, group_width):
    total_sum = jnp.zeros((left.shape[0], right.shape[1]), jnp.float32)
    for group_index in range(N_TP):
        lower = group_index * group_width
        partial_term = jnp.dot(left[:, lower:lower + group_width], right[lower:lower + group_width], preferred_element_type=jnp.float32)
        total_sum = total_sum + widened(partial_term)
    return total_sum

def reference(queries, latents, rope_key, w_key, w_value, w_out, resid, gain_mix, w_gate, w_up, w_down, gain_out):
    positions = jnp.arange(TOKENS, dtype=jnp.int32)
    cosine, sine = rotary_tables(positions, ROPE, GRID_W)
    key_rot = lax.optimization_barrier(rotate(rope_key, cosine, sine)).astype(jnp.float32)
    shaped = queries.reshape(TOKENS, HEADS, NOPE + ROPE)
    q_nope = shaped[:, :, :NOPE]
    q_rot = rotate(shaped[:, :, NOPE:], cosine[:, None, :], sine[:, None, :])
    key_nope = widened(jnp.dot(latents, w_key, preferred_element_type=jnp.float32)).reshape(TOKENS, HEADS, NOPE)
    head_values = widened(jnp.dot(latents, w_value, preferred_element_type=jnp.float32)).reshape(TOKENS, HEADS, VDIM)
    block_rows = math.gcd(TOKENS, 512)
    score_scale = (NOPE + ROPE) ** (-0.5)

    def attend(block_index):
        first_row = (block_index * block_rows).astype(jnp.int32)
        query_nope = lax.dynamic_slice_in_dim(q_nope, first_row, block_rows, 0).astype(jnp.float32)
        query_rope = lax.dynamic_slice_in_dim(q_rot, first_row, block_rows, 0).astype(jnp.float32)
        scores = jnp.einsum('qhd,khd->hqk', query_nope, key_nope) + jnp.einsum('qhd,kd->hqk', query_rope, key_rot)
        scores = scores * score_scale
        row_max = lax.optimization_barrier(jnp.max(scores, axis=-1, keepdims=True))
        weights = jnp.exp(scores - row_max)
        totals = lax.optimization_barrier(jnp.sum(weights, axis=-1))
        prob_weights = widened(weights)
        heads_block = jnp.einsum('hqk,khd->qhd', prob_weights, head_values) / jnp.transpose(totals)[:, :, None]
        return heads_block.astype(jnp.bfloat16).reshape(block_rows, HEADS * VDIM)
    heads_out = lax.map(attend, jnp.arange(TOKENS // block_rows, dtype=jnp.int32)).reshape(TOKENS, HEADS * VDIM)
    attn_sum = group_sum(heads_out, w_out, HEADS * VDIM // N_TP)
    mixed_in = DEEP_ALPHA * resid.astype(jnp.float32) + attn_sum
    hidden_in = layer_norm(mixed_in, gain_mix)
    gate_sum = jnp.dot(hidden_in, w_gate, preferred_element_type=jnp.float32)
    up_sum = jnp.dot(hidden_in, w_up, preferred_element_type=jnp.float32)
    hidden = (jax.nn.silu(gate_sum) * up_sum).astype(jnp.bfloat16)
    mixer_sum = group_sum(hidden, w_down, FF // N_TP)
    return layer_norm(DEEP_ALPHA * hidden_in.astype(jnp.float32) + HALF_STEP * mixer_sum, gain_out)
```

```python
import functools

import jax
import jax.numpy as jnp
from jax import lax
from jax.experimental import pallas as pl
from jax.experimental.pallas import tpu as pltpu
from jax.sharding import PartitionSpec as P

NOPE = 64
ROPE = 32
VDIM = 64
GRID_W = 64
LANES = 128

ROTARY_BASE = 10000.0
NORM_EPSILON = 1e-06
DEEP_ALPHA = 8.0**0.25
HALF_STEP = 0.5
MESH = pl.DeviceIdType.MESH


def rotary_tables(first, rows):
    at = first + lax.broadcasted_iota(jnp.int32, (rows, LANES), 0)
    column = lax.broadcasted_iota(jnp.int32, (rows, LANES), 1)
    freq_count = ROPE // 4
    grid_row = (at // GRID_W).astype(jnp.float32)
    grid_col = (at % GRID_W).astype(jnp.float32)
    spot = jnp.where(column % (2 * freq_count) < freq_count, grid_row, grid_col)
    inverse = jnp.ones((rows, LANES), jnp.float32)
    for k in range(1, freq_count):
        inverse = jnp.where(column % freq_count == k, ROTARY_BASE ** (-k / freq_count), inverse)
    angles = spot * inverse
    return (jnp.cos(angles)[:, : ROPE // 2], jnp.sin(angles)[:, : ROPE // 2])


def rotate(vectors, cosine, sine):
    half_width = ROPE // 2
    leading = vectors[:, :half_width]
    trailing = vectors[:, half_width:]
    return [leading * cosine - trailing * sine, leading * sine + trailing * cosine]


def ring_device(place, count):
    return jnp.where(place < count // 2, 2 * place, 2 * (count - 1 - place) + 1)


def ring_place(index, count):
    return jnp.where(index % 2 == 0, index // 2, count - 1 - index // 2)


def dot(left, right):
    return jnp.dot(left, right, preferred_element_type=jnp.float32)


def dot_nt(left, right):
    return lax.dot_general(
        left, right, (((1,), (1,)), ((), ())), preferred_element_type=jnp.float32
    )


def layer_kernel(
    n_sp,
    n_tp,
    splits,
    q_ref,
    lat_ref,
    rope_ref,
    wk_ref,
    wv_ref,
    wo_ref,
    resid_ref,
    gain_mix_ref,
    gain_out_ref,
    wg_ref,
    wu_ref,
    wd_ref,
    out_ref,
    lat_all,
    keys,
    rotary,
    values,
    gate_all,
    up_all,
    down_all,
    q_all,
    heads,
    part_send,
    part_recv,
    stat_send,
    stat_recv,
    rows_all,
    part2_send,
    part2_recv,
    stat2_send,
    stat2_recv,
    hid,
    local_sem,
    lat_send,
    lat_recv,
    share_send,
    share_recv,
    ring_send,
    ring_recv,
    tp_send,
    tp_recv,
    down_send,
    down_recv,
):
    sp = lax.axis_index("sp")
    tp = lax.axis_index("tp")
    place = ring_place(sp, n_sp)
    ahead = ring_device((place + 1) % n_sp, n_sp)
    behind = ring_device((place + n_sp - 1) % n_sp, n_sp)
    targets = (ahead, behind)
    partner = tp + 1 - 2 * (tp % 2)
    core = tp % 2
    n_rows = q_ref.shape[0]
    head_count = wk_ref.shape[1] // NOPE
    rank = wk_ref.shape[0]
    lat_rows = lat_all.shape[2]
    n_cols = out_ref.shape[1]

    barrier = pltpu.get_barrier_semaphore()
    for device in targets:
        pl.semaphore_signal(barrier, inc=1, device_id={"sp": device}, device_id_type=MESH)
    for step in range(1, n_tp):
        pl.semaphore_signal(
            barrier, inc=1, device_id={"tp": (tp + step) % n_tp}, device_id_type=MESH
        )

    own = []
    lat_own = pltpu.make_async_copy(
        lat_ref, lat_all.at[sp, :, :, pl.ds(0, rank)], local_sem.at[0]
    )
    lat_own.start()
    weights = (gate_all, up_all, down_all)
    for i, source in enumerate((wg_ref, wu_ref)):
        copy = pltpu.make_async_copy(source, weights[i].at[sp], local_sem.at[i + 1])
        copy.start()
        own.append(copy)
    cosine, sine = rotary_tables(sp * n_rows, n_rows)
    key_rot = rotate(rope_ref[...].astype(jnp.float32), cosine, sine)
    key_rot.append(jnp.zeros((n_rows, LANES - ROPE), jnp.float32))
    lat_all[sp, :, :, pl.ds(rank, LANES)] = (
        jnp.concatenate(key_rot, axis=1).astype(jnp.bfloat16).reshape(4, lat_rows, LANES)
    )

    def prepare_queries(head):
        base = head * (NOPE + ROPE)
        wide_q = q_ref[...].astype(jnp.float32)
        nope = wide_q[:, base : base + NOPE]
        other = jnp.zeros((n_rows, NOPE), jnp.float32)
        rotary = rotate(wide_q[:, base + NOPE : base + NOPE + ROPE], cosine, sine)
        parts = [nope, other] if head % 2 == 0 else [other, nope]
        parts = parts + rotary + [jnp.zeros((n_rows, LANES - ROPE), jnp.float32)]
        q_all[head] = jnp.concatenate(parts, axis=1).astype(jnp.bfloat16)

    def prepare_down():
        count = wd_ref.shape[1]
        across = lax.broadcasted_iota(jnp.int32, (count, count), 1)
        diagonal = (lax.broadcasted_iota(jnp.int32, (count, count), 0) == across).astype(
            jnp.float32
        ).astype(jnp.bfloat16)
        down_all[sp] = dot_nt(diagonal, wd_ref[...]).astype(jnp.bfloat16)

    preparing = [functools.partial(prepare_queries, head) for head in range(head_count)]
    preparing.append(prepare_down)
    pl.semaphore_wait(barrier, 2 + n_tp - 1)

    def origin(hop, direction):
        if direction == 0:
            return ring_device((place + n_sp - hop) % n_sp, n_sp)
        return ring_device((place + hop) % n_sp, n_sp)

    def lat_copy(hop, direction):
        block = lat_all.at[origin(hop - 1, direction), core * 2 + direction]
        return pltpu.make_async_remote_copy(
            src_ref=block,
            dst_ref=block,
            send_sem=lat_send.at[direction],
            recv_sem=lat_recv.at[direction, hop - 1],
            device_id={"sp": targets[direction]},
            device_id_type=MESH,
        )

    def lat_arrival(hop, direction):
        block = lat_all.at[origin(hop, direction), core * 2 + direction]
        return pltpu.make_async_remote_copy(
            src_ref=block,
            dst_ref=block,
            send_sem=lat_send.at[direction],
            recv_sem=lat_recv.at[direction, hop - 1],
            device_id={"sp": targets[direction]},
            device_id_type=MESH,
        )

    def share_copy(hop, direction, which):
        block = lat_all.at[origin(hop, direction), which * 2 + direction]
        return pltpu.make_async_remote_copy(
            src_ref=block,
            dst_ref=block,
            send_sem=share_send.at[direction],
            recv_sem=share_recv.at[direction, hop - 1],
            device_id={"tp": partner},
            device_id_type=MESH,
        )

    piece_rows = wg_ref.shape[0] // (2 * splits)

    def ring_copy(array, piece, hop, direction, arriving):
        block = origin(hop if arriving else hop - 1, direction)
        rows = pl.ds((direction * splits + piece) * piece_rows, piece_rows)
        ref = weights[array].at[block, rows]
        return pltpu.make_async_remote_copy(
            src_ref=ref,
            dst_ref=ref,
            send_sem=ring_send.at[array, piece, direction],
            recv_sem=ring_recv.at[array, piece, direction, hop - 1],
            device_id={"sp": targets[direction]},
            device_id_type=MESH,
        )

    started = set()

    def ring_step(array, piece, hop):
        if hop == 1 and array < 2 and array not in started:
            own[array].wait()
            started.add(array)
        for direction in range(2):
            if hop > 1:
                ring_copy(array, piece, hop - 1, direction, True).wait_recv()
                ring_copy(array, piece, hop - 1, direction, False).wait_send()
            if hop < n_sp:
                ring_copy(array, piece, hop, direction, False).start()

    first = [
        (array, piece, hop)
        for hop in range(1, n_sp)
        for array in range(2)
        for piece in range(splits)
    ]
    second = [(2, piece, hop) for hop in range(1, n_sp) for piece in range(splits)]
    queue = [first + second, 0]

    def advance(count):
        steps, at = queue
        for step in steps[at : at + count]:
            ring_step(*step)
        queue[1] = min(at + count, len(steps))

    unit = max(1, len(first) // 28)

    lat_own.wait()
    for hop in range(1, n_sp + 1):
        for direction in range(2):
            if hop > 1:
                lat_arrival(hop - 1, direction).wait_recv()
                lat_copy(hop - 1, direction).wait_send()
            if hop < n_sp:
                lat_copy(hop, direction).start()
            if hop > 2:
                share_copy(hop - 2, direction, core).wait_send()
            if hop > 1:
                share_copy(hop - 1, direction, core).start()
        if hop < n_sp and queue[1] < 7 * unit:
            advance(1)
        if preparing:
            preparing.pop(0)()
    while preparing:
        preparing.pop(0)()
    for direction in range(2):
        share_copy(n_sp - 1, direction, core).wait_send()
        for hop in range(1, n_sp):
            share_copy(hop, direction, 1 - core).wait_recv()

    total_rows = n_sp * n_rows
    lat_wide = lat_all.shape[3]
    chunk_blocks = max(1, min(n_sp, 1536 // n_rows))
    chunks = n_sp // chunk_blocks
    chunk = chunk_blocks * n_rows
    half_blocks = max(1, chunk_blocks // 2)

    def project(step):
        rows = half_blocks * n_rows
        blocks = pl.ds(step * half_blocks, half_blocks)
        lat = lat_all[blocks, :, :, pl.ds(0, rank)].reshape(rows, rank)
        rotary[pl.ds(step * rows, rows)] = lat_all[blocks, :, :, pl.ds(rank, LANES)].reshape(
            rows, LANES
        )
        keys[pl.ds(step * rows, rows)] = dot(lat, wk_ref[...]).astype(jnp.bfloat16)
        values[pl.ds(step * rows, rows)] = dot(lat, wv_ref[...]).astype(jnp.bfloat16)

    if chunks == 1:
        for step in range(n_sp // half_blocks):
            project(step)
            advance(unit)
    else:
        pl.loop(0, n_sp // half_blocks)(project)
        advance(2 * unit)

    score_scale = (NOPE + ROPE) ** (-0.5)
    lane = lax.broadcasted_iota(jnp.int32, (n_rows, LANES), 1)

    def attend(head, at, state):
        maxima, totals, running = state
        rows = pl.ds(at * chunk, chunk)
        pair = slice(head // 2 * LANES, (head // 2 + 1) * LANES)
        whole_keys = jnp.concatenate([keys[rows, pair], rotary[rows]], axis=1)
        scores = dot_nt(q_all[head], whole_keys) * score_scale
        top = jnp.max(scores, axis=1, keepdims=True)
        if maxima is not None:
            top = jnp.maximum(maxima, top)
        probs = jnp.exp(scores - top)
        sums = jnp.sum(probs, axis=1, keepdims=True)
        update = dot(probs.astype(jnp.bfloat16), values[rows, pair])
        if maxima is not None:
            factor = jnp.exp(maxima - top)
            sums = totals * factor + sums
            update = running * factor + update
        return (top, sums, update)

    for head in range(head_count):
        state = attend(head, 0, (None, None, None))
        if chunks > 1:
            state = lax.fori_loop(1, chunks, functools.partial(attend_loop, attend, head), state)
        result = state[2] / state[1]
        pair = slice(head // 2 * LANES, (head // 2 + 1) * LANES)
        if head % 2 == 0:
            heads[:, pair] = result.astype(jnp.bfloat16)
        else:
            heads[:, pair] = jnp.where(
                lane < VDIM, heads[:, pair].astype(jnp.float32), result
            ).astype(jnp.bfloat16)
        advance(unit)

    def tp_copy(stage, slot_source, slot_target, to, slot_semaphore):
        return pltpu.make_async_remote_copy(
            src_ref=slot_source,
            dst_ref=slot_target,
            send_sem=tp_send.at[stage, slot_semaphore],
            recv_sem=tp_recv.at[stage, slot_semaphore],
            device_id={"tp": to},
            device_id_type=MESH,
        )

    def exchange(stage, source_of, target_of):
        copies = []
        for k in range(1, n_tp):
            to = (tp + k) % n_tp
            copies.append(tp_copy(stage, source_of(to), target_of(k), to, k))
        return copies

    copies = exchange(0, lambda to: part_send.at[to], lambda k: part_recv.at[k])
    for k in range(1, n_tp + 1):
        to = (tp + k) % n_tp
        part_send[to] = dot(
            heads[...], wo_ref[:, pl.ds(pl.multiple_of(to * n_cols, LANES), n_cols)]
        ).astype(jnp.bfloat16)
        if k < n_tp:
            copies[k - 1].start()
    advance(4 * unit)
    mixed = DEEP_ALPHA * resid_ref[...].astype(jnp.float32) + part_send[tp].astype(jnp.float32)
    for k in range(1, n_tp):
        copies[k - 1].wait_recv()
        mixed = mixed + part_recv[k].astype(jnp.float32)
    pending = list(copies)

    width_total = n_cols * n_tp

    def normed(rows_in, gain_ref, stage, send, recv, between):
        sums = jnp.sum(rows_in, axis=1, keepdims=True)
        squares = jnp.sum(rows_in * rows_in, axis=1, keepdims=True)
        mine = jnp.transpose(jnp.where(lane < 4, sums, squares))[:8]
        send[...] = mine
        copies = exchange(stage, lambda to: send, lambda k: recv.at[k])
        for copy in copies:
            copy.start()
        between()
        for k in range(1, n_tp):
            copies[k - 1].wait_recv()
            mine = mine + recv[k]
        pending.extend(copies)
        whole = jnp.transpose(mine) / width_total
        row_mean = whole[:, :1]
        variance = whole[:, 4:5] - row_mean * row_mean
        return (
            (rows_in - row_mean) * lax.rsqrt(variance + NORM_EPSILON) * gain_ref[...]
        ).astype(jnp.bfloat16)

    hidden_in = normed(
        mixed, gain_mix_ref, 1, stat_send, stat_recv, lambda: advance(2 * unit)
    )
    rows_all[tp] = hidden_in
    copies = exchange(2, lambda to: rows_all.at[tp], lambda k: rows_all.at[tp])
    for copy in copies:
        copy.start()
    pending.extend(copies)
    advance(4 * unit)
    for k in range(1, n_tp):
        sender = (tp + n_tp - k) % n_tp
        tp_copy(2, rows_all.at[sender], rows_all.at[sender], sender, k).wait_recv()

    advance(len(first) - queue[1])
    advance(splits)

    def last_hop(array):
        for piece in range(splits):
            for direction in range(2):
                ring_copy(array, piece, n_sp - 1, direction, True).wait_recv()
                ring_copy(array, piece, n_sp - 1, direction, False).wait_send()

    last_hop(0)
    group = n_sp // n_tp
    depth = group * wg_ref.shape[0]
    hidden_width = wg_ref.shape[1]

    def wide(weight):
        total = None
        for t in range(n_tp):
            term = dot(
                rows_all[t],
                weight[t * group : (t + 1) * group].reshape(depth, hidden_width),
            )
            total = term if total is None else total + term
            advance(1)
        return total

    gate_sum = wide(gate_all)
    last_hop(1)
    up_sum = wide(up_all)
    hidden = (gate_sum / (1.0 + jnp.exp(-gate_sum)) * up_sum).astype(jnp.bfloat16)
    advance(1)

    half_rows = piece_rows * splits
    if half_rows % LANES == 0:
        hid[...] = hidden

        def down_copy(k, slot, to, columns):
            ref = part2_send.at[to, :, columns]
            return pltpu.make_async_remote_copy(
                src_ref=ref,
                dst_ref=part2_recv.at[k, :, columns],
                send_sem=down_send.at[k, slot],
                recv_sem=down_recv.at[k, slot],
                device_id={"tp": to},
                device_id_type=MESH,
            )

        def slot_columns(slot):
            return pl.ds(pl.multiple_of(slot * half_rows, LANES), half_rows)

        def make_columns(hop):
            for direction in range(2):
                block = origin(hop, direction)
                owner = block // group
                slot = (block % group) * 2 + direction
                rows = pl.ds(direction * half_rows, half_rows)
                part2_send[owner, :, slot_columns(slot)] = dot_nt(
                    hid[...], down_all[block, rows]
                ).astype(jnp.bfloat16)

                @pl.when(owner != tp)
                def send_away():
                    down_copy((owner + n_tp - tp) % n_tp, slot, owner, slot_columns(slot)).start()

        made = 0
        while queue[1] < len(queue[0]):
            array, piece, hop = queue[0][queue[1]]
            advance(1)
            if piece == splits - 1:
                made_to = hop
                while made < made_to:
                    make_columns(made)
                    made += 1
        while made < n_sp - 1:
            make_columns(made)
            made += 1
        last_hop(2)
        make_columns(n_sp - 1)
        mixer = part2_send[tp].astype(jnp.float32)
        for k in range(1, n_tp):
            for slot in range(2 * group):
                down_copy(k, slot, (tp + k) % n_tp, slot_columns(slot)).wait_recv()
            mixer = mixer + part2_recv[k].astype(jnp.float32)
    else:
        advance(len(queue[0]))
        last_hop(2)
        copies = exchange(3, lambda to: part2_send.at[to], lambda k: part2_recv.at[k])
        for k in range(1, n_tp + 1):
            to = (tp + k) % n_tp
            part2_send[to] = dot_nt(
                hidden, down_all[pl.ds(to * group, group)].reshape(depth, hidden_width)
            ).astype(jnp.bfloat16)
            if k < n_tp:
                copies[k - 1].start()
        mixer = part2_send[tp].astype(jnp.float32)
        for k in range(1, n_tp):
            copies[k - 1].wait_recv()
            mixer = mixer + part2_recv[k].astype(jnp.float32)
        pending.extend(copies)
    final = DEEP_ALPHA * rows_all[tp].astype(jnp.float32) + HALF_STEP * mixer
    out_ref[...] = normed(final, gain_out_ref, 4, stat2_send, stat2_recv, lambda: None)
    for copy in pending:
        copy.wait_send()
    if half_rows % LANES == 0:
        for k in range(1, n_tp):
            for slot in range(2 * group):
                down_copy(k, slot, (tp + k) % n_tp, slot_columns(slot)).wait_send()


def attend_loop(attend, head, at, state):
    return attend(head, at, state)


def flip(value, mask):
    result = value
    bit = 1
    while bit <= mask:
        if mask & bit:
            result = result + bit - 2 * bit * ((value // bit) % 2)
        bit *= 2
    return result


class Slots:
    def __init__(self, sends, recvs):
        self.sends, self.recvs, self.base, self.used = sends, recvs, {}, 0

    def at(self, name, count, index):
        if name not in self.base:
            self.base[name] = self.used
            self.used += count
        place = self.base[name] + index
        return self.sends.at[place], self.recvs.at[place]


def slot_total(n_hi, pieces):
    return 16 * n_hi + 6 * n_hi * pieces + 64


def paired_kernel(
    n_sp,
    n_tp,
    pieces,
    q_in,
    lat_ref,
    rope_in,
    wk_in,
    wv_in,
    wo_ref,
    resid_in,
    gain_mix_in,
    gain_out_in,
    wg_ref,
    wu_ref,
    wd_ref,
    out_ref,
    q_ref,
    rope_ref,
    wk_ref,
    wv_ref,
    resid_ref,
    gain_mix_ref,
    gain_out_ref,
    lat_all,
    keys,
    rotary,
    values,
    q_all,
    heads_all,
    wo_all,
    wide_all,
    down_all,
    rows_all,
    hid,
    summed,
    core_send,
    core_recv,
    far_send,
    far_recv,
    pair_send,
    pair_recv,
    stat_send,
    stat_recv,
    local_sem,
    input_sem,
    sends,
    recvs,
):
    sp = lax.axis_index("sp")
    tp = lax.axis_index("tp")
    n_hi = n_sp // 2
    z, x = sp // 2, sp % 2
    half = z % 2
    edge = half == (z // 2) % 2
    n_rows = q_ref.shape[0]
    head_count = wk_ref.shape[1] // NOPE
    rank = wk_ref.shape[0]
    lat_rows = lat_all.shape[2]
    n_cols = out_ref.shape[1]
    group = n_sp // n_tp
    depth = wg_ref.shape[0]
    width = wg_ref.shape[1] // 2
    down_cols = wd_ref.shape[1]
    total_rows = n_sp * n_rows
    slots = Slots(sends, recvs)
    pending = []

    order = [(1, flip(z, 1))]
    for m in range(2, n_hi, 2):
        low, high = flip(z, m), flip(z, m + 1)
        order.append((jnp.where(edge, m, m + 1), jnp.where(edge, low, high)))
        order.append((jnp.where(edge, m + 1, m), jnp.where(edge, high, low)))

    def sp_of(place, side):
        return 2 * place + side

    def remote(name, count, index, source, target, device):
        send, recv = slots.at(name, count, index)
        return pltpu.make_async_remote_copy(
            src_ref=source,
            dst_ref=target,
            send_sem=send,
            recv_sem=recv,
            device_id=device,
            device_id_type=MESH,
        )

    def start(copy):
        copy.start()
        pending.append(copy)

    other_x = 1 - x
    partner, across, corner = flip(tp, 1), flip(tp, 2), flip(tp, 3)
    to_x = {"sp": sp_of(z, other_x)}
    to_pair = {"sp": sp_of(flip(z, 1), x)}
    to_core = {"tp": partner}
    to_across = {"tp": across}

    barrier = pltpu.get_barrier_semaphore()
    peers = [{"sp": sp_of(flip(z, k), x)} for k in range(1, n_hi)] + [to_x]
    peers += [{"tp": flip(tp, j)} for j in range(1, n_tp)]
    peers.append({"sp": sp_of(flip(z, 1), x), "tp": across})
    for device in peers:
        pl.semaphore_signal(barrier, inc=1, device_id=device, device_id_type=MESH)

    inputs = {}
    for at, (name, source, target) in enumerate(
        (
            ("rope", rope_in, rope_ref),
            ("q", q_in, q_ref),
            ("wk", wk_in, wk_ref),
            ("wv", wv_in, wv_ref),
            ("resid", resid_in, resid_ref),
            ("mix", gain_mix_in, gain_mix_ref),
            ("out", gain_out_in, gain_out_ref),
        )
    ):
        inputs[name] = pltpu.make_async_copy(source, target, input_sem.at[at])

    def weight_rows(array, piece):
        size = (depth if array < 2 else width) // pieces
        return piece * size, size

    def weight_source(array, which, piece):
        first, size = weight_rows(array, piece)
        if array == 2:
            return wd_ref.at[pl.ds(pl.multiple_of(which * width + first, 16), size)]
        columns = pl.ds(pl.multiple_of(which * width, LANES), width)
        return (wg_ref, wu_ref)[array].at[pl.ds(first, size), columns]

    def weight_block(array, block, piece):
        first, size = weight_rows(array, piece)
        if array == 2:
            return down_all.at[block, pl.ds(first, size)]
        return wide_all.at[block, pl.ds(first, size), pl.ds(array * width, width)]

    def weight_out(array, k):
        place = flip(z, k)
        for piece in range(pieces):
            remote(
                ("wz", array, piece),
                n_hi,
                k,
                weight_source(array, place % 2, piece),
                weight_block(array, sp, piece),
                {"sp": sp_of(place, x)},
            ).start()

    def weight_in(array, at, piece):
        k, place = order[at]
        block = weight_block(array, sp_of(place, x), piece)
        return remote(("wz", array, piece), n_hi, k, block, block, to_x)

    def weight_side(array, k, place, piece):
        block = weight_block(array, sp_of(place, x), piece)
        return remote(("wx", array, piece), n_hi, k, block, block, to_x)

    def weight_side_in(array, k, place, piece):
        block = weight_block(array, sp_of(place, other_x), piece)
        return remote(("wx", array, piece), n_hi, k, block, block, to_x)

    def weight_own(array, piece):
        start(
            remote(
                ("wx", array, piece),
                n_hi,
                0,
                weight_source(array, half, piece),
                weight_block(array, sp, piece),
                to_x,
            )
        )

    def relay(array, at):
        for piece in range(pieces):
            weight_in(array, at, piece).wait_recv()
            start(weight_side(array, order[at][0], order[at][1], piece))

    lat_own = pltpu.make_async_copy(
        lat_ref, lat_all.at[sp, :, :, pl.ds(0, rank)], local_sem.at[0]
    )
    inputs["rope"].start()
    lat_own.start()
    for name in ("q", "wk", "wv", "resid", "mix", "out"):
        inputs[name].start()
    own = []
    for array in range(3):
        for piece in range(pieces):
            copy = pltpu.make_async_copy(
                weight_source(array, half, piece),
                weight_block(array, sp, piece),
                local_sem.at[1 + array * pieces + piece],
            )
            copy.start()
            own.append(copy)

    def wo_columns(which):
        return wo_ref.at[:, pl.ds(pl.multiple_of(which * n_cols, LANES), n_cols)]

    wo_own = pltpu.make_async_copy(
        wo_columns(tp), wo_all.at[tp], local_sem.at[1 + 3 * pieces]
    )
    wo_own.start()
    cosine, sine = rotary_tables(sp * n_rows, n_rows)
    inputs["rope"].wait()
    turned_in = jnp.concatenate(
        [rope_ref[...].astype(jnp.float32), jnp.zeros((LANES - ROPE, n_rows), jnp.float32)],
        axis=0,
    )
    key_rot = rotate(jnp.transpose(turned_in)[:, :ROPE], cosine, sine)
    key_rot.append(jnp.zeros((n_rows, LANES - ROPE), jnp.float32))
    lat_all[sp, :, :, pl.ds(rank, LANES)] = (
        jnp.concatenate(key_rot, axis=1).astype(jnp.bfloat16).reshape(n_tp, lat_rows, LANES)
    )

    def prepare_queries(head):
        base = head * (NOPE + ROPE)
        wide_q = q_ref[...].astype(jnp.float32)
        nope = wide_q[:, base : base + NOPE]
        other = jnp.zeros((n_rows, NOPE), jnp.float32)
        turned = rotate(wide_q[:, base + NOPE : base + NOPE + ROPE], cosine, sine)
        parts = [nope, other] if head % 2 == 0 else [other, nope]
        parts = parts + turned + [jnp.zeros((n_rows, LANES - ROPE), jnp.float32)]
        q_all[head] = jnp.concatenate(parts, axis=1).astype(jnp.bfloat16)

    pl.semaphore_wait(barrier, len(peers))
    lat_own.wait()

    def lat_block(place, side, quarter):
        return lat_all.at[sp_of(place, side), quarter]

    def lat_copy(name, k, place, side, quarter, device):
        block = lat_block(place, side, quarter)
        return remote(("lat", name), n_hi, k, block, block, device)

    def lat_z_in(at):
        k, place = order[at]
        lat_copy("z", k, place, x, tp, to_x).wait_recv()
        start(lat_copy("x", k, place, x, tp, to_x))
        start(lat_copy("y", k, place, x, tp, to_across))
        start(lat_copy("cz", k, place, x, tp, to_core))

    def lat_x_in(k, place):
        lat_copy("x", k, place, other_x, tp, to_x).wait_recv()
        start(lat_copy("yd", k, place, other_x, tp, to_across))
        start(lat_copy("cx", k, place, other_x, tp, to_core))

    def lat_y_in(k, place):
        lat_copy("y", k, place, x, across, to_across).wait_recv()
        start(lat_copy("cy", k, place, x, across, to_core))

    def lat_yd_in(k, place):
        lat_copy("yd", k, place, other_x, across, to_across).wait_recv()
        start(lat_copy("cyd", k, place, other_x, across, to_core))

    for k in list(range(n_hi - 1, 0, -1)):
        block = lat_block(z, x, tp)
        start(remote(("lat", "z"), n_hi, k, block, block, {"sp": sp_of(flip(z, k), x)}))
    start(lat_copy("x", 0, z, x, tp, to_x))
    weight_own(0, 0)

    far = list(range(2, n_hi))

    def first_batch():
        for array in range(3):
            weight_out(array, 1)
        for array in range(2):
            for k in far:
                weight_out(array, k)

    def second_batch():
        for k in far:
            weight_out(2, k)

    @pl.when(edge)
    def outer_first():
        first_batch()

    inputs["q"].wait()
    prepare_queries(0)
    lat_x_in(0, z)
    lat_z_in(0)

    @pl.when(jnp.logical_not(edge))
    def inner_first():
        first_batch()

    prepare_queries(1)
    lat_z_in(1)
    lat_x_in(*order[0])
    for at in range(2, len(order)):
        lat_z_in(at)
    for head in range(2, head_count):
        prepare_queries(head)
    for at in range(1, len(order)):
        lat_x_in(*order[at])
    lat_y_in(*order[0])
    lat_yd_in(0, z)
    lat_yd_in(*order[0])
    for at in range(1, len(order)):
        lat_y_in(*order[at])
    for piece in range(1, pieces):
        weight_own(0, piece)
    for array in (1, 2):
        for piece in range(pieces):
            weight_own(array, piece)
    for j in (2, 3, 1):
        to = flip(tp, j)
        start(
            remote("wo", n_tp, j, wo_columns(to), wo_all.at[tp], {"tp": to})
        )
    for at in range(1, len(order)):
        lat_yd_in(*order[at])
    for k, place in [(0, z)] + order:
        if place is not z:
            lat_copy("cz", k, place, x, partner, to_core).wait_recv()
            lat_copy("cy", k, place, x, corner, to_core).wait_recv()
        lat_copy("cx", k, place, other_x, partner, to_core).wait_recv()
        lat_copy("cyd", k, place, other_x, corner, to_core).wait_recv()

    near, rest = list(range(1, len(order), 2)), list(range(2, len(order), 2))
    relays = [(0, 0)] + [(0, at) for at in near] + [(1, 0), (2, 0)]
    relays += [(1, at) for at in near] + [(0, at) for at in rest]
    relays_early = len(relays)
    relays += [(1, at) for at in rest]
    relays_wide = len(relays)
    relays += [(2, at) for at in near] + [(2, at) for at in rest]
    queue = [0]

    def advance(count):
        for array, at in relays[queue[0] : queue[0] + count]:
            relay(array, at)
        queue[0] = min(queue[0] + count, len(relays))

    half_blocks = n_sp // 2

    def project(step):
        rows = half_blocks * n_rows
        blocks = pl.ds(step * half_blocks, half_blocks)
        lat = lat_all[blocks, :, :, pl.ds(0, rank)].reshape(rows, rank)
        rotary[pl.ds(step * rows, rows)] = lat_all[blocks, :, :, pl.ds(rank, LANES)].reshape(
            rows, LANES
        )
        keys[pl.ds(step * rows, rows)] = dot(lat, wk_ref[...]).astype(jnp.bfloat16)
        values[pl.ds(step * rows, rows)] = dot(lat, wv_ref[...]).astype(jnp.bfloat16)

    inputs["wk"].wait()
    inputs["wv"].wait()
    advance(1)
    for step in range(n_sp // half_blocks):
        project(step)
    advance(1)

    score_scale = (NOPE + ROPE) ** (-0.5)
    lane = lax.broadcasted_iota(jnp.int32, (n_rows, LANES), 1)

    def heads_copy(piece, j, owner):
        block = heads_all.at[owner, :, pl.ds(piece * LANES, LANES)]
        return remote(("heads", piece), n_tp, j, block, block, {"tp": flip(tp, j)})

    for head in range(head_count):
        pair = slice(head // 2 * LANES, (head // 2 + 1) * LANES)
        whole_keys = jnp.concatenate([keys[:, pair], rotary[...]], axis=1)
        scores = dot_nt(q_all[head], whole_keys) * score_scale
        top = jnp.max(scores, axis=1, keepdims=True)
        probs = jnp.exp(scores - top)
        sums = jnp.sum(probs, axis=1, keepdims=True)
        result = dot(probs.astype(jnp.bfloat16), values[:, pair]) / sums
        if head % 2 == 0:
            held = result
        else:
            heads_all[tp, :, pair] = jnp.where(lane < VDIM, held, result).astype(jnp.bfloat16)
            for j in (2, 3, 1):
                start(heads_copy(head // 2, j, tp))
        if head < head_count - 1:
            advance(1)

    @pl.when(jnp.logical_not(edge))
    def inner_rest():
        second_batch()

    advance(relays_early - queue[0])
    inputs["resid"].wait()
    inputs["mix"].wait()
    inputs["out"].wait()
    mixed = DEEP_ALPHA * resid_ref[...].astype(jnp.float32)
    wo_own.wait()
    mixed = mixed + dot(heads_all[tp], wo_all[tp])
    for j in (1, 2, 3):
        sender = flip(tp, j)
        remote("wo", n_tp, j, wo_all.at[sender], wo_all.at[sender], to_core).wait_recv()
        for piece in range(head_count // 2):
            heads_copy(piece, j, sender).wait_recv()
        mixed = mixed + dot(heads_all[sender], wo_all[sender])

    width_total = n_cols * n_tp

    def normed(rows_in, gain_ref, stage, between):
        sums = jnp.sum(rows_in, axis=1, keepdims=True)
        squares = jnp.sum(rows_in * rows_in, axis=1, keepdims=True)
        mine = jnp.transpose(jnp.where(lane < 4, sums, squares))[:8]
        stat_send[stage] = mine
        for j in (2, 3, 1):
            start(
                remote(
                    ("stat", stage),
                    n_tp,
                    j,
                    stat_send.at[stage],
                    stat_recv.at[stage, j],
                    {"tp": flip(tp, j)},
                )
            )
        between()
        for j in (1, 2, 3):
            remote(
                ("stat", stage),
                n_tp,
                j,
                stat_send.at[stage],
                stat_recv.at[stage, j],
                to_core,
            ).wait_recv()
            mine = mine + stat_recv[stage, j]
        whole = jnp.transpose(mine) / width_total
        row_mean = whole[:, :1]
        variance = whole[:, 4:5] - row_mean * row_mean
        return (
            (rows_in - row_mean) * lax.rsqrt(variance + NORM_EPSILON) * gain_ref[...]
        ).astype(jnp.bfloat16)

    hidden_in = normed(mixed, gain_mix_ref, 0, lambda: None)
    mine = pl.ds(pl.multiple_of(half * n_rows, 16), n_rows)
    theirs = pl.ds(pl.multiple_of((1 - half) * n_rows, 16), n_rows)
    rows_all[tp, mine] = hidden_in

    def rows_copy(name, owner, rows, device):
        block = rows_all.at[owner, rows]
        return remote(("rows", name), 1, 0, block, block, device)

    start(
        rows_copy("yz", tp, mine, {"sp": sp_of(flip(z, 1), x), "tp": across})
    )
    start(rows_copy("y", tp, mine, to_across))
    start(rows_copy("z", tp, mine, to_pair))
    start(rows_copy("c", tp, mine, to_core))

    @pl.when(edge)
    def outer_rest():
        second_batch()

    rows_copy("z", tp, theirs, to_pair).wait_recv()
    start(rows_copy("cz", tp, theirs, to_core))
    rows_copy("y", across, mine, to_across).wait_recv()
    start(rows_copy("cy", across, mine, to_core))
    rows_copy("yz", across, theirs, to_across).wait_recv()
    start(rows_copy("cyz", across, theirs, to_core))
    rows_copy("c", partner, mine, to_core).wait_recv()
    rows_copy("cz", partner, theirs, to_core).wait_recv()
    rows_copy("cy", corner, mine, to_core).wait_recv()
    rows_copy("cyz", corner, theirs, to_core).wait_recv()
    advance(relays_wide - queue[0])
    for copy in own:
        copy.wait()
    for k, place in [(0, z)] + order:
        for array in range(2):
            for piece in range(pieces):
                weight_side_in(array, k, place, piece).wait_recv()

    total = None
    for t in range(n_tp):
        term = dot(
            rows_all[t], wide_all[t * group : (t + 1) * group].reshape(group * depth, 2 * width)
        )
        total = term if total is None else total + term
    gate_sum, up_sum = total[:, :width], total[:, width:]
    hid[...] = (gate_sum / (1.0 + jnp.exp(-gate_sum)) * up_sum).astype(jnp.bfloat16)

    blocks = []
    for k, place in [(0, z)] + order:
        blocks += [(k, place, x), (k, place, other_x)]

    def block_facts(at):
        k, place, side = blocks[at]
        block = sp_of(place, side)
        owner = block // group
        return block, owner, tp % 2 == owner % 2, tp // 2 == owner // 2

    def core_copy(block):
        return remote(
            "core", n_sp, block, core_send.at[block], core_recv.at[block], to_core
        )

    def far_copy(block):
        return remote("far", n_sp, block, far_send.at[block], far_recv.at[block], to_across)

    def pair_copy(block):
        slot = block % group
        return remote("pair", group, slot, pair_send.at[slot], pair_recv.at[slot], to_pair)

    def make_block(at):
        block, owner, same_core, same_chip = block_facts(at)
        product = dot(hid[...], down_all[block])

        @pl.when(same_core)
        def keep():
            summed[block] = product

        @pl.when(jnp.logical_not(same_core))
        def give():
            core_send[block] = product.astype(jnp.bfloat16)
            core_copy(block).start()

    def add_core(at):
        block, owner, same_core, same_chip = block_facts(at)

        @pl.when(same_core)
        def add():
            core_copy(block).wait_recv()
            both = summed[block] + core_recv[block].astype(jnp.float32)

            @pl.when(same_chip)
            def keep():
                summed[block] = both

            @pl.when(jnp.logical_not(same_chip))
            def give():
                far_send[block] = both.astype(jnp.bfloat16)
                far_copy(block).start()

    def add_far(at):
        block, owner, same_core, same_chip = block_facts(at)

        @pl.when(owner == tp)
        def add():
            far_copy(block).wait_recv()
            summed[block] = summed[block] + far_recv[block].astype(jnp.float32)
            pair_send[block % group] = summed[block, theirs].astype(jnp.bfloat16)
            pair_copy(block).start()

    def down_ready(at):
        k, place, side = blocks[at]
        if at % 2 == 1:
            for piece in range(pieces):
                weight_side_in(2, k, place, piece).wait_recv()

    last = len(blocks)
    steps = last // 2
    for step in range(steps + 2):
        if step < steps:
            if step > 1:
                advance(1)
            for at in (2 * step, 2 * step + 1):
                down_ready(at)
                make_block(at)
        if 1 <= step <= steps:
            add_core(2 * step - 2)
            add_core(2 * step - 1)
        if step >= 2:
            add_far(2 * step - 4)
            add_far(2 * step - 3)

    final = []
    for slot in range(group):
        block = tp * group + slot
        pair_copy(block).wait_recv()
        final.append(summed[block, mine] + pair_recv[slot].astype(jnp.float32))
    mixer = jnp.concatenate(final, axis=1)
    last_in = DEEP_ALPHA * rows_all[tp, mine].astype(jnp.float32) + HALF_STEP * mixer
    out_ref[...] = normed(last_in, gain_out_ref, 1, lambda: None)

    for copy in pending:
        copy.wait_send()
    for array in range(3):
        for k in range(1, n_hi):
            for piece in range(pieces):
                block = weight_block(array, sp, piece)
                remote(("wz", array, piece), n_hi, k, block, block, to_x).wait_send()
    for at in range(last):
        block, owner, same_core, same_chip = block_facts(at)

        @pl.when(jnp.logical_not(same_core))
        def core_sent():
            core_copy(block).wait_send()

        @pl.when(jnp.logical_and(same_core, jnp.logical_not(same_chip)))
        def far_sent():
            far_copy(block).wait_send()

    for slot in range(group):
        pair_copy(tp * group + slot).wait_send()


def paired_call(n_sp, n_tp, operands):
    queries, latents, rope_key, w_key, w_value, w_out, resid, gain_mix = operands[:8]
    w_gate, w_up, w_down, gain_out = operands[8:]
    rows = queries.shape[0]
    head_count = w_key.shape[1] // NOPE
    rank = latents.shape[1]
    cols = resid.shape[1]
    depth, hidden_width = w_gate.shape
    width = hidden_width // 2
    down_cols = w_down.shape[1]
    total_rows = n_sp * rows
    group = n_sp // n_tp
    pieces = 2
    bf16 = jnp.bfloat16
    vmem = pl.BlockSpec(memory_space=pltpu.VMEM)
    anywhere = pl.BlockSpec(memory_space=pl.ANY)
    dma = pltpu.SemaphoreType.DMA
    count = 132
    return pl.pallas_call(
        functools.partial(paired_kernel, n_sp, n_tp, pieces),
        out_shape=jax.ShapeDtypeStruct((rows, cols), bf16),
        in_specs=[anywhere] * 12,
        out_specs=vmem,
        scratch_shapes=[
            pltpu.VMEM(queries.shape, bf16),
            pltpu.VMEM((rope_key.shape[1], rows), bf16),
            pltpu.VMEM(w_key.shape, bf16),
            pltpu.VMEM(w_value.shape, bf16),
            pltpu.VMEM(resid.shape, bf16),
            pltpu.VMEM((1, cols), jnp.float32),
            pltpu.VMEM((1, cols), jnp.float32),
            pltpu.VMEM((n_sp, n_tp, rows // n_tp, rank + LANES), bf16),
            pltpu.VMEM((total_rows, head_count * NOPE), bf16),
            pltpu.VMEM((total_rows, LANES), bf16),
            pltpu.VMEM((total_rows, head_count * VDIM), bf16),
            pltpu.VMEM((head_count, rows, 2 * LANES), bf16),
            pltpu.VMEM((n_tp, rows, head_count * VDIM), bf16),
            pltpu.VMEM((n_tp, head_count * VDIM, cols), bf16),
            pltpu.VMEM((n_sp, depth, 2 * width), bf16),
            pltpu.VMEM((n_sp, width, down_cols), bf16),
            pltpu.VMEM((n_tp, 2 * rows, cols), bf16),
            pltpu.VMEM((2 * rows, width), bf16),
            pltpu.VMEM((n_sp, 2 * rows, down_cols), jnp.float32),
            pltpu.VMEM((n_sp, 2 * rows, down_cols), bf16),
            pltpu.VMEM((n_sp, 2 * rows, down_cols), bf16),
            pltpu.VMEM((n_sp, 2 * rows, down_cols), bf16),
            pltpu.VMEM((n_sp, 2 * rows, down_cols), bf16),
            pltpu.VMEM((group, rows, down_cols), bf16),
            pltpu.VMEM((group, rows, down_cols), bf16),
            pltpu.VMEM((2, 8, rows), jnp.float32),
            pltpu.VMEM((2, n_tp, 8, rows), jnp.float32),
            dma((2 + 3 * pieces,)),
            dma((7,)),
            dma((count,)),
            dma((count,)),
        ],
        compiler_params=pltpu.CompilerParams(
            collective_id=1, has_side_effects=True, vmem_limit_bytes=66000000
        ),
    )(
        queries,
        latents.reshape(n_tp, rows // n_tp, rank),
        rope_key.T,
        w_key,
        w_value,
        w_out,
        resid,
        gain_mix.reshape(1, -1),
        gain_out.reshape(1, -1),
        w_gate,
        w_up,
        w_down,
    )


def fits_pairs(n_sp, n_tp, operands):
    queries, w_key, w_gate, w_down = operands[0], operands[3], operands[8], operands[10]
    return (
        n_tp == 4
        and n_sp % n_tp == 0
        and (n_sp & (n_sp - 1)) == 0
        and queries.shape[0] % 64 == 0
        and n_sp * queries.shape[0] <= 1536
        and (w_key.shape[1] // NOPE) % 2 == 0
        and w_gate.shape[1] % (2 * LANES) == 0
        and w_gate.shape[0] % 32 == 0
        and w_down.shape[1] % LANES == 0
    )


def local(
    queries,
    latents,
    rope_key,
    w_key,
    w_value,
    w_out,
    resid,
    gain_mix,
    w_gate,
    w_up,
    w_down,
    gain_out,
):
    n_sp = lax.axis_size("sp")
    n_tp = lax.axis_size("tp")
    operands = (queries, latents, rope_key, w_key, w_value, w_out, resid, gain_mix)
    operands += (w_gate, w_up, w_down, gain_out)
    if fits_pairs(n_sp, n_tp, operands):
        return paired_call(n_sp, n_tp, operands)
    rows = queries.shape[0]
    head_count = w_key.shape[1] // NOPE
    rank = latents.shape[1]
    cols = resid.shape[1]
    hidden_width = w_gate.shape[1]
    weight_rows = w_gate.shape[0]
    lat_wide = rank + LANES
    splits = 2 if weight_rows % 64 == 0 else 1
    bf16 = jnp.bfloat16
    total_rows = n_sp * rows
    vmem = pl.BlockSpec(memory_space=pltpu.VMEM)
    anywhere = pl.BlockSpec(memory_space=pl.ANY)
    dma = pltpu.SemaphoreType.DMA
    return pl.pallas_call(
        functools.partial(layer_kernel, n_sp, n_tp, splits),
        out_shape=jax.ShapeDtypeStruct((rows, cols), bf16),
        in_specs=[vmem, anywhere] + [vmem] * 7 + [anywhere] * 2 + [vmem],
        out_specs=vmem,
        scratch_shapes=[
            pltpu.VMEM((n_sp, 4, rows // 4, lat_wide), bf16),
            pltpu.VMEM((total_rows, head_count * NOPE), bf16),
            pltpu.VMEM((total_rows, LANES), bf16),
            pltpu.VMEM((total_rows, head_count * VDIM), bf16),
            pltpu.VMEM((n_sp, weight_rows, hidden_width), bf16),
            pltpu.VMEM((n_sp, weight_rows, hidden_width), bf16),
            pltpu.VMEM((n_sp, weight_rows, hidden_width), bf16),
            pltpu.VMEM((head_count, rows, 2 * LANES), bf16),
            pltpu.VMEM((rows, head_count * VDIM), bf16),
            pltpu.VMEM((n_tp, rows, cols), bf16),
            pltpu.VMEM((n_tp, rows, cols), bf16),
            pltpu.VMEM((8, rows), jnp.float32),
            pltpu.VMEM((n_tp, 8, rows), jnp.float32),
            pltpu.VMEM((n_tp, rows, cols), bf16),
            pltpu.VMEM((n_tp, rows, cols), bf16),
            pltpu.VMEM((n_tp, rows, cols), bf16),
            pltpu.VMEM((8, rows), jnp.float32),
            pltpu.VMEM((n_tp, 8, rows), jnp.float32),
            pltpu.VMEM((rows, hidden_width), bf16),
            dma((4,)),
            dma((2,)),
            dma((2, n_sp - 1)),
            dma((2,)),
            dma((2, n_sp - 1)),
            dma((3, splits, 2)),
            dma((3, splits, 2, n_sp - 1)),
            dma((5, n_tp)),
            dma((5, n_tp)),
            dma((n_tp, 2 * (n_sp // n_tp))),
            dma((n_tp, 2 * (n_sp // n_tp))),
        ],
        compiler_params=pltpu.CompilerParams(
            collective_id=0, has_side_effects=True, vmem_limit_bytes=66000000
        ),
    )(
        queries,
        latents.reshape(4, rows // 4, rank),
        rope_key,
        w_key,
        w_value,
        w_out,
        resid,
        gain_mix.reshape(1, -1),
        gain_out.reshape(1, -1),
        w_gate,
        w_up,
        w_down,
    )


def solution(mesh):
    placed = (
        P("sp", "tp"),
        P("sp", None),
        P("sp", None),
        P(None, "tp"),
        P(None, "tp"),
        P("tp", None),
        P("sp", "tp"),
        P("tp"),
        P("sp", "tp"),
        P("sp", "tp"),
        P("tp", "sp"),
        P("tp"),
    )
    return jax.shard_map(
        local, mesh=mesh, in_specs=placed, out_specs=P("sp", "tp"), check_vma=False
    )
```

```python
import functools

import jax
import jax.numpy as jnp
from jax import lax
from jax.experimental import pallas as pl
from jax.experimental.pallas import tpu as pltpu
from jax.sharding import PartitionSpec as P

NOPE = 64
ROPE = 32
VDIM = 64
GRID_W = 64
LANES = 128

ROTARY_BASE = 10000.0
NORM_EPSILON = 1e-06
DEEP_ALPHA = 8.0**0.25
HALF_STEP = 0.5
MESH = pl.DeviceIdType.MESH


def rotary_tables(first, rows):
    at = first + lax.broadcasted_iota(jnp.int32, (rows, LANES), 0)
    column = lax.broadcasted_iota(jnp.int32, (rows, LANES), 1)
    freq_count = ROPE // 4
    grid_row = (at // GRID_W).astype(jnp.float32)
    grid_col = (at % GRID_W).astype(jnp.float32)
    spot = jnp.where(column % (2 * freq_count) < freq_count, grid_row, grid_col)
    inverse = jnp.ones((rows, LANES), jnp.float32)
    for k in range(1, freq_count):
        inverse = jnp.where(column % freq_count == k, ROTARY_BASE ** (-k / freq_count), inverse)
    angles = spot * inverse
    return (jnp.cos(angles)[:, : ROPE // 2], jnp.sin(angles)[:, : ROPE // 2])


def rotate(vectors, cosine, sine):
    half_width = ROPE // 2
    leading = vectors[:, :half_width]
    trailing = vectors[:, half_width:]
    return [leading * cosine - trailing * sine, leading * sine + trailing * cosine]


def ring_device(place, count):
    return jnp.where(place < count // 2, 2 * place, 2 * (count - 1 - place) + 1)


def ring_place(index, count):
    return jnp.where(index % 2 == 0, index // 2, count - 1 - index // 2)


def dot(left, right):
    return jnp.dot(left, right, preferred_element_type=jnp.float32)


def dot_nt(left, right):
    return lax.dot_general(
        left, right, (((1,), (1,)), ((), ())), preferred_element_type=jnp.float32
    )


def layer_kernel(
    n_sp,
    n_tp,
    splits,
    q_ref,
    lat_ref,
    rope_ref,
    wk_ref,
    wv_ref,
    wo_ref,
    resid_ref,
    gain_mix_ref,
    gain_out_ref,
    wg_ref,
    wu_ref,
    wd_ref,
    out_ref,
    lat_all,
    keys,
    rotary,
    values,
    gate_all,
    up_all,
    down_all,
    q_all,
    heads,
    part_send,
    part_recv,
    stat_send,
    stat_recv,
    rows_all,
    part2_send,
    part2_recv,
    stat2_send,
    stat2_recv,
    hid,
    local_sem,
    lat_send,
    lat_recv,
    share_send,
    share_recv,
    ring_send,
    ring_recv,
    tp_send,
    tp_recv,
    down_send,
    down_recv,
):
    sp = lax.axis_index("sp")
    tp = lax.axis_index("tp")
    place = ring_place(sp, n_sp)
    ahead = ring_device((place + 1) % n_sp, n_sp)
    behind = ring_device((place + n_sp - 1) % n_sp, n_sp)
    targets = (ahead, behind)
    partner = tp + 1 - 2 * (tp % 2)
    core = tp % 2
    n_rows = q_ref.shape[0]
    head_count = wk_ref.shape[1] // NOPE
    rank = wk_ref.shape[0]
    lat_rows = lat_all.shape[2]
    n_cols = out_ref.shape[1]

    barrier = pltpu.get_barrier_semaphore()
    for device in targets:
        pl.semaphore_signal(barrier, inc=1, device_id={"sp": device}, device_id_type=MESH)
    for step in range(1, n_tp):
        pl.semaphore_signal(
            barrier, inc=1, device_id={"tp": (tp + step) % n_tp}, device_id_type=MESH
        )

    own = []
    lat_own = pltpu.make_async_copy(
        lat_ref, lat_all.at[sp, :, :, pl.ds(0, rank)], local_sem.at[0]
    )
    lat_own.start()
    weights = (gate_all, up_all, down_all)
    for i, source in enumerate((wg_ref, wu_ref)):
        copy = pltpu.make_async_copy(source, weights[i].at[sp], local_sem.at[i + 1])
        copy.start()
        own.append(copy)
    cosine, sine = rotary_tables(sp * n_rows, n_rows)
    key_rot = rotate(rope_ref[...].astype(jnp.float32), cosine, sine)
    key_rot.append(jnp.zeros((n_rows, LANES - ROPE), jnp.float32))
    lat_all[sp, :, :, pl.ds(rank, LANES)] = (
        jnp.concatenate(key_rot, axis=1).astype(jnp.bfloat16).reshape(4, lat_rows, LANES)
    )

    def prepare_queries(head):
        base = head * (NOPE + ROPE)
        wide_q = q_ref[...].astype(jnp.float32)
        nope = wide_q[:, base : base + NOPE]
        other = jnp.zeros((n_rows, NOPE), jnp.float32)
        rotary = rotate(wide_q[:, base + NOPE : base + NOPE + ROPE], cosine, sine)
        parts = [nope, other] if head % 2 == 0 else [other, nope]
        parts = parts + rotary + [jnp.zeros((n_rows, LANES - ROPE), jnp.float32)]
        q_all[head] = jnp.concatenate(parts, axis=1).astype(jnp.bfloat16)

    def prepare_down():
        count = wd_ref.shape[1]
        across = lax.broadcasted_iota(jnp.int32, (count, count), 1)
        diagonal = (lax.broadcasted_iota(jnp.int32, (count, count), 0) == across).astype(
            jnp.float32
        ).astype(jnp.bfloat16)
        down_all[sp] = dot_nt(diagonal, wd_ref[...]).astype(jnp.bfloat16)

    preparing = [functools.partial(prepare_queries, head) for head in range(head_count)]
    preparing.append(prepare_down)
    pl.semaphore_wait(barrier, 2 + n_tp - 1)

    def origin(hop, direction):
        if direction == 0:
            return ring_device((place + n_sp - hop) % n_sp, n_sp)
        return ring_device((place + hop) % n_sp, n_sp)

    def lat_copy(hop, direction):
        block = lat_all.at[origin(hop - 1, direction), core * 2 + direction]
        return pltpu.make_async_remote_copy(
            src_ref=block,
            dst_ref=block,
            send_sem=lat_send.at[direction],
            recv_sem=lat_recv.at[direction, hop - 1],
            device_id={"sp": targets[direction]},
            device_id_type=MESH,
        )

    def lat_arrival(hop, direction):
        block = lat_all.at[origin(hop, direction), core * 2 + direction]
        return pltpu.make_async_remote_copy(
            src_ref=block,
            dst_ref=block,
            send_sem=lat_send.at[direction],
            recv_sem=lat_recv.at[direction, hop - 1],
            device_id={"sp": targets[direction]},
            device_id_type=MESH,
        )

    def share_copy(hop, direction, which):
        block = lat_all.at[origin(hop, direction), which * 2 + direction]
        return pltpu.make_async_remote_copy(
            src_ref=block,
            dst_ref=block,
            send_sem=share_send.at[direction],
            recv_sem=share_recv.at[direction, hop - 1],
            device_id={"tp": partner},
            device_id_type=MESH,
        )

    piece_rows = wg_ref.shape[0] // (2 * splits)

    def ring_copy(array, piece, hop, direction, arriving):
        block = origin(hop if arriving else hop - 1, direction)
        rows = pl.ds((direction * splits + piece) * piece_rows, piece_rows)
        ref = weights[array].at[block, rows]
        return pltpu.make_async_remote_copy(
            src_ref=ref,
            dst_ref=ref,
            send_sem=ring_send.at[array, piece, direction],
            recv_sem=ring_recv.at[array, piece, direction, hop - 1],
            device_id={"sp": targets[direction]},
            device_id_type=MESH,
        )

    started = set()

    def ring_step(array, piece, hop):
        if hop == 1 and array < 2 and array not in started:
            own[array].wait()
            started.add(array)
        for direction in range(2):
            if hop > 1:
                ring_copy(array, piece, hop - 1, direction, True).wait_recv()
                ring_copy(array, piece, hop - 1, direction, False).wait_send()
            if hop < n_sp:
                ring_copy(array, piece, hop, direction, False).start()

    first = [
        (array, piece, hop)
        for hop in range(1, n_sp)
        for array in range(2)
        for piece in range(splits)
    ]
    second = [(2, piece, hop) for hop in range(1, n_sp) for piece in range(splits)]
    queue = [first + second, 0]

    def advance(count):
        steps, at = queue
        for step in steps[at : at + count]:
            ring_step(*step)
        queue[1] = min(at + count, len(steps))

    unit = max(1, len(first) // 28)

    lat_own.wait()
    for hop in range(1, n_sp + 1):
        for direction in range(2):
            if hop > 1:
                lat_arrival(hop - 1, direction).wait_recv()
                lat_copy(hop - 1, direction).wait_send()
            if hop < n_sp:
                lat_copy(hop, direction).start()
            if hop > 2:
                share_copy(hop - 2, direction, core).wait_send()
            if hop > 1:
                share_copy(hop - 1, direction, core).start()
        if hop < n_sp and queue[1] < 7 * unit:
            advance(1)
        if preparing:
            preparing.pop(0)()
    while preparing:
        preparing.pop(0)()
    for direction in range(2):
        share_copy(n_sp - 1, direction, core).wait_send()
        for hop in range(1, n_sp):
            share_copy(hop, direction, 1 - core).wait_recv()

    total_rows = n_sp * n_rows
    lat_wide = lat_all.shape[3]
    chunk_blocks = max(1, min(n_sp, 1536 // n_rows))
    chunks = n_sp // chunk_blocks
    chunk = chunk_blocks * n_rows
    half_blocks = max(1, chunk_blocks // 2)

    def project(step):
        rows = half_blocks * n_rows
        blocks = pl.ds(step * half_blocks, half_blocks)
        lat = lat_all[blocks, :, :, pl.ds(0, rank)].reshape(rows, rank)
        rotary[pl.ds(step * rows, rows)] = lat_all[blocks, :, :, pl.ds(rank, LANES)].reshape(
            rows, LANES
        )
        keys[pl.ds(step * rows, rows)] = dot(lat, wk_ref[...]).astype(jnp.bfloat16)
        values[pl.ds(step * rows, rows)] = dot(lat, wv_ref[...]).astype(jnp.bfloat16)

    if chunks == 1:
        for step in range(n_sp // half_blocks):
            project(step)
            advance(unit)
    else:
        pl.loop(0, n_sp // half_blocks)(project)
        advance(2 * unit)

    score_scale = (NOPE + ROPE) ** (-0.5)
    lane = lax.broadcasted_iota(jnp.int32, (n_rows, LANES), 1)

    def attend(head, at, state):
        maxima, totals, running = state
        rows = pl.ds(at * chunk, chunk)
        pair = slice(head // 2 * LANES, (head // 2 + 1) * LANES)
        whole_keys = jnp.concatenate([keys[rows, pair], rotary[rows]], axis=1)
        scores = dot_nt(q_all[head], whole_keys) * score_scale
        top = jnp.max(scores, axis=1, keepdims=True)
        if maxima is not None:
            top = jnp.maximum(maxima, top)
        probs = jnp.exp(scores - top)
        sums = jnp.sum(probs, axis=1, keepdims=True)
        update = dot(probs.astype(jnp.bfloat16), values[rows, pair])
        if maxima is not None:
            factor = jnp.exp(maxima - top)
            sums = totals * factor + sums
            update = running * factor + update
        return (top, sums, update)

    for head in range(head_count):
        state = attend(head, 0, (None, None, None))
        if chunks > 1:
            state = lax.fori_loop(1, chunks, functools.partial(attend_loop, attend, head), state)
        result = state[2] / state[1]
        pair = slice(head // 2 * LANES, (head // 2 + 1) * LANES)
        if head % 2 == 0:
            heads[:, pair] = result.astype(jnp.bfloat16)
        else:
            heads[:, pair] = jnp.where(
                lane < VDIM, heads[:, pair].astype(jnp.float32), result
            ).astype(jnp.bfloat16)
        advance(unit)

    def tp_copy(stage, slot_source, slot_target, to, slot_semaphore):
        return pltpu.make_async_remote_copy(
            src_ref=slot_source,
            dst_ref=slot_target,
            send_sem=tp_send.at[stage, slot_semaphore],
            recv_sem=tp_recv.at[stage, slot_semaphore],
            device_id={"tp": to},
            device_id_type=MESH,
        )

    def exchange(stage, source_of, target_of):
        copies = []
        for k in range(1, n_tp):
            to = (tp + k) % n_tp
            copies.append(tp_copy(stage, source_of(to), target_of(k), to, k))
        return copies

    copies = exchange(0, lambda to: part_send.at[to], lambda k: part_recv.at[k])
    for k in range(1, n_tp + 1):
        to = (tp + k) % n_tp
        part_send[to] = dot(
            heads[...], wo_ref[:, pl.ds(pl.multiple_of(to * n_cols, LANES), n_cols)]
        ).astype(jnp.bfloat16)
        if k < n_tp:
            copies[k - 1].start()
    advance(4 * unit)
    mixed = DEEP_ALPHA * resid_ref[...].astype(jnp.float32) + part_send[tp].astype(jnp.float32)
    for k in range(1, n_tp):
        copies[k - 1].wait_recv()
        mixed = mixed + part_recv[k].astype(jnp.float32)
    pending = list(copies)

    width_total = n_cols * n_tp

    def normed(rows_in, gain_ref, stage, send, recv, between):
        sums = jnp.sum(rows_in, axis=1, keepdims=True)
        squares = jnp.sum(rows_in * rows_in, axis=1, keepdims=True)
        mine = jnp.transpose(jnp.where(lane < 4, sums, squares))[:8]
        send[...] = mine
        copies = exchange(stage, lambda to: send, lambda k: recv.at[k])
        for copy in copies:
            copy.start()
        between()
        for k in range(1, n_tp):
            copies[k - 1].wait_recv()
            mine = mine + recv[k]
        pending.extend(copies)
        whole = jnp.transpose(mine) / width_total
        row_mean = whole[:, :1]
        variance = whole[:, 4:5] - row_mean * row_mean
        return (
            (rows_in - row_mean) * lax.rsqrt(variance + NORM_EPSILON) * gain_ref[...]
        ).astype(jnp.bfloat16)

    hidden_in = normed(
        mixed, gain_mix_ref, 1, stat_send, stat_recv, lambda: advance(2 * unit)
    )
    rows_all[tp] = hidden_in
    copies = exchange(2, lambda to: rows_all.at[tp], lambda k: rows_all.at[tp])
    for copy in copies:
        copy.start()
    pending.extend(copies)
    advance(4 * unit)
    for k in range(1, n_tp):
        sender = (tp + n_tp - k) % n_tp
        tp_copy(2, rows_all.at[sender], rows_all.at[sender], sender, k).wait_recv()

    advance(len(first) - queue[1])
    advance(splits)

    def last_hop(array):
        for piece in range(splits):
            for direction in range(2):
                ring_copy(array, piece, n_sp - 1, direction, True).wait_recv()
                ring_copy(array, piece, n_sp - 1, direction, False).wait_send()

    last_hop(0)
    group = n_sp // n_tp
    depth = group * wg_ref.shape[0]
    hidden_width = wg_ref.shape[1]

    def wide(weight):
        total = None
        for t in range(n_tp):
            term = dot(
                rows_all[t],
                weight[t * group : (t + 1) * group].reshape(depth, hidden_width),
            )
            total = term if total is None else total + term
            advance(1)
        return total

    gate_sum = wide(gate_all)
    last_hop(1)
    up_sum = wide(up_all)
    hidden = (gate_sum / (1.0 + jnp.exp(-gate_sum)) * up_sum).astype(jnp.bfloat16)
    advance(1)

    half_rows = piece_rows * splits
    if half_rows % LANES == 0:
        hid[...] = hidden

        def down_copy(k, slot, to, columns):
            ref = part2_send.at[to, :, columns]
            return pltpu.make_async_remote_copy(
                src_ref=ref,
                dst_ref=part2_recv.at[k, :, columns],
                send_sem=down_send.at[k, slot],
                recv_sem=down_recv.at[k, slot],
                device_id={"tp": to},
                device_id_type=MESH,
            )

        def slot_columns(slot):
            return pl.ds(pl.multiple_of(slot * half_rows, LANES), half_rows)

        def make_columns(hop):
            for direction in range(2):
                block = origin(hop, direction)
                owner = block // group
                slot = (block % group) * 2 + direction
                rows = pl.ds(direction * half_rows, half_rows)
                part2_send[owner, :, slot_columns(slot)] = dot_nt(
                    hid[...], down_all[block, rows]
                ).astype(jnp.bfloat16)

                @pl.when(owner != tp)
                def send_away():
                    down_copy((owner + n_tp - tp) % n_tp, slot, owner, slot_columns(slot)).start()

        made = 0
        while queue[1] < len(queue[0]):
            array, piece, hop = queue[0][queue[1]]
            advance(1)
            if piece == splits - 1:
                made_to = hop
                while made < made_to:
                    make_columns(made)
                    made += 1
        while made < n_sp - 1:
            make_columns(made)
            made += 1
        last_hop(2)
        make_columns(n_sp - 1)
        mixer = part2_send[tp].astype(jnp.float32)
        for k in range(1, n_tp):
            for slot in range(2 * group):
                down_copy(k, slot, (tp + k) % n_tp, slot_columns(slot)).wait_recv()
            mixer = mixer + part2_recv[k].astype(jnp.float32)
    else:
        advance(len(queue[0]))
        last_hop(2)
        copies = exchange(3, lambda to: part2_send.at[to], lambda k: part2_recv.at[k])
        for k in range(1, n_tp + 1):
            to = (tp + k) % n_tp
            part2_send[to] = dot_nt(
                hidden, down_all[pl.ds(to * group, group)].reshape(depth, hidden_width)
            ).astype(jnp.bfloat16)
            if k < n_tp:
                copies[k - 1].start()
        mixer = part2_send[tp].astype(jnp.float32)
        for k in range(1, n_tp):
            copies[k - 1].wait_recv()
            mixer = mixer + part2_recv[k].astype(jnp.float32)
        pending.extend(copies)
    final = DEEP_ALPHA * rows_all[tp].astype(jnp.float32) + HALF_STEP * mixer
    out_ref[...] = normed(final, gain_out_ref, 4, stat2_send, stat2_recv, lambda: None)
    for copy in pending:
        copy.wait_send()
    if half_rows % LANES == 0:
        for k in range(1, n_tp):
            for slot in range(2 * group):
                down_copy(k, slot, (tp + k) % n_tp, slot_columns(slot)).wait_send()


def attend_loop(attend, head, at, state):
    return attend(head, at, state)


def flip(value, mask):
    result = value
    bit = 1
    while bit <= mask:
        if mask & bit:
            result = result + bit - 2 * bit * ((value // bit) % 2)
        bit *= 2
    return result


class Semaphores:
    def __init__(self, refs):
        self.refs, self.base, self.used = refs, {}, 0

    def at(self, name, count=1, index=0):
        if name not in self.base:
            self.base[name] = self.used
            self.used += count
        return self.refs.at[self.base[name] + index]


def paired_kernel(
    n_sp,
    n_tp,
    pieces,
    q_in,
    lat_ref,
    rope_in,
    wk_in,
    wv_in,
    wo_ref,
    resid_in,
    gain_mix_in,
    gain_out_in,
    wg_ref,
    wu_ref,
    wd_ref,
    out_ref,
    q_ref,
    rope_ref,
    wk_ref,
    wv_ref,
    resid_ref,
    gain_mix_ref,
    gain_out_ref,
    lat_all,
    keys,
    rotary,
    values,
    q_all,
    heads_all,
    wo_all,
    wide_all,
    down_own,
    down_all,
    rows_all,
    hid,
    summed,
    core_send,
    core_recv,
    far_send,
    far_recv,
    pair_send,
    pair_recv,
    stat_send,
    stat_recv,
    local_sem,
    remote_sem,
):
    sp = lax.axis_index("sp")
    tp = lax.axis_index("tp")
    n_hi = n_sp // 2
    z, x = sp // 2, sp % 2
    half = z % 2
    edge = half == (z // 2) % 2
    inner = jnp.logical_not(edge)
    n_rows = q_ref.shape[0]
    head_count = wk_ref.shape[1] // NOPE
    rank = wk_ref.shape[0]
    lat_rows = lat_all.shape[2]
    n_cols = out_ref.shape[1]
    group = n_sp // n_tp
    depth = wg_ref.shape[0]
    width = wg_ref.shape[1] // 2
    piece_cols = wd_ref.shape[1] // pieces
    local_sems = Semaphores(local_sem)
    remote_sems = Semaphores(remote_sem)

    order = [(1, flip(z, 1))]
    for m in range(2, n_hi, 2):
        low, high = flip(z, m), flip(z, m + 1)
        order.append((jnp.where(edge, m, m + 1), jnp.where(edge, low, high)))
        order.append((jnp.where(edge, m + 1, m), jnp.where(edge, high, low)))
    near, rest = list(range(1, len(order), 2)), list(range(2, len(order), 2))

    def sp_of(place, side):
        return 2 * place + side

    def remote(source, target, device, sent, name, count=1, index=0):
        return pltpu.make_async_remote_copy(
            src_ref=source,
            dst_ref=target,
            send_sem=remote_sems.at(("sent", sent)),
            recv_sem=remote_sems.at(name, count, index),
            device_id=device,
            device_id_type=MESH,
        )

    other_x = 1 - x
    partner, across, corner = flip(tp, 1), flip(tp, 2), flip(tp, 3)
    to_x = {"sp": sp_of(z, other_x)}
    to_pair = {"sp": sp_of(flip(z, 1), x)}
    to_core = {"tp": partner}
    to_across = {"tp": across}

    barrier = pltpu.get_barrier_semaphore()
    peers = [{"sp": sp_of(flip(z, k), x)} for k in range(1, n_hi)] + [to_x]
    peers += [{"tp": flip(tp, j)} for j in range(1, n_tp)]
    for device in peers:
        pl.semaphore_signal(barrier, inc=1, device_id=device, device_id_type=MESH)

    def local(source, target, name):
        return pltpu.make_async_copy(source, target, local_sems.at(name))

    inputs = {
        "rope": local(rope_in, rope_ref, "rope"),
        "q": local(q_in, q_ref, "q"),
        "wk": local(wk_in, wk_ref, "wk"),
        "wv": local(wv_in, wv_ref, "wv"),
        "resid": local(resid_in, resid_ref, "resid"),
        "mix": local(gain_mix_in, gain_mix_ref, "mix"),
        "out": local(gain_out_in, gain_out_ref, "out"),
    }

    wide_rows = depth // pieces

    def wide_source(array, which, piece):
        columns = pl.ds(pl.multiple_of(which * width, LANES), width)
        return (wg_ref, wu_ref)[array].at[pl.ds(piece * wide_rows, wide_rows), columns]

    def wide_block(array, place, side, piece):
        rows = pl.ds(piece * wide_rows, wide_rows)
        return wide_all.at[sp_of(place, side), rows, pl.ds(array * width, width)]

    def down_rows(which, piece):
        rows = pl.ds(pl.multiple_of(which * width, 16), width)
        return wd_ref.at[rows, pl.ds(piece * piece_cols, piece_cols)]

    def down_block(place, side, piece):
        return down_all.at[place * pieces + piece, side]

    def weight_source(array, which, piece):
        if array == 2:
            return down_own.at[which, piece]
        return wide_source(array, which, piece)

    def weight_block(array, place, side, piece):
        if array == 2:
            return down_block(place, side, piece)
        return wide_block(array, place, side, piece)

    def sent_of(array):
        return "down" if array == 2 else "wide"

    def weight_out(array, k, piece):
        place = flip(z, k)
        remote(
            weight_source(array, place % 2, piece),
            weight_block(array, z, x, piece),
            {"sp": sp_of(place, x)},
            sent_of(array),
            ("wz", array, piece),
            n_hi - 1,
            k - 1,
        ).start()

    def weight_side(array, k, place, piece, source=None):
        block = weight_block(array, place, x, piece)
        name = ("wx", piece) if array == 2 else "wx"
        count, index = (n_hi, k) if array == 2 else (1, 0)
        source = block if source is None else source
        remote(source, block, to_x, sent_of(array), name, count, index).start()

    def weight_own(array, piece):
        weight_side(array, 0, z, piece, weight_source(array, half, piece))

    def relay(array, at, piece):
        k, place = order[at]
        block = weight_block(array, place, x, piece)
        remote(
            block, block, to_x, sent_of(array), ("wz", array, piece), n_hi - 1, k - 1
        ).wait_recv()
        weight_side(array, k, place, piece)

    def relay_all(array, at):
        for piece in range(pieces):
            relay(array, at, piece)

    lat_own = local(lat_ref, lat_all.at[sp, :, :, pl.ds(0, rank)], "lat")
    inputs["rope"].start()
    lat_own.start()
    for name in ("q", "wk", "wv", "resid", "mix", "out"):
        inputs[name].start()
    staged = []
    for piece in range(pieces):
        for which in range(2):
            name = ("staged", which, piece)
            staged.append(local(down_rows(which, piece), down_own.at[which, piece], name))
            staged[-1].start()
        for array in range(2):
            local(
                weight_source(array, half, piece), weight_block(array, z, x, piece), "wide"
            ).start()
    down_mine = []
    for piece in range(pieces):
        down_mine.append(
            local(down_rows(half, piece), down_block(z, x, piece), ("down", piece))
        )
        down_mine[-1].start()

    def wo_columns(which):
        return wo_ref.at[:, pl.ds(pl.multiple_of(which * n_cols, LANES), n_cols)]

    wo_own = local(wo_columns(tp), wo_all.at[tp], "wo")
    wo_own.start()
    cosine, sine = rotary_tables(sp * n_rows, n_rows)
    inputs["rope"].wait()
    turned_in = jnp.concatenate(
        [rope_ref[...].astype(jnp.float32), jnp.zeros((LANES - ROPE, n_rows), jnp.float32)],
        axis=0,
    )
    key_rot = rotate(jnp.transpose(turned_in)[:, :ROPE], cosine, sine)
    key_rot.append(jnp.zeros((n_rows, LANES - ROPE), jnp.float32))
    lat_all[sp, :, :, pl.ds(rank, LANES)] = (
        jnp.concatenate(key_rot, axis=1).astype(jnp.bfloat16).reshape(n_tp, lat_rows, LANES)
    )

    def prepare_queries(head):
        base = head * (NOPE + ROPE)
        wide_q = q_ref[...].astype(jnp.float32)
        nope = wide_q[:, base : base + NOPE]
        other = jnp.zeros((n_rows, NOPE), jnp.float32)
        turned = rotate(wide_q[:, base + NOPE : base + NOPE + ROPE], cosine, sine)
        parts = [nope, other] if head % 2 == 0 else [other, nope]
        parts = parts + turned + [jnp.zeros((n_rows, LANES - ROPE), jnp.float32)]
        q_all[head] = jnp.concatenate(parts, axis=1).astype(jnp.bfloat16)

    pl.semaphore_wait(barrier, len(peers))
    lat_own.wait()
    for copy in staged:
        copy.wait()

    def lat_copy(name, k, place, side, quarter, device):
        block = lat_all.at[sp_of(place, side), quarter]
        return remote(block, block, device, "lat", ("lat", name), n_hi, k)

    def lat_core(place, side, quarter):
        block = lat_all.at[sp_of(place, side), quarter]
        remote(block, block, to_core, "lat", "latc").start()

    def lat_z_in(at):
        k, place = order[at]
        lat_copy("z", k, place, x, tp, to_x).wait_recv()
        lat_copy("x", k, place, x, tp, to_x).start()
        lat_copy("y", k, place, x, tp, to_across).start()
        lat_core(place, x, tp)

    def lat_x_in(at):
        k, place = (0, z) if at is None else order[at]
        lat_copy("x", k, place, other_x, tp, to_x).wait_recv()
        if at is not None:
            lat_copy("yd", k, place, other_x, tp, to_across).start()
        lat_core(place, other_x, tp)

    def lat_y_in(at):
        k, place = order[at]
        lat_copy("y", k, place, x, across, to_across).wait_recv()
        lat_core(place, x, across)

    def lat_yd_in(at):
        k, place = order[at]
        lat_copy("yd", k, place, other_x, across, to_across).wait_recv()
        lat_core(place, other_x, across)

    for k in range(1, n_hi):
        block = lat_all.at[sp, tp]
        remote(
            block, block, {"sp": sp_of(flip(z, k), x)}, "lat", ("lat", "z"), n_hi, k
        ).start()
    lat_copy("x", 0, z, x, tp, to_x).start()
    block = lat_all.at[sp, across]
    remote(block, block, to_x, "lat", ("lat", "xa")).start()
    weight_own(0, 0)

    far = list(range(2, n_hi))

    def send_near(arrays):
        for array in arrays:
            for piece in range(pieces):
                weight_out(array, 1, piece)

    def send_far(array, which):
        for piece in which:
            for k in far:
                weight_out(array, k, piece)

    every = range(pieces)
    early, late = range(pieces // 2), range(pieces // 2, pieces)

    @pl.when(edge)
    def outer_first():
        send_near((0, 1))
        send_far(0, every)
        send_far(1, early)

    inputs["q"].wait()
    prepare_queries(0)
    lat_x_in(None)
    lat_z_in(0)

    @pl.when(inner)
    def inner_first():
        send_near((0, 1, 2))
        send_far(0, every)
        send_far(1, every)

    prepare_queries(1)
    block = lat_all.at[sp_of(z, other_x), across]
    remote(block, block, to_x, "lat", ("lat", "xa")).wait_recv()
    lat_core(z, other_x, across)
    for at in near:
        lat_z_in(at)
    lat_x_in(0)
    lat_y_in(0)
    for at in rest:
        lat_z_in(at)
    for piece in range(1, pieces):
        weight_own(0, piece)
    for piece in range(pieces):
        weight_own(1, piece)
    for head in range(2, head_count):
        prepare_queries(head)
    for at in near:
        lat_x_in(at)
        lat_y_in(at)
    lat_yd_in(0)
    for at in rest:
        lat_x_in(at)
        lat_y_in(at)
    for j in (2, 3, 1):
        to = flip(tp, j)
        remote(wo_columns(to), wo_all.at[tp], {"tp": to}, "wo", "wo").start()
    for at in near + rest:
        lat_yd_in(at)
    relay_all(0, 0)
    whole = lat_all.at[pl.ds(0, n_sp - 1), pl.ds(0, 2)]
    remote(whole, whole, to_core, "lat", "latc").wait_recv()

    half_blocks = n_sp // 2

    def project(step):
        rows = half_blocks * n_rows
        blocks = pl.ds(step * half_blocks, half_blocks)
        lat = lat_all[blocks, :, :, pl.ds(0, rank)].reshape(rows, rank)
        rotary[pl.ds(step * rows, rows)] = lat_all[blocks, :, :, pl.ds(rank, LANES)].reshape(
            rows, LANES
        )
        keys[pl.ds(step * rows, rows)] = dot(lat, wk_ref[...]).astype(jnp.bfloat16)
        values[pl.ds(step * rows, rows)] = dot(lat, wv_ref[...]).astype(jnp.bfloat16)

    inputs["wk"].wait()
    inputs["wv"].wait()
    for step in range(n_sp // half_blocks):
        project(step)

    score_scale = (NOPE + ROPE) ** (-0.5)
    lane = lax.broadcasted_iota(jnp.int32, (n_rows, LANES), 1)

    for head in range(head_count):
        pair = slice(head // 2 * LANES, (head // 2 + 1) * LANES)
        whole_keys = jnp.concatenate([keys[:, pair], rotary[...]], axis=1)
        scores = dot_nt(q_all[head], whole_keys) * score_scale
        top = jnp.max(scores, axis=1, keepdims=True)
        probs = jnp.exp(scores - top)
        sums = jnp.sum(probs, axis=1, keepdims=True)
        result = dot(probs.astype(jnp.bfloat16), values[:, pair]) / sums
        if head % 2 == 0:
            held = result
        else:
            heads_all[tp, :, pair] = jnp.where(lane < VDIM, held, result).astype(jnp.bfloat16)
            block = heads_all.at[tp, :, pl.ds(head // 2 * LANES, LANES)]
            for j in (2, 3, 1):
                remote(block, block, {"tp": flip(tp, j)}, "heads", "heads").start()
        if head == head_count // 2 - 1:
            relay_all(1, 0)
        if head == head_count // 2:
            for at in near:
                relay_all(0, at)

    for at in rest:
        relay_all(0, at)
    for name in ("resid", "mix", "out"):
        inputs[name].wait()
    mixed = DEEP_ALPHA * resid_ref[...].astype(jnp.float32)
    wo_own.wait()
    mixed = mixed + dot(heads_all[tp], wo_all[tp])
    others = pl.ds(0, n_tp - 1)
    remote(wo_all.at[others], wo_all.at[others], to_core, "wo", "wo").wait_recv()
    remote(heads_all.at[others], heads_all.at[others], to_core, "heads", "heads").wait_recv()
    for j in (1, 2, 3):
        sender = flip(tp, j)
        mixed = mixed + dot(heads_all[sender], wo_all[sender])

    width_total = n_cols * n_tp

    def normed(rows_in, gain_ref, stage, between):
        sums = jnp.sum(rows_in, axis=1, keepdims=True)
        squares = jnp.sum(rows_in * rows_in, axis=1, keepdims=True)
        mine = jnp.transpose(jnp.where(lane < 4, sums, squares))[:8]
        stat_send[stage] = mine
        for j in (2, 3, 1):
            remote(
                stat_send.at[stage],
                stat_recv.at[stage, j - 1],
                {"tp": flip(tp, j)},
                ("stat", stage),
                ("stat", stage),
            ).start()
        between()
        arrived = stat_recv.at[stage]
        remote(arrived, arrived, to_core, ("stat", stage), ("stat", stage)).wait_recv()
        for j in (1, 2, 3):
            mine = mine + stat_recv[stage, j - 1]
        whole = jnp.transpose(mine) / width_total
        row_mean = whole[:, :1]
        variance = whole[:, 4:5] - row_mean * row_mean
        return (
            (rows_in - row_mean) * lax.rsqrt(variance + NORM_EPSILON) * gain_ref[...]
        ).astype(jnp.bfloat16)

    def more_down():
        for piece in range(pieces):
            weight_own(2, piece)

    hidden_in = normed(mixed, gain_mix_ref, 0, more_down)
    mine = pl.ds(pl.multiple_of(half * n_rows, 16), n_rows)
    theirs = pl.ds(pl.multiple_of((1 - half) * n_rows, 16), n_rows)
    rows_all[tp, mine] = hidden_in

    def rows_copy(name, owner, rows, device):
        block = rows_all.at[owner, rows]
        return remote(block, block, device, "rows", ("rows", name))

    def rows_core(owner, rows):
        block = rows_all.at[owner, rows]
        remote(block, block, to_core, "rowsc", "rowsc").start()

    rows_copy("y", tp, mine, to_across).start()
    rows_copy("z", tp, mine, to_pair).start()
    rows_core(tp, mine)

    @pl.when(edge)
    def outer_last():
        send_far(1, late)
        send_near((2,))
        send_far(2, every)

    @pl.when(inner)
    def inner_last():
        send_far(2, every)

    for at in near:
        relay_all(1, at)
    rows_copy("z", tp, theirs, to_pair).wait_recv()
    rows_copy("yz", tp, theirs, to_across).start()
    rows_core(tp, theirs)
    rows_copy("y", across, mine, to_across).wait_recv()
    rows_core(across, mine)
    rows_copy("yz", across, theirs, to_across).wait_recv()
    rows_core(across, theirs)
    for at in rest:
        relay_all(1, at)
    for at in near:
        relay_all(2, at)
    both = rows_all.at[pl.ds(0, 2)]
    remote(both, both, to_core, "rowsc", "rowsc").wait_recv()
    local(wg_ref, wide_all.at[0], "wide").wait()
    arrived = wide_all.at[pl.ds(0, n_hi)]
    remote(arrived, arrived, to_x, "wide", "wx").wait_recv()

    total = None
    for t in range(n_tp):
        term = dot(
            rows_all[t], wide_all[t * group : (t + 1) * group].reshape(group * depth, 2 * width)
        )
        total = term if total is None else total + term
    gate_sum, up_sum = total[:, :width], total[:, width:]
    hid[...] = (gate_sum / (1.0 + jnp.exp(-gate_sum)) * up_sum).astype(jnp.bfloat16)
    for copy in down_mine:
        copy.wait()

    steps = [(None, piece) for piece in range(pieces)] + [(0, piece) for piece in range(pieces)]
    for first, second in zip(near, rest):
        steps += [(first, piece) for piece in range(pieces)]
        steps += [(second, piece) for piece in range(pieces)]

    def facts(at, piece):
        k, place = (0, z) if at is None else order[at]
        unit = place * pieces + piece
        return k, place, unit, tp % 2 == place % 2, tp // 2 == place // 2

    def core_copy(place, unit, piece):
        return remote(
            core_send.at[unit],
            core_recv.at[unit],
            to_core,
            "core",
            "core",
            n_tp // 2 * pieces,
            place // 2 * pieces + piece,
        )

    def far_copy(piece):
        return remote(
            far_send.at[piece], far_recv.at[piece], to_across, "far", "far", pieces, piece
        )

    def pair_copy(piece):
        return remote(
            pair_send.at[piece], pair_recv.at[piece], to_pair, "pair", "pair", pieces, piece
        )

    def make_block(at, piece):
        k, place, unit, same_core, same_chip = facts(at, piece)
        block = down_block(place, other_x, piece)
        remote(block, block, to_x, "down", ("wx", piece), n_hi, k).wait_recv()
        columns = jnp.concatenate([down_all[unit, 0], down_all[unit, 1]], axis=1)
        product = dot(hid[...], columns)

        @pl.when(same_core)
        def keep():
            summed[unit] = product

        @pl.when(jnp.logical_not(same_core))
        def give():
            core_send[unit] = product.astype(jnp.bfloat16)
            core_copy(place, unit, piece).start()

    def add_core(at, piece):
        k, place, unit, same_core, same_chip = facts(at, piece)

        @pl.when(same_core)
        def add():
            core_copy(place, unit, piece).wait_recv()
            both = summed[unit] + core_recv[unit].astype(jnp.float32)

            @pl.when(same_chip)
            def keep():
                summed[unit] = both

            @pl.when(jnp.logical_not(same_chip))
            def give():
                far_send[piece] = both.astype(jnp.bfloat16)
                far_copy(piece).start()

    def add_far(at, piece):
        k, place, unit, same_core, same_chip = facts(at, piece)

        @pl.when(place == tp)
        def add():
            far_copy(piece).wait_recv()
            summed[unit, mine] = summed[unit, mine] + far_recv[piece, mine].astype(jnp.float32)
            pair_send[piece] = (
                summed[unit, theirs] + far_recv[piece, theirs].astype(jnp.float32)
            ).astype(jnp.bfloat16)
            pair_copy(piece).start()

    for at in [0] + rest:
        relay_all(2, at)
    ready = [step for step in steps if step[0] not in rest]
    waiting = [step for step in steps if step[0] in rest]
    for step in ready:
        make_block(*step)
    for step in ready:
        add_core(*step)
    for step in waiting:
        make_block(*step)
    for step in waiting:
        add_core(*step)
    for step in ready + waiting:
        add_far(*step)

    final = []
    for piece in range(pieces):
        pair_copy(piece).wait_recv()
        final.append(summed[tp * pieces + piece, mine] + pair_recv[piece].astype(jnp.float32))
    sides = []
    for side in range(2):
        for piece in range(pieces):
            sides.append(final[piece][:, side * piece_cols : (side + 1) * piece_cols])
    mixer = jnp.concatenate(sides, axis=1)
    last_in = DEEP_ALPHA * rows_all[tp, mine].astype(jnp.float32) + HALF_STEP * mixer
    out_ref[...] = normed(last_in, gain_out_ref, 1, lambda: None)

    def all_sent(sent, name, whole):
        remote(whole, whole, to_core, sent, name).wait_send()

    all_sent("lat", "latc", lat_all.at[pl.ds(0, n_sp - 1)])
    all_sent("wide", "wx", wide_all.at[pl.ds(0, n_sp - 1)])
    all_sent("down", "wx", down_all.at[pl.ds(0, (n_sp - 1) * pieces // 2)])
    all_sent("wo", "wo", wo_all.at[others])
    all_sent("heads", "heads", heads_all.at[others])
    all_sent("rows", ("rows", "z"), rows_all.at[others, pl.ds(0, n_rows)])
    all_sent("rowsc", "rowsc", both)
    for stage in range(2):
        all_sent(("stat", stage), ("stat", stage), stat_recv.at[stage])
    all_sent("core", "core", core_send.at[pl.ds(0, n_hi * pieces // 2)])
    all_sent("far", "far", far_send)
    all_sent("pair", "pair", pair_send)


def paired_call(n_sp, n_tp, operands):
    queries, latents, rope_key, w_key, w_value, w_out, resid, gain_mix = operands[:8]
    w_gate, w_up, w_down, gain_out = operands[8:]
    rows = queries.shape[0]
    head_count = w_key.shape[1] // NOPE
    rank = latents.shape[1]
    cols = resid.shape[1]
    depth, hidden_width = w_gate.shape
    width = hidden_width // 2
    pieces = 2
    n_hi = n_sp // 2
    unit_cols = 2 * w_down.shape[1] // pieces
    total_rows = n_sp * rows
    bf16 = jnp.bfloat16
    f32 = jnp.float32
    vmem = pl.BlockSpec(memory_space=pltpu.VMEM)
    anywhere = pl.BlockSpec(memory_space=pl.ANY)
    dma = pltpu.SemaphoreType.DMA
    signals = 18 + 5 * n_hi + 2 * (n_hi - 1) * pieces + (2 * n_hi - 1) * pieces + 11
    signals += (n_tp // 2 + 2) * pieces + 4
    return pl.pallas_call(
        functools.partial(paired_kernel, n_sp, n_tp, pieces),
        out_shape=jax.ShapeDtypeStruct((rows, cols), bf16),
        in_specs=[anywhere] * 12,
        out_specs=vmem,
        scratch_shapes=[
            pltpu.VMEM(queries.shape, bf16),
            pltpu.VMEM((rope_key.shape[1], rows), bf16),
            pltpu.VMEM(w_key.shape, bf16),
            pltpu.VMEM(w_value.shape, bf16),
            pltpu.VMEM(resid.shape, bf16),
            pltpu.VMEM((1, cols), f32),
            pltpu.VMEM((1, cols), f32),
            pltpu.VMEM((n_sp, n_tp, rows // n_tp, rank + LANES), bf16),
            pltpu.VMEM((total_rows, head_count * NOPE), bf16),
            pltpu.VMEM((total_rows, LANES), bf16),
            pltpu.VMEM((total_rows, head_count * VDIM), bf16),
            pltpu.VMEM((head_count, rows, 2 * LANES), bf16),
            pltpu.VMEM((n_tp, rows, head_count * VDIM), bf16),
            pltpu.VMEM((n_tp, head_count * VDIM, cols), bf16),
            pltpu.VMEM((n_sp, depth, 2 * width), bf16),
            pltpu.VMEM((2, pieces, width, unit_cols // 2), bf16),
            pltpu.VMEM((n_hi * pieces, 2, width, unit_cols // 2), bf16),
            pltpu.VMEM((n_tp, 2 * rows, cols), bf16),
            pltpu.VMEM((2 * rows, width), bf16),
            pltpu.VMEM((n_hi * pieces, 2 * rows, unit_cols), f32),
            pltpu.VMEM((n_hi * pieces, 2 * rows, unit_cols), bf16),
            pltpu.VMEM((n_hi * pieces, 2 * rows, unit_cols), bf16),
            pltpu.VMEM((pieces, 2 * rows, unit_cols), bf16),
            pltpu.VMEM((pieces, 2 * rows, unit_cols), bf16),
            pltpu.VMEM((pieces, rows, unit_cols), bf16),
            pltpu.VMEM((pieces, rows, unit_cols), bf16),
            pltpu.VMEM((2, 8, rows), f32),
            pltpu.VMEM((2, n_tp - 1, 8, rows), f32),
            dma((10 + 3 * pieces,)),
            dma((signals,)),
        ],
        compiler_params=pltpu.CompilerParams(
            collective_id=1, has_side_effects=True, vmem_limit_bytes=66000000
        ),
    )(
        queries,
        latents.reshape(n_tp, rows // n_tp, rank),
        rope_key.T,
        w_key,
        w_value,
        w_out,
        resid,
        gain_mix.reshape(1, -1),
        gain_out.reshape(1, -1),
        w_gate,
        w_up,
        w_down,
    )


def fits_pairs(n_sp, n_tp, operands):
    queries, w_key, w_gate, w_down = operands[0], operands[3], operands[8], operands[10]
    return (
        n_tp == 4
        and n_sp == 2 * n_tp
        and queries.shape[0] % 64 == 0
        and n_sp * queries.shape[0] <= 1536
        and (w_key.shape[1] // NOPE) % 2 == 0
        and w_gate.shape[1] % (2 * LANES) == 0
        and w_gate.shape[0] % 32 == 0
        and w_down.shape[1] % (2 * LANES) == 0
    )


def local(
    queries,
    latents,
    rope_key,
    w_key,
    w_value,
    w_out,
    resid,
    gain_mix,
    w_gate,
    w_up,
    w_down,
    gain_out,
):
    n_sp = lax.axis_size("sp")
    n_tp = lax.axis_size("tp")
    operands = (queries, latents, rope_key, w_key, w_value, w_out, resid, gain_mix)
    operands += (w_gate, w_up, w_down, gain_out)
    if fits_pairs(n_sp, n_tp, operands):
        return paired_call(n_sp, n_tp, operands)
    rows = queries.shape[0]
    head_count = w_key.shape[1] // NOPE
    rank = latents.shape[1]
    cols = resid.shape[1]
    hidden_width = w_gate.shape[1]
    weight_rows = w_gate.shape[0]
    lat_wide = rank + LANES
    splits = 2 if weight_rows % 64 == 0 else 1
    bf16 = jnp.bfloat16
    total_rows = n_sp * rows
    vmem = pl.BlockSpec(memory_space=pltpu.VMEM)
    anywhere = pl.BlockSpec(memory_space=pl.ANY)
    dma = pltpu.SemaphoreType.DMA
    return pl.pallas_call(
        functools.partial(layer_kernel, n_sp, n_tp, splits),
        out_shape=jax.ShapeDtypeStruct((rows, cols), bf16),
        in_specs=[vmem, anywhere] + [vmem] * 7 + [anywhere] * 2 + [vmem],
        out_specs=vmem,
        scratch_shapes=[
            pltpu.VMEM((n_sp, 4, rows // 4, lat_wide), bf16),
            pltpu.VMEM((total_rows, head_count * NOPE), bf16),
            pltpu.VMEM((total_rows, LANES), bf16),
            pltpu.VMEM((total_rows, head_count * VDIM), bf16),
            pltpu.VMEM((n_sp, weight_rows, hidden_width), bf16),
            pltpu.VMEM((n_sp, weight_rows, hidden_width), bf16),
            pltpu.VMEM((n_sp, weight_rows, hidden_width), bf16),
            pltpu.VMEM((head_count, rows, 2 * LANES), bf16),
            pltpu.VMEM((rows, head_count * VDIM), bf16),
            pltpu.VMEM((n_tp, rows, cols), bf16),
            pltpu.VMEM((n_tp, rows, cols), bf16),
            pltpu.VMEM((8, rows), jnp.float32),
            pltpu.VMEM((n_tp, 8, rows), jnp.float32),
            pltpu.VMEM((n_tp, rows, cols), bf16),
            pltpu.VMEM((n_tp, rows, cols), bf16),
            pltpu.VMEM((n_tp, rows, cols), bf16),
            pltpu.VMEM((8, rows), jnp.float32),
            pltpu.VMEM((n_tp, 8, rows), jnp.float32),
            pltpu.VMEM((rows, hidden_width), bf16),
            dma((4,)),
            dma((2,)),
            dma((2, n_sp - 1)),
            dma((2,)),
            dma((2, n_sp - 1)),
            dma((3, splits, 2)),
            dma((3, splits, 2, n_sp - 1)),
            dma((5, n_tp)),
            dma((5, n_tp)),
            dma((n_tp, 2 * (n_sp // n_tp))),
            dma((n_tp, 2 * (n_sp // n_tp))),
        ],
        compiler_params=pltpu.CompilerParams(
            collective_id=0, has_side_effects=True, vmem_limit_bytes=66000000
        ),
    )(
        queries,
        latents.reshape(4, rows // 4, rank),
        rope_key,
        w_key,
        w_value,
        w_out,
        resid,
        gain_mix.reshape(1, -1),
        gain_out.reshape(1, -1),
        w_gate,
        w_up,
        w_down,
    )


def solution(mesh):
    placed = (
        P("sp", "tp"),
        P("sp", None),
        P("sp", None),
        P(None, "tp"),
        P(None, "tp"),
        P("tp", None),
        P("sp", "tp"),
        P("tp"),
        P("sp", "tp"),
        P("sp", "tp"),
        P("tp", "sp"),
        P("tp"),
    )
    return jax.shard_map(
        local, mesh=mesh, in_specs=placed, out_specs=P("sp", "tp"), check_vma=False
    )
```

```python
import functools

import jax
import jax.numpy as jnp
from jax import lax
from jax.experimental import pallas as pl
from jax.experimental.pallas import tpu as pltpu
from jax.sharding import PartitionSpec as P

NOPE = 64
ROPE = 32
VDIM = 64
GRID_W = 64
LANES = 128

ROTARY_BASE = 10000.0
NORM_EPSILON = 1e-06
DEEP_ALPHA = 8.0**0.25
HALF_STEP = 0.5
MESH = pl.DeviceIdType.MESH


def rotary_tables(first, rows):
    at = first + lax.broadcasted_iota(jnp.int32, (rows, LANES), 0)
    column = lax.broadcasted_iota(jnp.int32, (rows, LANES), 1)
    freq_count = ROPE // 4
    grid_row = (at // GRID_W).astype(jnp.float32)
    grid_col = (at % GRID_W).astype(jnp.float32)
    spot = jnp.where(column % (2 * freq_count) < freq_count, grid_row, grid_col)
    inverse = jnp.ones((rows, LANES), jnp.float32)
    for k in range(1, freq_count):
        inverse = jnp.where(column % freq_count == k, ROTARY_BASE ** (-k / freq_count), inverse)
    angles = spot * inverse
    return (jnp.cos(angles)[:, : ROPE // 2], jnp.sin(angles)[:, : ROPE // 2])


def rotate(vectors, cosine, sine):
    half_width = ROPE // 2
    leading = vectors[:, :half_width]
    trailing = vectors[:, half_width:]
    return [leading * cosine - trailing * sine, leading * sine + trailing * cosine]


def ring_device(place, count):
    return jnp.where(place < count // 2, 2 * place, 2 * (count - 1 - place) + 1)


def ring_place(index, count):
    return jnp.where(index % 2 == 0, index // 2, count - 1 - index // 2)


def dot(left, right):
    return jnp.dot(left, right, preferred_element_type=jnp.float32)


def dot_nt(left, right):
    return lax.dot_general(
        left, right, (((1,), (1,)), ((), ())), preferred_element_type=jnp.float32
    )


def layer_kernel(
    n_sp,
    n_tp,
    splits,
    q_ref,
    lat_ref,
    rope_ref,
    wk_ref,
    wv_ref,
    wo_ref,
    resid_ref,
    gain_mix_ref,
    gain_out_ref,
    wg_ref,
    wu_ref,
    wd_ref,
    out_ref,
    lat_all,
    keys,
    rotary,
    values,
    gate_all,
    up_all,
    down_all,
    q_all,
    heads,
    part_send,
    part_recv,
    stat_send,
    stat_recv,
    rows_all,
    part2_send,
    part2_recv,
    stat2_send,
    stat2_recv,
    hid,
    local_sem,
    lat_send,
    lat_recv,
    share_send,
    share_recv,
    ring_send,
    ring_recv,
    tp_send,
    tp_recv,
    down_send,
    down_recv,
):
    sp = lax.axis_index("sp")
    tp = lax.axis_index("tp")
    place = ring_place(sp, n_sp)
    ahead = ring_device((place + 1) % n_sp, n_sp)
    behind = ring_device((place + n_sp - 1) % n_sp, n_sp)
    targets = (ahead, behind)
    partner = tp + 1 - 2 * (tp % 2)
    core = tp % 2
    n_rows = q_ref.shape[0]
    head_count = wk_ref.shape[1] // NOPE
    rank = wk_ref.shape[0]
    lat_rows = lat_all.shape[2]
    n_cols = out_ref.shape[1]

    barrier = pltpu.get_barrier_semaphore()
    for device in targets:
        pl.semaphore_signal(barrier, inc=1, device_id={"sp": device}, device_id_type=MESH)
    for step in range(1, n_tp):
        pl.semaphore_signal(
            barrier, inc=1, device_id={"tp": (tp + step) % n_tp}, device_id_type=MESH
        )

    own = []
    lat_own = pltpu.make_async_copy(
        lat_ref, lat_all.at[sp, :, :, pl.ds(0, rank)], local_sem.at[0]
    )
    lat_own.start()
    weights = (gate_all, up_all, down_all)
    for i, source in enumerate((wg_ref, wu_ref)):
        copy = pltpu.make_async_copy(source, weights[i].at[sp], local_sem.at[i + 1])
        copy.start()
        own.append(copy)
    cosine, sine = rotary_tables(sp * n_rows, n_rows)
    key_rot = rotate(rope_ref[...].astype(jnp.float32), cosine, sine)
    key_rot.append(jnp.zeros((n_rows, LANES - ROPE), jnp.float32))
    lat_all[sp, :, :, pl.ds(rank, LANES)] = (
        jnp.concatenate(key_rot, axis=1).astype(jnp.bfloat16).reshape(4, lat_rows, LANES)
    )

    def prepare_queries(head):
        base = head * (NOPE + ROPE)
        wide_q = q_ref[...].astype(jnp.float32)
        nope = wide_q[:, base : base + NOPE]
        other = jnp.zeros((n_rows, NOPE), jnp.float32)
        rotary = rotate(wide_q[:, base + NOPE : base + NOPE + ROPE], cosine, sine)
        parts = [nope, other] if head % 2 == 0 else [other, nope]
        parts = parts + rotary + [jnp.zeros((n_rows, LANES - ROPE), jnp.float32)]
        q_all[head] = jnp.concatenate(parts, axis=1).astype(jnp.bfloat16)

    def prepare_down():
        count = wd_ref.shape[1]
        across = lax.broadcasted_iota(jnp.int32, (count, count), 1)
        diagonal = (lax.broadcasted_iota(jnp.int32, (count, count), 0) == across).astype(
            jnp.float32
        ).astype(jnp.bfloat16)
        down_all[sp] = dot_nt(diagonal, wd_ref[...]).astype(jnp.bfloat16)

    preparing = [functools.partial(prepare_queries, head) for head in range(head_count)]
    preparing.append(prepare_down)
    pl.semaphore_wait(barrier, 2 + n_tp - 1)

    def origin(hop, direction):
        if direction == 0:
            return ring_device((place + n_sp - hop) % n_sp, n_sp)
        return ring_device((place + hop) % n_sp, n_sp)

    def lat_copy(hop, direction):
        block = lat_all.at[origin(hop - 1, direction), core * 2 + direction]
        return pltpu.make_async_remote_copy(
            src_ref=block,
            dst_ref=block,
            send_sem=lat_send.at[direction],
            recv_sem=lat_recv.at[direction, hop - 1],
            device_id={"sp": targets[direction]},
            device_id_type=MESH,
        )

    def lat_arrival(hop, direction):
        block = lat_all.at[origin(hop, direction), core * 2 + direction]
        return pltpu.make_async_remote_copy(
            src_ref=block,
            dst_ref=block,
            send_sem=lat_send.at[direction],
            recv_sem=lat_recv.at[direction, hop - 1],
            device_id={"sp": targets[direction]},
            device_id_type=MESH,
        )

    def share_copy(hop, direction, which):
        block = lat_all.at[origin(hop, direction), which * 2 + direction]
        return pltpu.make_async_remote_copy(
            src_ref=block,
            dst_ref=block,
            send_sem=share_send.at[direction],
            recv_sem=share_recv.at[direction, hop - 1],
            device_id={"tp": partner},
            device_id_type=MESH,
        )

    piece_rows = wg_ref.shape[0] // (2 * splits)

    def ring_copy(array, piece, hop, direction, arriving):
        block = origin(hop if arriving else hop - 1, direction)
        rows = pl.ds((direction * splits + piece) * piece_rows, piece_rows)
        ref = weights[array].at[block, rows]
        return pltpu.make_async_remote_copy(
            src_ref=ref,
            dst_ref=ref,
            send_sem=ring_send.at[array, piece, direction],
            recv_sem=ring_recv.at[array, piece, direction, hop - 1],
            device_id={"sp": targets[direction]},
            device_id_type=MESH,
        )

    started = set()

    def ring_step(array, piece, hop):
        if hop == 1 and array < 2 and array not in started:
            own[array].wait()
            started.add(array)
        for direction in range(2):
            if hop > 1:
                ring_copy(array, piece, hop - 1, direction, True).wait_recv()
                ring_copy(array, piece, hop - 1, direction, False).wait_send()
            if hop < n_sp:
                ring_copy(array, piece, hop, direction, False).start()

    first = [
        (array, piece, hop)
        for hop in range(1, n_sp)
        for array in range(2)
        for piece in range(splits)
    ]
    second = [(2, piece, hop) for hop in range(1, n_sp) for piece in range(splits)]
    queue = [first + second, 0]

    def advance(count):
        steps, at = queue
        for step in steps[at : at + count]:
            ring_step(*step)
        queue[1] = min(at + count, len(steps))

    unit = max(1, len(first) // 28)

    lat_own.wait()
    for hop in range(1, n_sp + 1):
        for direction in range(2):
            if hop > 1:
                lat_arrival(hop - 1, direction).wait_recv()
                lat_copy(hop - 1, direction).wait_send()
            if hop < n_sp:
                lat_copy(hop, direction).start()
            if hop > 2:
                share_copy(hop - 2, direction, core).wait_send()
            if hop > 1:
                share_copy(hop - 1, direction, core).start()
        if hop < n_sp and queue[1] < 7 * unit:
            advance(1)
        if preparing:
            preparing.pop(0)()
    while preparing:
        preparing.pop(0)()
    for direction in range(2):
        share_copy(n_sp - 1, direction, core).wait_send()
        for hop in range(1, n_sp):
            share_copy(hop, direction, 1 - core).wait_recv()

    total_rows = n_sp * n_rows
    lat_wide = lat_all.shape[3]
    chunk_blocks = max(1, min(n_sp, 1536 // n_rows))
    chunks = n_sp // chunk_blocks
    chunk = chunk_blocks * n_rows
    half_blocks = max(1, chunk_blocks // 2)

    def project(step):
        rows = half_blocks * n_rows
        blocks = pl.ds(step * half_blocks, half_blocks)
        lat = lat_all[blocks, :, :, pl.ds(0, rank)].reshape(rows, rank)
        rotary[pl.ds(step * rows, rows)] = lat_all[blocks, :, :, pl.ds(rank, LANES)].reshape(
            rows, LANES
        )
        keys[pl.ds(step * rows, rows)] = dot(lat, wk_ref[...]).astype(jnp.bfloat16)
        values[pl.ds(step * rows, rows)] = dot(lat, wv_ref[...]).astype(jnp.bfloat16)

    if chunks == 1:
        for step in range(n_sp // half_blocks):
            project(step)
            advance(unit)
    else:
        pl.loop(0, n_sp // half_blocks)(project)
        advance(2 * unit)

    score_scale = (NOPE + ROPE) ** (-0.5)
    lane = lax.broadcasted_iota(jnp.int32, (n_rows, LANES), 1)

    def attend(head, at, state):
        maxima, totals, running = state
        rows = pl.ds(at * chunk, chunk)
        pair = slice(head // 2 * LANES, (head // 2 + 1) * LANES)
        whole_keys = jnp.concatenate([keys[rows, pair], rotary[rows]], axis=1)
        scores = dot_nt(q_all[head], whole_keys) * score_scale
        top = jnp.max(scores, axis=1, keepdims=True)
        if maxima is not None:
            top = jnp.maximum(maxima, top)
        probs = jnp.exp(scores - top)
        sums = jnp.sum(probs, axis=1, keepdims=True)
        update = dot(probs.astype(jnp.bfloat16), values[rows, pair])
        if maxima is not None:
            factor = jnp.exp(maxima - top)
            sums = totals * factor + sums
            update = running * factor + update
        return (top, sums, update)

    for head in range(head_count):
        state = attend(head, 0, (None, None, None))
        if chunks > 1:
            state = lax.fori_loop(1, chunks, functools.partial(attend_loop, attend, head), state)
        result = state[2] / state[1]
        pair = slice(head // 2 * LANES, (head // 2 + 1) * LANES)
        if head % 2 == 0:
            heads[:, pair] = result.astype(jnp.bfloat16)
        else:
            heads[:, pair] = jnp.where(
                lane < VDIM, heads[:, pair].astype(jnp.float32), result
            ).astype(jnp.bfloat16)
        advance(unit)

    def tp_copy(stage, slot_source, slot_target, to, slot_semaphore):
        return pltpu.make_async_remote_copy(
            src_ref=slot_source,
            dst_ref=slot_target,
            send_sem=tp_send.at[stage, slot_semaphore],
            recv_sem=tp_recv.at[stage, slot_semaphore],
            device_id={"tp": to},
            device_id_type=MESH,
        )

    def exchange(stage, source_of, target_of):
        copies = []
        for k in range(1, n_tp):
            to = (tp + k) % n_tp
            copies.append(tp_copy(stage, source_of(to), target_of(k), to, k))
        return copies

    copies = exchange(0, lambda to: part_send.at[to], lambda k: part_recv.at[k])
    for k in range(1, n_tp + 1):
        to = (tp + k) % n_tp
        part_send[to] = dot(
            heads[...], wo_ref[:, pl.ds(pl.multiple_of(to * n_cols, LANES), n_cols)]
        ).astype(jnp.bfloat16)
        if k < n_tp:
            copies[k - 1].start()
    advance(4 * unit)
    mixed = DEEP_ALPHA * resid_ref[...].astype(jnp.float32) + part_send[tp].astype(jnp.float32)
    for k in range(1, n_tp):
        copies[k - 1].wait_recv()
        mixed = mixed + part_recv[k].astype(jnp.float32)
    pending = list(copies)

    width_total = n_cols * n_tp

    def normed(rows_in, gain_ref, stage, send, recv, between):
        sums = jnp.sum(rows_in, axis=1, keepdims=True)
        squares = jnp.sum(rows_in * rows_in, axis=1, keepdims=True)
        mine = jnp.transpose(jnp.where(lane < 4, sums, squares))[:8]
        send[...] = mine
        copies = exchange(stage, lambda to: send, lambda k: recv.at[k])
        for copy in copies:
            copy.start()
        between()
        for k in range(1, n_tp):
            copies[k - 1].wait_recv()
            mine = mine + recv[k]
        pending.extend(copies)
        whole = jnp.transpose(mine) / width_total
        row_mean = whole[:, :1]
        variance = whole[:, 4:5] - row_mean * row_mean
        return (
            (rows_in - row_mean) * lax.rsqrt(variance + NORM_EPSILON) * gain_ref[...]
        ).astype(jnp.bfloat16)

    hidden_in = normed(
        mixed, gain_mix_ref, 1, stat_send, stat_recv, lambda: advance(2 * unit)
    )
    rows_all[tp] = hidden_in
    copies = exchange(2, lambda to: rows_all.at[tp], lambda k: rows_all.at[tp])
    for copy in copies:
        copy.start()
    pending.extend(copies)
    advance(4 * unit)
    for k in range(1, n_tp):
        sender = (tp + n_tp - k) % n_tp
        tp_copy(2, rows_all.at[sender], rows_all.at[sender], sender, k).wait_recv()

    advance(len(first) - queue[1])
    advance(splits)

    def last_hop(array):
        for piece in range(splits):
            for direction in range(2):
                ring_copy(array, piece, n_sp - 1, direction, True).wait_recv()
                ring_copy(array, piece, n_sp - 1, direction, False).wait_send()

    last_hop(0)
    group = n_sp // n_tp
    depth = group * wg_ref.shape[0]
    hidden_width = wg_ref.shape[1]

    def wide(weight):
        total = None
        for t in range(n_tp):
            term = dot(
                rows_all[t],
                weight[t * group : (t + 1) * group].reshape(depth, hidden_width),
            )
            total = term if total is None else total + term
            advance(1)
        return total

    gate_sum = wide(gate_all)
    last_hop(1)
    up_sum = wide(up_all)
    hidden = (gate_sum / (1.0 + jnp.exp(-gate_sum)) * up_sum).astype(jnp.bfloat16)
    advance(1)

    half_rows = piece_rows * splits
    if half_rows % LANES == 0:
        hid[...] = hidden

        def down_copy(k, slot, to, columns):
            ref = part2_send.at[to, :, columns]
            return pltpu.make_async_remote_copy(
                src_ref=ref,
                dst_ref=part2_recv.at[k, :, columns],
                send_sem=down_send.at[k, slot],
                recv_sem=down_recv.at[k, slot],
                device_id={"tp": to},
                device_id_type=MESH,
            )

        def slot_columns(slot):
            return pl.ds(pl.multiple_of(slot * half_rows, LANES), half_rows)

        def make_columns(hop):
            for direction in range(2):
                block = origin(hop, direction)
                owner = block // group
                slot = (block % group) * 2 + direction
                rows = pl.ds(direction * half_rows, half_rows)
                part2_send[owner, :, slot_columns(slot)] = dot_nt(
                    hid[...], down_all[block, rows]
                ).astype(jnp.bfloat16)

                @pl.when(owner != tp)
                def send_away():
                    down_copy((owner + n_tp - tp) % n_tp, slot, owner, slot_columns(slot)).start()

        made = 0
        while queue[1] < len(queue[0]):
            array, piece, hop = queue[0][queue[1]]
            advance(1)
            if piece == splits - 1:
                made_to = hop
                while made < made_to:
                    make_columns(made)
                    made += 1
        while made < n_sp - 1:
            make_columns(made)
            made += 1
        last_hop(2)
        make_columns(n_sp - 1)
        mixer = part2_send[tp].astype(jnp.float32)
        for k in range(1, n_tp):
            for slot in range(2 * group):
                down_copy(k, slot, (tp + k) % n_tp, slot_columns(slot)).wait_recv()
            mixer = mixer + part2_recv[k].astype(jnp.float32)
    else:
        advance(len(queue[0]))
        last_hop(2)
        copies = exchange(3, lambda to: part2_send.at[to], lambda k: part2_recv.at[k])
        for k in range(1, n_tp + 1):
            to = (tp + k) % n_tp
            part2_send[to] = dot_nt(
                hidden, down_all[pl.ds(to * group, group)].reshape(depth, hidden_width)
            ).astype(jnp.bfloat16)
            if k < n_tp:
                copies[k - 1].start()
        mixer = part2_send[tp].astype(jnp.float32)
        for k in range(1, n_tp):
            copies[k - 1].wait_recv()
            mixer = mixer + part2_recv[k].astype(jnp.float32)
        pending.extend(copies)
    final = DEEP_ALPHA * rows_all[tp].astype(jnp.float32) + HALF_STEP * mixer
    out_ref[...] = normed(final, gain_out_ref, 4, stat2_send, stat2_recv, lambda: None)
    for copy in pending:
        copy.wait_send()
    if half_rows % LANES == 0:
        for k in range(1, n_tp):
            for slot in range(2 * group):
                down_copy(k, slot, (tp + k) % n_tp, slot_columns(slot)).wait_send()


def attend_loop(attend, head, at, state):
    return attend(head, at, state)


def flip(value, mask):
    result = value
    bit = 1
    while bit <= mask:
        if mask & bit:
            result = result + bit - 2 * bit * ((value // bit) % 2)
        bit *= 2
    return result


class Semaphores:
    def __init__(self, refs):
        self.refs, self.base, self.used = refs, {}, 0

    def at(self, name, count=1, index=0):
        if name not in self.base:
            self.base[name] = self.used
            self.used += count
        return self.refs.at[self.base[name] + index]


def paired_kernel(
    n_sp,
    n_tp,
    pieces,
    q_in,
    lat_ref,
    rope_in,
    wk_in,
    wv_in,
    wo_ref,
    resid_in,
    gain_mix_in,
    gain_out_in,
    wg_ref,
    wu_ref,
    wd_ref,
    out_ref,
    q_ref,
    rope_ref,
    wk_ref,
    wv_ref,
    resid_ref,
    gain_mix_ref,
    gain_out_ref,
    lat_all,
    keys,
    rotary,
    values,
    q_all,
    heads_all,
    wo_all,
    wide_all,
    down_own,
    down_all,
    rows_all,
    hid,
    summed,
    core_send,
    core_recv,
    far_send,
    far_recv,
    pair_send,
    pair_recv,
    first_send,
    first_recv,
    last_send,
    last_recv,
    total_sum,
    stat_send,
    stat_recv,
    local_sem,
    remote_sem,
):
    sp = lax.axis_index("sp")
    tp = lax.axis_index("tp")
    n_hi = n_sp // 2
    z, x = sp // 2, sp % 2
    half = z % 2
    edge = half == (z // 2) % 2
    inner = jnp.logical_not(edge)
    n_rows = q_ref.shape[0]
    head_count = wk_ref.shape[1] // NOPE
    rank = wk_ref.shape[0]
    lat_rows = lat_all.shape[2]
    n_cols = out_ref.shape[1]
    group = n_sp // n_tp
    depth = wg_ref.shape[0]
    width = wg_ref.shape[1] // 2
    piece_cols = wd_ref.shape[1] // pieces
    local_sems = Semaphores(local_sem)
    remote_sems = Semaphores(remote_sem)

    order = [(1, flip(z, 1))]
    for m in range(2, n_hi, 2):
        low, high = flip(z, m), flip(z, m + 1)
        order.append((jnp.where(edge, m, m + 1), jnp.where(edge, low, high)))
        order.append((jnp.where(edge, m + 1, m), jnp.where(edge, high, low)))
    near, rest = list(range(1, len(order), 2)), list(range(2, len(order), 2))

    def sp_of(place, side):
        return 2 * place + side

    def remote(source, target, device, sent, name, count=1, index=0):
        return pltpu.make_async_remote_copy(
            src_ref=source,
            dst_ref=target,
            send_sem=remote_sems.at(("sent", sent)),
            recv_sem=remote_sems.at(name, count, index),
            device_id=device,
            device_id_type=MESH,
        )

    other_x = 1 - x
    partner, across, corner = flip(tp, 1), flip(tp, 2), flip(tp, 3)
    to_x = {"sp": sp_of(z, other_x)}
    to_pair = {"sp": sp_of(flip(z, 1), x)}
    to_core = {"tp": partner}
    to_across = {"tp": across}

    barrier = pltpu.get_barrier_semaphore()
    peers = [{"sp": sp_of(flip(z, k), x)} for k in range(1, n_hi)] + [to_x]
    peers += [{"tp": flip(tp, j)} for j in range(1, n_tp)]
    for device in peers:
        pl.semaphore_signal(barrier, inc=1, device_id=device, device_id_type=MESH)

    def local(source, target, name):
        return pltpu.make_async_copy(source, target, local_sems.at(name))

    inputs = {
        "rope": local(rope_in, rope_ref, "rope"),
        "q": local(q_in, q_ref, "q"),
        "wk": local(wk_in, wk_ref, "wk"),
        "wv": local(wv_in, wv_ref, "wv"),
        "resid": local(resid_in, resid_ref, "resid"),
        "mix": local(gain_mix_in, gain_mix_ref, "mix"),
        "out": local(gain_out_in, gain_out_ref, "out"),
    }

    wide_rows = depth // pieces

    def wide_source(array, which, piece):
        columns = pl.ds(pl.multiple_of(which * width, LANES), width)
        return (wg_ref, wu_ref)[array].at[pl.ds(piece * wide_rows, wide_rows), columns]

    def wide_block(array, place, side, piece):
        rows = pl.ds(piece * wide_rows, wide_rows)
        return wide_all.at[sp_of(place, side), rows, pl.ds(array * width, width)]

    def down_rows(which, piece):
        rows = pl.ds(pl.multiple_of(which * width, 16), width)
        return wd_ref.at[rows, pl.ds(piece * piece_cols, piece_cols)]

    def down_block(place, side, piece):
        return down_all.at[place * pieces + piece, side]

    def weight_source(array, which, piece):
        if array == 2:
            return down_own.at[which, piece]
        return wide_source(array, which, piece)

    def weight_block(array, place, side, piece):
        if array == 2:
            return down_block(place, side, piece)
        return wide_block(array, place, side, piece)

    def sent_of(array):
        return "down" if array == 2 else "wide"

    def weight_out(array, k, piece):
        place = flip(z, k)
        remote(
            weight_source(array, place % 2, piece),
            weight_block(array, z, x, piece),
            {"sp": sp_of(place, x)},
            sent_of(array),
            ("wz", array, piece),
            n_hi - 1,
            k - 1,
        ).start()

    def weight_side(array, k, place, piece, source=None):
        block = weight_block(array, place, x, piece)
        name = ("wx", piece) if array == 2 else "wx"
        count, index = (n_hi, k) if array == 2 else (1, 0)
        source = block if source is None else source
        remote(source, block, to_x, sent_of(array), name, count, index).start()

    def weight_own(array, piece):
        weight_side(array, 0, z, piece, weight_source(array, half, piece))

    def relay(array, at, piece):
        k, place = order[at]
        block = weight_block(array, place, x, piece)
        remote(
            block, block, to_x, sent_of(array), ("wz", array, piece), n_hi - 1, k - 1
        ).wait_recv()
        weight_side(array, k, place, piece)

    def relay_all(array, at):
        for piece in range(pieces):
            relay(array, at, piece)

    lat_own = local(lat_ref, lat_all.at[sp, :, :, pl.ds(0, rank)], "lat")
    inputs["rope"].start()
    lat_own.start()
    for name in ("q", "wk", "wv", "resid", "mix", "out"):
        inputs[name].start()
    staged = []
    for piece in range(pieces):
        for which in range(2):
            name = ("staged", which, piece)
            staged.append(local(down_rows(which, piece), down_own.at[which, piece], name))
            staged[-1].start()
        for array in range(2):
            local(
                weight_source(array, half, piece), weight_block(array, z, x, piece), "wide"
            ).start()
    down_mine = []
    for piece in range(pieces):
        down_mine.append(
            local(down_rows(half, piece), down_block(z, x, piece), ("down", piece))
        )
        down_mine[-1].start()

    def wo_columns(which):
        return wo_ref.at[:, pl.ds(pl.multiple_of(which * n_cols, LANES), n_cols)]

    wo_own = local(wo_columns(tp), wo_all.at[tp], "wo")
    wo_own.start()
    cosine, sine = rotary_tables(sp * n_rows, n_rows)
    inputs["rope"].wait()
    turned_in = jnp.concatenate(
        [rope_ref[...].astype(jnp.float32), jnp.zeros((LANES - ROPE, n_rows), jnp.float32)],
        axis=0,
    )
    key_rot = rotate(jnp.transpose(turned_in)[:, :ROPE], cosine, sine)
    key_rot.append(jnp.zeros((n_rows, LANES - ROPE), jnp.float32))
    lat_all[sp, :, :, pl.ds(rank, LANES)] = (
        jnp.concatenate(key_rot, axis=1).astype(jnp.bfloat16).reshape(n_tp, lat_rows, LANES)
    )

    def prepare_queries(head):
        base = head * (NOPE + ROPE)
        wide_q = q_ref[...].astype(jnp.float32)
        nope = wide_q[:, base : base + NOPE]
        other = jnp.zeros((n_rows, NOPE), jnp.float32)
        turned = rotate(wide_q[:, base + NOPE : base + NOPE + ROPE], cosine, sine)
        parts = [nope, other] if head % 2 == 0 else [other, nope]
        parts = parts + turned + [jnp.zeros((n_rows, LANES - ROPE), jnp.float32)]
        q_all[head] = jnp.concatenate(parts, axis=1).astype(jnp.bfloat16)

    pl.semaphore_wait(barrier, len(peers))
    lat_own.wait()
    for copy in staged:
        copy.wait()

    def lat_copy(name, k, place, side, quarter, device):
        block = lat_all.at[sp_of(place, side), quarter]
        return remote(block, block, device, "lat", ("lat", name), n_hi, k)

    def lat_core(place, side, quarter):
        block = lat_all.at[sp_of(place, side), quarter]
        remote(block, block, to_core, "lat", "latc").start()

    def lat_z_in(at):
        k, place = order[at]
        lat_copy("z", k, place, x, tp, to_x).wait_recv()
        lat_copy("x", k, place, x, tp, to_x).start()
        lat_copy("y", k, place, x, tp, to_across).start()
        lat_core(place, x, tp)

    def lat_x_in(at):
        k, place = (0, z) if at is None else order[at]
        lat_copy("x", k, place, other_x, tp, to_x).wait_recv()
        if at is not None:
            lat_copy("yd", k, place, other_x, tp, to_across).start()
        lat_core(place, other_x, tp)

    def lat_y_in(at):
        k, place = order[at]
        lat_copy("y", k, place, x, across, to_across).wait_recv()
        lat_core(place, x, across)

    def lat_yd_in(at):
        k, place = order[at]
        lat_copy("yd", k, place, other_x, across, to_across).wait_recv()
        lat_core(place, other_x, across)

    for k in range(1, n_hi):
        block = lat_all.at[sp, tp]
        remote(
            block, block, {"sp": sp_of(flip(z, k), x)}, "lat", ("lat", "z"), n_hi, k
        ).start()
    lat_copy("x", 0, z, x, tp, to_x).start()
    block = lat_all.at[sp, across]
    remote(block, block, to_x, "lat", ("lat", "xa")).start()
    weight_own(0, 0)

    far = list(range(2, n_hi))

    def send_near(arrays):
        for array in arrays:
            for piece in range(pieces):
                weight_out(array, 1, piece)

    def send_far(array, which):
        for piece in which:
            for k in far:
                weight_out(array, k, piece)

    every = range(pieces)
    early, late = range(pieces // 2), range(pieces // 2, pieces)

    @pl.when(edge)
    def outer_first():
        send_near((0, 1))
        send_far(0, every)
        send_far(1, early)

    @pl.when(inner)
    def inner_first():
        send_near((0, 1, 2))
        send_far(0, every)
        send_far(1, every)

    inputs["q"].wait()
    prepare_queries(0)
    lat_x_in(None)
    lat_z_in(0)

    prepare_queries(1)
    block = lat_all.at[sp_of(z, other_x), across]
    remote(block, block, to_x, "lat", ("lat", "xa")).wait_recv()
    lat_core(z, other_x, across)
    for at in near:
        lat_z_in(at)
    lat_x_in(0)
    lat_y_in(0)
    for at in rest:
        lat_z_in(at)
    for piece in range(1, pieces):
        weight_own(0, piece)
    for piece in range(pieces):
        weight_own(1, piece)
    for piece in range(pieces):
        weight_own(2, piece)
    for head in range(2, head_count):
        prepare_queries(head)
    for at in near:
        lat_x_in(at)
        lat_y_in(at)
    lat_yd_in(0)
    for at in rest:
        lat_x_in(at)
        lat_y_in(at)
    for j in (2, 3, 1):
        to = flip(tp, j)
        remote(wo_columns(to), wo_all.at[tp], {"tp": to}, "wo", "wo").start()
    for at in near + rest:
        lat_yd_in(at)
    relay_all(0, 0)
    whole = lat_all.at[pl.ds(0, n_sp - 1), pl.ds(0, 2)]
    remote(whole, whole, to_core, "lat", "latc").wait_recv()

    half_blocks = n_sp // 2

    def project(step):
        rows = half_blocks * n_rows
        blocks = pl.ds(step * half_blocks, half_blocks)
        lat = lat_all[blocks, :, :, pl.ds(0, rank)].reshape(rows, rank)
        rotary[pl.ds(step * rows, rows)] = lat_all[blocks, :, :, pl.ds(rank, LANES)].reshape(
            rows, LANES
        )
        keys[pl.ds(step * rows, rows)] = dot(lat, wk_ref[...]).astype(jnp.bfloat16)
        values[pl.ds(step * rows, rows)] = dot(lat, wv_ref[...]).astype(jnp.bfloat16)

    inputs["wk"].wait()
    inputs["wv"].wait()
    for step in range(n_sp // half_blocks):
        project(step)

    score_scale = (NOPE + ROPE) ** (-0.5)
    lane = lax.broadcasted_iota(jnp.int32, (n_rows, LANES), 1)

    for head in range(head_count):
        pair = slice(head // 2 * LANES, (head // 2 + 1) * LANES)
        whole_keys = jnp.concatenate([keys[:, pair], rotary[...]], axis=1)
        scores = dot_nt(q_all[head], whole_keys) * score_scale
        top = jnp.max(scores, axis=1, keepdims=True)
        probs = jnp.exp(scores - top)
        sums = jnp.sum(probs, axis=1, keepdims=True)
        result = dot(probs.astype(jnp.bfloat16), values[:, pair]) / sums
        if head % 2 == 0:
            held = result
        else:
            heads_all[tp, :, pair] = jnp.where(lane < VDIM, held, result).astype(jnp.bfloat16)
            block = heads_all.at[tp, :, pl.ds(head // 2 * LANES, LANES)]
            for j in (2, 3, 1):
                remote(block, block, {"tp": flip(tp, j)}, "heads", "heads").start()
        if head == head_count // 2 - 1:
            relay_all(1, 0)
    for name in ("resid", "mix", "out"):
        inputs[name].wait()
    mixed = DEEP_ALPHA * resid_ref[...].astype(jnp.float32)
    wo_own.wait()
    mixed = mixed + dot(heads_all[tp], wo_all[tp])
    others = pl.ds(0, n_tp - 1)
    remote(wo_all.at[others], wo_all.at[others], to_core, "wo", "wo").wait_recv()
    remote(heads_all.at[others], heads_all.at[others], to_core, "heads", "heads").wait_recv()
    for j in (1, 2, 3):
        sender = flip(tp, j)
        mixed = mixed + dot(heads_all[sender], wo_all[sender])

    width_total = n_cols * n_tp

    def normed(rows_in, gain_ref, stage, between):
        sums = jnp.sum(rows_in, axis=1, keepdims=True)
        squares = jnp.sum(rows_in * rows_in, axis=1, keepdims=True)
        mine = jnp.transpose(jnp.where(lane < 4, sums, squares))[:8]
        stat_send[stage] = mine
        for j in (2, 3, 1):
            remote(
                stat_send.at[stage],
                stat_recv.at[stage, j - 1],
                {"tp": flip(tp, j)},
                ("stat", stage),
                ("stat", stage),
            ).start()
        between()
        arrived = stat_recv.at[stage]
        remote(arrived, arrived, to_core, ("stat", stage), ("stat", stage)).wait_recv()
        for j in (1, 2, 3):
            mine = mine + stat_recv[stage, j - 1]
        whole = jnp.transpose(mine) / width_total
        row_mean = whole[:, :1]
        variance = whole[:, 4:5] - row_mean * row_mean
        return (
            (rows_in - row_mean) * lax.rsqrt(variance + NORM_EPSILON) * gain_ref[...]
        ).astype(jnp.bfloat16)

    def more_wide():
        for at in near + rest:
            relay_all(0, at)

    hidden_in = normed(mixed, gain_mix_ref, 0, more_wide)
    mine = pl.ds(pl.multiple_of(half * n_rows, 16), n_rows)
    theirs = pl.ds(pl.multiple_of((1 - half) * n_rows, 16), n_rows)
    rows_all[tp, mine] = hidden_in

    def rows_copy(name, owner, rows, device):
        block = rows_all.at[owner, rows]
        return remote(block, block, device, "rows", ("rows", name))

    def rows_core(owner, rows):
        block = rows_all.at[owner, rows]
        remote(block, block, to_core, "rowsc", "rowsc").start()

    rows_copy("y", tp, mine, to_across).start()
    rows_copy("z", tp, mine, to_pair).start()
    rows_core(tp, mine)

    @pl.when(edge)
    def outer_last():
        send_far(1, late)
        send_near((2,))
        send_far(2, every)

    @pl.when(inner)
    def inner_last():
        send_far(2, every)

    for at in near:
        relay_all(1, at)
    for at in rest:
        for piece in early:
            relay(1, at, piece)
    rows_copy("z", tp, theirs, to_pair).wait_recv()
    rows_copy("yz", tp, theirs, to_across).start()
    rows_core(tp, theirs)
    rows_copy("y", across, mine, to_across).wait_recv()
    rows_core(across, mine)
    for at in rest:
        for piece in late:
            relay(1, at, piece)
    rows_copy("yz", across, theirs, to_across).wait_recv()
    rows_core(across, theirs)
    relay_all(2, 0)
    for at in near:
        for piece in early:
            relay(2, at, piece)
    both = rows_all.at[pl.ds(0, 2)]
    remote(both, both, to_core, "rowsc", "rowsc").wait_recv()
    local(wg_ref, wide_all.at[0], "wide").wait()
    arrived = wide_all.at[pl.ds(0, n_hi)]
    remote(arrived, arrived, to_x, "wide", "wx").wait_recv()

    total = None
    for t in range(n_tp):
        term = dot(
            rows_all[t], wide_all[t * group : (t + 1) * group].reshape(group * depth, 2 * width)
        )
        total = term if total is None else total + term
    gate_sum, up_sum = total[:, :width], total[:, width:]
    hid[...] = (gate_sum / (1.0 + jnp.exp(-gate_sum)) * up_sum).astype(jnp.bfloat16)
    for copy in down_mine:
        copy.wait()

    def facts(at, piece):
        k, place = (0, z) if at is None else order[at]
        unit = place * pieces + piece
        return k, place, unit, tp % 2 == place % 2, tp // 2 == place // 2

    def core_copy(place, unit, piece):
        return remote(
            core_send.at[unit],
            core_recv.at[unit],
            to_core,
            "core",
            "core",
            n_tp // 2 * pieces,
            place // 2 * pieces + piece,
        )

    def far_copy(piece):
        return remote(
            far_send.at[piece], far_recv.at[piece], to_across, "far", "far", pieces, piece
        )

    def pair_copy(piece):
        return remote(
            pair_send.at[piece], pair_recv.at[piece], to_pair, "pair", "pair", pieces, piece
        )

    def pair_first_copy(piece):
        source, target = first_send.at[piece], first_recv.at[piece]
        return remote(source, target, to_pair, "first", "first", pieces, piece)

    def far_last_copy(piece):
        source, target = last_send.at[piece], last_recv.at[piece]
        return remote(source, target, to_across, "last", "last", pieces, piece)

    def make_block(at, piece):
        k, place, unit, same_core, same_chip = facts(at, piece)
        block = down_block(place, other_x, piece)
        remote(block, block, to_x, "down", ("wx", piece), n_hi, k).wait_recv()
        columns = jnp.concatenate([down_all[unit, 0], down_all[unit, 1]], axis=1)
        product = dot(hid[...], columns)

        @pl.when(same_core)
        def keep():
            summed[unit] = product

        @pl.when(jnp.logical_not(same_core))
        def give():
            core_send[unit] = product.astype(jnp.bfloat16)
            core_copy(place, unit, piece).start()

    def add_core(at, piece):
        k, place, unit, same_core, same_chip = facts(at, piece)

        @pl.when(same_core)
        def add():
            core_copy(place, unit, piece).wait_recv()
            both = summed[unit] + core_recv[unit].astype(jnp.float32)

            @pl.when(same_chip)
            def keep():
                summed[unit] = both

            @pl.when(jnp.logical_not(same_chip))
            def give():
                far_send[piece] = both.astype(jnp.bfloat16)
                far_copy(piece).start()

    def add_far(at, piece):
        k, place, unit, same_core, same_chip = facts(at, piece)

        @pl.when(place == tp)
        def add():
            far_copy(piece).wait_recv()
            summed[unit, mine] = summed[unit, mine] + far_recv[piece, mine].astype(jnp.float32)
            pair_send[piece] = (
                summed[unit, theirs] + far_recv[piece, theirs].astype(jnp.float32)
            ).astype(jnp.bfloat16)
            pair_copy(piece).start()

    def pair_first(at, piece):
        k, place, unit, same_core, same_chip = facts(at, piece)

        @pl.when(same_core)
        def add():
            core_copy(place, unit, piece).wait_recv()
            first_send[piece] = (
                summed[unit, theirs] + core_recv[unit, theirs].astype(jnp.float32)
            ).astype(jnp.bfloat16)
            pair_first_copy(piece).start()

    def pair_added(at, piece):
        k, place, unit, same_core, same_chip = facts(at, piece)

        @pl.when(same_core)
        def add():
            pair_first_copy(piece).wait_recv()
            both = summed[unit, mine] + core_recv[unit, mine].astype(jnp.float32)
            both = both + first_recv[piece].astype(jnp.float32)

            @pl.when(same_chip)
            def keep():
                total_sum[piece] = both

            @pl.when(jnp.logical_not(same_chip))
            def give():
                last_send[piece] = both.astype(jnp.bfloat16)
                far_last_copy(piece).start()

    def finish_far(at, piece):
        k, place, unit, same_core, same_chip = facts(at, piece)

        @pl.when(place == tp)
        def add():
            far_last_copy(piece).wait_recv()
            total_sum[piece] = total_sum[piece] + last_recv[piece].astype(jnp.float32)

    def finish_pair(at, piece):
        k, place, unit, same_core, same_chip = facts(at, piece)

        @pl.when(place == tp)
        def add():
            pair_copy(piece).wait_recv()
            total_sum[piece] = summed[unit, mine] + pair_recv[piece].astype(jnp.float32)

    def each(apply, ats, which):
        for piece in which:
            for at in ats:
                apply(at, piece)

    close = [None, 0]
    each(make_block, close, every)
    each(functools.partial(relay, 2), rest, early)
    each(add_core, close, every)
    each(make_block, near, early)
    each(functools.partial(relay, 2), rest, late)
    each(make_block, rest, early)
    each(functools.partial(relay, 2), near, late)
    each(pair_first, near + rest, early)
    each(make_block, rest, late)
    each(make_block, near, late)
    each(pair_first, rest + near, late)
    each(add_far, close, every)
    each(pair_added, near + rest, early)
    each(pair_added, rest + near, late)
    each(finish_pair, close, every)
    each(finish_far, near + rest, every)
    final = [total_sum[piece] for piece in range(pieces)]
    sides = []
    for side in range(2):
        for piece in range(pieces):
            sides.append(final[piece][:, side * piece_cols : (side + 1) * piece_cols])
    mixer = jnp.concatenate(sides, axis=1)
    last_in = DEEP_ALPHA * rows_all[tp, mine].astype(jnp.float32) + HALF_STEP * mixer
    out_ref[...] = normed(last_in, gain_out_ref, 1, lambda: None)

    def all_sent(sent, name, whole):
        remote(whole, whole, to_core, sent, name).wait_send()

    all_sent("lat", "latc", lat_all.at[pl.ds(0, n_sp - 1)])
    all_sent("wide", "wx", wide_all.at[pl.ds(0, n_sp - 1)])
    all_sent("down", "wx", down_all.at[pl.ds(0, (n_sp - 1) * pieces // 2)])
    all_sent("wo", "wo", wo_all.at[others])
    all_sent("heads", "heads", heads_all.at[others])
    all_sent("rows", ("rows", "z"), rows_all.at[others, pl.ds(0, n_rows)])
    all_sent("rowsc", "rowsc", both)
    for stage in range(2):
        all_sent(("stat", stage), ("stat", stage), stat_recv.at[stage])
    all_sent("core", "core", core_send.at[pl.ds(0, n_hi * pieces // 2)])
    all_sent("first", "first", first_send)
    home = tp // 2 == z // 2

    @pl.when(home)
    def sent_home():
        all_sent("pair", "pair", pair_send)
        all_sent("last", "last", last_send)

    @pl.when(jnp.logical_not(home))
    def sent_away():
        all_sent("far", "far", far_send)


def paired_call(n_sp, n_tp, operands):
    queries, latents, rope_key, w_key, w_value, w_out, resid, gain_mix = operands[:8]
    w_gate, w_up, w_down, gain_out = operands[8:]
    rows = queries.shape[0]
    head_count = w_key.shape[1] // NOPE
    rank = latents.shape[1]
    cols = resid.shape[1]
    depth, hidden_width = w_gate.shape
    width = hidden_width // 2
    pieces = 2
    n_hi = n_sp // 2
    unit_cols = 2 * w_down.shape[1] // pieces
    total_rows = n_sp * rows
    bf16 = jnp.bfloat16
    f32 = jnp.float32
    vmem = pl.BlockSpec(memory_space=pltpu.VMEM)
    anywhere = pl.BlockSpec(memory_space=pl.ANY)
    dma = pltpu.SemaphoreType.DMA
    signals = 18 + 5 * n_hi + 2 * (n_hi - 1) * pieces + (2 * n_hi - 1) * pieces + 11
    signals += (n_tp // 2 + 4) * pieces + 6
    return pl.pallas_call(
        functools.partial(paired_kernel, n_sp, n_tp, pieces),
        out_shape=jax.ShapeDtypeStruct((rows, cols), bf16),
        in_specs=[anywhere] * 12,
        out_specs=vmem,
        scratch_shapes=[
            pltpu.VMEM(queries.shape, bf16),
            pltpu.VMEM((rope_key.shape[1], rows), bf16),
            pltpu.VMEM(w_key.shape, bf16),
            pltpu.VMEM(w_value.shape, bf16),
            pltpu.VMEM(resid.shape, bf16),
            pltpu.VMEM((1, cols), f32),
            pltpu.VMEM((1, cols), f32),
            pltpu.VMEM((n_sp, n_tp, rows // n_tp, rank + LANES), bf16),
            pltpu.VMEM((total_rows, head_count * NOPE), bf16),
            pltpu.VMEM((total_rows, LANES), bf16),
            pltpu.VMEM((total_rows, head_count * VDIM), bf16),
            pltpu.VMEM((head_count, rows, 2 * LANES), bf16),
            pltpu.VMEM((n_tp, rows, head_count * VDIM), bf16),
            pltpu.VMEM((n_tp, head_count * VDIM, cols), bf16),
            pltpu.VMEM((n_sp, depth, 2 * width), bf16),
            pltpu.VMEM((2, pieces, width, unit_cols // 2), bf16),
            pltpu.VMEM((n_hi * pieces, 2, width, unit_cols // 2), bf16),
            pltpu.VMEM((n_tp, 2 * rows, cols), bf16),
            pltpu.VMEM((2 * rows, width), bf16),
            pltpu.VMEM((n_hi * pieces, 2 * rows, unit_cols), f32),
            pltpu.VMEM((n_hi * pieces, 2 * rows, unit_cols), bf16),
            pltpu.VMEM((n_hi * pieces, 2 * rows, unit_cols), bf16),
            pltpu.VMEM((pieces, 2 * rows, unit_cols), bf16),
            pltpu.VMEM((pieces, 2 * rows, unit_cols), bf16),
            pltpu.VMEM((pieces, rows, unit_cols), bf16),
            pltpu.VMEM((pieces, rows, unit_cols), bf16),
            pltpu.VMEM((pieces, rows, unit_cols), bf16),
            pltpu.VMEM((pieces, rows, unit_cols), bf16),
            pltpu.VMEM((pieces, rows, unit_cols), bf16),
            pltpu.VMEM((pieces, rows, unit_cols), bf16),
            pltpu.VMEM((pieces, rows, unit_cols), f32),
            pltpu.VMEM((2, 8, rows), f32),
            pltpu.VMEM((2, n_tp - 1, 8, rows), f32),
            dma((10 + 3 * pieces,)),
            dma((signals,)),
        ],
        compiler_params=pltpu.CompilerParams(
            collective_id=1, has_side_effects=True, vmem_limit_bytes=66000000
        ),
    )(
        queries,
        latents.reshape(n_tp, rows // n_tp, rank),
        rope_key.T,
        w_key,
        w_value,
        w_out,
        resid,
        gain_mix.reshape(1, -1),
        gain_out.reshape(1, -1),
        w_gate,
        w_up,
        w_down,
    )


def fits_pairs(n_sp, n_tp, operands):
    queries, w_key, w_gate, w_down = operands[0], operands[3], operands[8], operands[10]
    return (
        n_tp == 4
        and n_sp == 2 * n_tp
        and queries.shape[0] % 64 == 0
        and n_sp * queries.shape[0] <= 1536
        and (w_key.shape[1] // NOPE) % 2 == 0
        and w_gate.shape[1] % (2 * LANES) == 0
        and w_gate.shape[0] % 32 == 0
        and w_down.shape[1] % (2 * LANES) == 0
    )


def local(
    queries,
    latents,
    rope_key,
    w_key,
    w_value,
    w_out,
    resid,
    gain_mix,
    w_gate,
    w_up,
    w_down,
    gain_out,
):
    n_sp = lax.axis_size("sp")
    n_tp = lax.axis_size("tp")
    operands = (queries, latents, rope_key, w_key, w_value, w_out, resid, gain_mix)
    operands += (w_gate, w_up, w_down, gain_out)
    if fits_pairs(n_sp, n_tp, operands):
        return paired_call(n_sp, n_tp, operands)
    rows = queries.shape[0]
    head_count = w_key.shape[1] // NOPE
    rank = latents.shape[1]
    cols = resid.shape[1]
    hidden_width = w_gate.shape[1]
    weight_rows = w_gate.shape[0]
    lat_wide = rank + LANES
    splits = 2 if weight_rows % 64 == 0 else 1
    bf16 = jnp.bfloat16
    total_rows = n_sp * rows
    vmem = pl.BlockSpec(memory_space=pltpu.VMEM)
    anywhere = pl.BlockSpec(memory_space=pl.ANY)
    dma = pltpu.SemaphoreType.DMA
    return pl.pallas_call(
        functools.partial(layer_kernel, n_sp, n_tp, splits),
        out_shape=jax.ShapeDtypeStruct((rows, cols), bf16),
        in_specs=[vmem, anywhere] + [vmem] * 7 + [anywhere] * 2 + [vmem],
        out_specs=vmem,
        scratch_shapes=[
            pltpu.VMEM((n_sp, 4, rows // 4, lat_wide), bf16),
            pltpu.VMEM((total_rows, head_count * NOPE), bf16),
            pltpu.VMEM((total_rows, LANES), bf16),
            pltpu.VMEM((total_rows, head_count * VDIM), bf16),
            pltpu.VMEM((n_sp, weight_rows, hidden_width), bf16),
            pltpu.VMEM((n_sp, weight_rows, hidden_width), bf16),
            pltpu.VMEM((n_sp, weight_rows, hidden_width), bf16),
            pltpu.VMEM((head_count, rows, 2 * LANES), bf16),
            pltpu.VMEM((rows, head_count * VDIM), bf16),
            pltpu.VMEM((n_tp, rows, cols), bf16),
            pltpu.VMEM((n_tp, rows, cols), bf16),
            pltpu.VMEM((8, rows), jnp.float32),
            pltpu.VMEM((n_tp, 8, rows), jnp.float32),
            pltpu.VMEM((n_tp, rows, cols), bf16),
            pltpu.VMEM((n_tp, rows, cols), bf16),
            pltpu.VMEM((n_tp, rows, cols), bf16),
            pltpu.VMEM((8, rows), jnp.float32),
            pltpu.VMEM((n_tp, 8, rows), jnp.float32),
            pltpu.VMEM((rows, hidden_width), bf16),
            dma((4,)),
            dma((2,)),
            dma((2, n_sp - 1)),
            dma((2,)),
            dma((2, n_sp - 1)),
            dma((3, splits, 2)),
            dma((3, splits, 2, n_sp - 1)),
            dma((5, n_tp)),
            dma((5, n_tp)),
            dma((n_tp, 2 * (n_sp // n_tp))),
            dma((n_tp, 2 * (n_sp // n_tp))),
        ],
        compiler_params=pltpu.CompilerParams(
            collective_id=0, has_side_effects=True, vmem_limit_bytes=66000000
        ),
    )(
        queries,
        latents.reshape(4, rows // 4, rank),
        rope_key,
        w_key,
        w_value,
        w_out,
        resid,
        gain_mix.reshape(1, -1),
        gain_out.reshape(1, -1),
        w_gate,
        w_up,
        w_down,
    )


def solution(mesh):
    placed = (
        P("sp", "tp"),
        P("sp", None),
        P("sp", None),
        P(None, "tp"),
        P(None, "tp"),
        P("tp", None),
        P("sp", "tp"),
        P("tp"),
        P("sp", "tp"),
        P("sp", "tp"),
        P("tp", "sp"),
        P("tp"),
    )
    return jax.shard_map(
        local, mesh=mesh, in_specs=placed, out_specs=P("sp", "tp"), check_vma=False
    )
```

```python
import functools

import jax
import jax.numpy as jnp
from jax import lax
from jax.experimental import pallas as pl
from jax.experimental.pallas import tpu as pltpu
from jax.sharding import PartitionSpec as P

NOPE = 64
ROPE = 32
VDIM = 64
GRID_W = 64
LANES = 128

ROTARY_BASE = 10000.0
NORM_EPSILON = 1e-06
DEEP_ALPHA = 8.0**0.25
HALF_STEP = 0.5
MESH = pl.DeviceIdType.MESH


def rotary_tables(first, rows):
    at = first + lax.broadcasted_iota(jnp.int32, (rows, LANES), 0)
    column = lax.broadcasted_iota(jnp.int32, (rows, LANES), 1)
    freq_count = ROPE // 4
    grid_row = (at // GRID_W).astype(jnp.float32)
    grid_col = (at % GRID_W).astype(jnp.float32)
    spot = jnp.where(column % (2 * freq_count) < freq_count, grid_row, grid_col)
    inverse = jnp.ones((rows, LANES), jnp.float32)
    for k in range(1, freq_count):
        inverse = jnp.where(column % freq_count == k, ROTARY_BASE ** (-k / freq_count), inverse)
    angles = spot * inverse
    return (jnp.cos(angles)[:, : ROPE // 2], jnp.sin(angles)[:, : ROPE // 2])


def rotate(vectors, cosine, sine):
    half_width = ROPE // 2
    leading = vectors[:, :half_width]
    trailing = vectors[:, half_width:]
    return [leading * cosine - trailing * sine, leading * sine + trailing * cosine]


def ring_device(place, count):
    return jnp.where(place < count // 2, 2 * place, 2 * (count - 1 - place) + 1)


def ring_place(index, count):
    return jnp.where(index % 2 == 0, index // 2, count - 1 - index // 2)


def dot(left, right):
    return jnp.dot(left, right, preferred_element_type=jnp.float32)


def dot_nt(left, right):
    return lax.dot_general(
        left, right, (((1,), (1,)), ((), ())), preferred_element_type=jnp.float32
    )


def layer_kernel(
    n_sp,
    n_tp,
    splits,
    q_ref,
    lat_ref,
    rope_ref,
    wk_ref,
    wv_ref,
    wo_ref,
    resid_ref,
    gain_mix_ref,
    gain_out_ref,
    wg_ref,
    wu_ref,
    wd_ref,
    out_ref,
    lat_all,
    keys,
    rotary,
    values,
    gate_all,
    up_all,
    down_all,
    q_all,
    heads,
    part_send,
    part_recv,
    stat_send,
    stat_recv,
    rows_all,
    part2_send,
    part2_recv,
    stat2_send,
    stat2_recv,
    hid,
    local_sem,
    lat_send,
    lat_recv,
    share_send,
    share_recv,
    ring_send,
    ring_recv,
    tp_send,
    tp_recv,
    down_send,
    down_recv,
):
    sp = lax.axis_index("sp")
    tp = lax.axis_index("tp")
    place = ring_place(sp, n_sp)
    ahead = ring_device((place + 1) % n_sp, n_sp)
    behind = ring_device((place + n_sp - 1) % n_sp, n_sp)
    targets = (ahead, behind)
    partner = tp + 1 - 2 * (tp % 2)
    core = tp % 2
    n_rows = q_ref.shape[0]
    head_count = wk_ref.shape[1] // NOPE
    rank = wk_ref.shape[0]
    lat_rows = lat_all.shape[2]
    n_cols = out_ref.shape[1]

    barrier = pltpu.get_barrier_semaphore()
    for device in targets:
        pl.semaphore_signal(barrier, inc=1, device_id={"sp": device}, device_id_type=MESH)
    for step in range(1, n_tp):
        pl.semaphore_signal(
            barrier, inc=1, device_id={"tp": (tp + step) % n_tp}, device_id_type=MESH
        )

    own = []
    lat_own = pltpu.make_async_copy(
        lat_ref, lat_all.at[sp, :, :, pl.ds(0, rank)], local_sem.at[0]
    )
    lat_own.start()
    weights = (gate_all, up_all, down_all)
    for i, source in enumerate((wg_ref, wu_ref)):
        copy = pltpu.make_async_copy(source, weights[i].at[sp], local_sem.at[i + 1])
        copy.start()
        own.append(copy)
    cosine, sine = rotary_tables(sp * n_rows, n_rows)
    key_rot = rotate(rope_ref[...].astype(jnp.float32), cosine, sine)
    key_rot.append(jnp.zeros((n_rows, LANES - ROPE), jnp.float32))
    lat_all[sp, :, :, pl.ds(rank, LANES)] = (
        jnp.concatenate(key_rot, axis=1).astype(jnp.bfloat16).reshape(4, lat_rows, LANES)
    )

    def prepare_queries(head):
        base = head * (NOPE + ROPE)
        wide_q = q_ref[...].astype(jnp.float32)
        nope = wide_q[:, base : base + NOPE]
        other = jnp.zeros((n_rows, NOPE), jnp.float32)
        rotary = rotate(wide_q[:, base + NOPE : base + NOPE + ROPE], cosine, sine)
        parts = [nope, other] if head % 2 == 0 else [other, nope]
        parts = parts + rotary + [jnp.zeros((n_rows, LANES - ROPE), jnp.float32)]
        q_all[head] = jnp.concatenate(parts, axis=1).astype(jnp.bfloat16)

    def prepare_down():
        count = wd_ref.shape[1]
        across = lax.broadcasted_iota(jnp.int32, (count, count), 1)
        diagonal = (lax.broadcasted_iota(jnp.int32, (count, count), 0) == across).astype(
            jnp.float32
        ).astype(jnp.bfloat16)
        down_all[sp] = dot_nt(diagonal, wd_ref[...]).astype(jnp.bfloat16)

    preparing = [functools.partial(prepare_queries, head) for head in range(head_count)]
    preparing.append(prepare_down)
    pl.semaphore_wait(barrier, 2 + n_tp - 1)

    def origin(hop, direction):
        if direction == 0:
            return ring_device((place + n_sp - hop) % n_sp, n_sp)
        return ring_device((place + hop) % n_sp, n_sp)

    def lat_copy(hop, direction):
        block = lat_all.at[origin(hop - 1, direction), core * 2 + direction]
        return pltpu.make_async_remote_copy(
            src_ref=block,
            dst_ref=block,
            send_sem=lat_send.at[direction],
            recv_sem=lat_recv.at[direction, hop - 1],
            device_id={"sp": targets[direction]},
            device_id_type=MESH,
        )

    def lat_arrival(hop, direction):
        block = lat_all.at[origin(hop, direction), core * 2 + direction]
        return pltpu.make_async_remote_copy(
            src_ref=block,
            dst_ref=block,
            send_sem=lat_send.at[direction],
            recv_sem=lat_recv.at[direction, hop - 1],
            device_id={"sp": targets[direction]},
            device_id_type=MESH,
        )

    def share_copy(hop, direction, which):
        block = lat_all.at[origin(hop, direction), which * 2 + direction]
        return pltpu.make_async_remote_copy(
            src_ref=block,
            dst_ref=block,
            send_sem=share_send.at[direction],
            recv_sem=share_recv.at[direction, hop - 1],
            device_id={"tp": partner},
            device_id_type=MESH,
        )

    piece_rows = wg_ref.shape[0] // (2 * splits)

    def ring_copy(array, piece, hop, direction, arriving):
        block = origin(hop if arriving else hop - 1, direction)
        rows = pl.ds((direction * splits + piece) * piece_rows, piece_rows)
        ref = weights[array].at[block, rows]
        return pltpu.make_async_remote_copy(
            src_ref=ref,
            dst_ref=ref,
            send_sem=ring_send.at[array, piece, direction],
            recv_sem=ring_recv.at[array, piece, direction, hop - 1],
            device_id={"sp": targets[direction]},
            device_id_type=MESH,
        )

    started = set()

    def ring_step(array, piece, hop):
        if hop == 1 and array < 2 and array not in started:
            own[array].wait()
            started.add(array)
        for direction in range(2):
            if hop > 1:
                ring_copy(array, piece, hop - 1, direction, True).wait_recv()
                ring_copy(array, piece, hop - 1, direction, False).wait_send()
            if hop < n_sp:
                ring_copy(array, piece, hop, direction, False).start()

    first = [
        (array, piece, hop)
        for hop in range(1, n_sp)
        for array in range(2)
        for piece in range(splits)
    ]
    second = [(2, piece, hop) for hop in range(1, n_sp) for piece in range(splits)]
    queue = [first + second, 0]

    def advance(count):
        steps, at = queue
        for step in steps[at : at + count]:
            ring_step(*step)
        queue[1] = min(at + count, len(steps))

    unit = max(1, len(first) // 28)

    lat_own.wait()
    for hop in range(1, n_sp + 1):
        for direction in range(2):
            if hop > 1:
                lat_arrival(hop - 1, direction).wait_recv()
                lat_copy(hop - 1, direction).wait_send()
            if hop < n_sp:
                lat_copy(hop, direction).start()
            if hop > 2:
                share_copy(hop - 2, direction, core).wait_send()
            if hop > 1:
                share_copy(hop - 1, direction, core).start()
        if hop < n_sp and queue[1] < 7 * unit:
            advance(1)
        if preparing:
            preparing.pop(0)()
    while preparing:
        preparing.pop(0)()
    for direction in range(2):
        share_copy(n_sp - 1, direction, core).wait_send()
        for hop in range(1, n_sp):
            share_copy(hop, direction, 1 - core).wait_recv()

    total_rows = n_sp * n_rows
    lat_wide = lat_all.shape[3]
    chunk_blocks = max(1, min(n_sp, 1536 // n_rows))
    chunks = n_sp // chunk_blocks
    chunk = chunk_blocks * n_rows
    half_blocks = max(1, chunk_blocks // 2)

    def project(step):
        rows = half_blocks * n_rows
        blocks = pl.ds(step * half_blocks, half_blocks)
        lat = lat_all[blocks, :, :, pl.ds(0, rank)].reshape(rows, rank)
        rotary[pl.ds(step * rows, rows)] = lat_all[blocks, :, :, pl.ds(rank, LANES)].reshape(
            rows, LANES
        )
        keys[pl.ds(step * rows, rows)] = dot(lat, wk_ref[...]).astype(jnp.bfloat16)
        values[pl.ds(step * rows, rows)] = dot(lat, wv_ref[...]).astype(jnp.bfloat16)

    if chunks == 1:
        for step in range(n_sp // half_blocks):
            project(step)
            advance(unit)
    else:
        pl.loop(0, n_sp // half_blocks)(project)
        advance(2 * unit)

    score_scale = (NOPE + ROPE) ** (-0.5)
    lane = lax.broadcasted_iota(jnp.int32, (n_rows, LANES), 1)

    def attend(head, at, state):
        maxima, totals, running = state
        rows = pl.ds(at * chunk, chunk)
        pair = slice(head // 2 * LANES, (head // 2 + 1) * LANES)
        whole_keys = jnp.concatenate([keys[rows, pair], rotary[rows]], axis=1)
        scores = dot_nt(q_all[head], whole_keys) * score_scale
        top = jnp.max(scores, axis=1, keepdims=True)
        if maxima is not None:
            top = jnp.maximum(maxima, top)
        probs = jnp.exp(scores - top)
        sums = jnp.sum(probs, axis=1, keepdims=True)
        update = dot(probs.astype(jnp.bfloat16), values[rows, pair])
        if maxima is not None:
            factor = jnp.exp(maxima - top)
            sums = totals * factor + sums
            update = running * factor + update
        return (top, sums, update)

    for head in range(head_count):
        state = attend(head, 0, (None, None, None))
        if chunks > 1:
            state = lax.fori_loop(1, chunks, functools.partial(attend_loop, attend, head), state)
        result = state[2] / state[1]
        pair = slice(head // 2 * LANES, (head // 2 + 1) * LANES)
        if head % 2 == 0:
            heads[:, pair] = result.astype(jnp.bfloat16)
        else:
            heads[:, pair] = jnp.where(
                lane < VDIM, heads[:, pair].astype(jnp.float32), result
            ).astype(jnp.bfloat16)
        advance(unit)

    def tp_copy(stage, slot_source, slot_target, to, slot_semaphore):
        return pltpu.make_async_remote_copy(
            src_ref=slot_source,
            dst_ref=slot_target,
            send_sem=tp_send.at[stage, slot_semaphore],
            recv_sem=tp_recv.at[stage, slot_semaphore],
            device_id={"tp": to},
            device_id_type=MESH,
        )

    def exchange(stage, source_of, target_of):
        copies = []
        for k in range(1, n_tp):
            to = (tp + k) % n_tp
            copies.append(tp_copy(stage, source_of(to), target_of(k), to, k))
        return copies

    copies = exchange(0, lambda to: part_send.at[to], lambda k: part_recv.at[k])
    for k in range(1, n_tp + 1):
        to = (tp + k) % n_tp
        part_send[to] = dot(
            heads[...], wo_ref[:, pl.ds(pl.multiple_of(to * n_cols, LANES), n_cols)]
        ).astype(jnp.bfloat16)
        if k < n_tp:
            copies[k - 1].start()
    advance(4 * unit)
    mixed = DEEP_ALPHA * resid_ref[...].astype(jnp.float32) + part_send[tp].astype(jnp.float32)
    for k in range(1, n_tp):
        copies[k - 1].wait_recv()
        mixed = mixed + part_recv[k].astype(jnp.float32)
    pending = list(copies)

    width_total = n_cols * n_tp

    def normed(rows_in, gain_ref, stage, send, recv, between):
        sums = jnp.sum(rows_in, axis=1, keepdims=True)
        squares = jnp.sum(rows_in * rows_in, axis=1, keepdims=True)
        mine = jnp.transpose(jnp.where(lane < 4, sums, squares))[:8]
        send[...] = mine
        copies = exchange(stage, lambda to: send, lambda k: recv.at[k])
        for copy in copies:
            copy.start()
        between()
        for k in range(1, n_tp):
            copies[k - 1].wait_recv()
            mine = mine + recv[k]
        pending.extend(copies)
        whole = jnp.transpose(mine) / width_total
        row_mean = whole[:, :1]
        variance = whole[:, 4:5] - row_mean * row_mean
        return (
            (rows_in - row_mean) * lax.rsqrt(variance + NORM_EPSILON) * gain_ref[...]
        ).astype(jnp.bfloat16)

    hidden_in = normed(
        mixed, gain_mix_ref, 1, stat_send, stat_recv, lambda: advance(2 * unit)
    )
    rows_all[tp] = hidden_in
    copies = exchange(2, lambda to: rows_all.at[tp], lambda k: rows_all.at[tp])
    for copy in copies:
        copy.start()
    pending.extend(copies)
    advance(4 * unit)
    for k in range(1, n_tp):
        sender = (tp + n_tp - k) % n_tp
        tp_copy(2, rows_all.at[sender], rows_all.at[sender], sender, k).wait_recv()

    advance(len(first) - queue[1])
    advance(splits)

    def last_hop(array):
        for piece in range(splits):
            for direction in range(2):
                ring_copy(array, piece, n_sp - 1, direction, True).wait_recv()
                ring_copy(array, piece, n_sp - 1, direction, False).wait_send()

    last_hop(0)
    group = n_sp // n_tp
    depth = group * wg_ref.shape[0]
    hidden_width = wg_ref.shape[1]

    def wide(weight):
        total = None
        for t in range(n_tp):
            term = dot(
                rows_all[t],
                weight[t * group : (t + 1) * group].reshape(depth, hidden_width),
            )
            total = term if total is None else total + term
            advance(1)
        return total

    gate_sum = wide(gate_all)
    last_hop(1)
    up_sum = wide(up_all)
    hidden = (gate_sum / (1.0 + jnp.exp(-gate_sum)) * up_sum).astype(jnp.bfloat16)
    advance(1)

    half_rows = piece_rows * splits
    if half_rows % LANES == 0:
        hid[...] = hidden

        def down_copy(k, slot, to, columns):
            ref = part2_send.at[to, :, columns]
            return pltpu.make_async_remote_copy(
                src_ref=ref,
                dst_ref=part2_recv.at[k, :, columns],
                send_sem=down_send.at[k, slot],
                recv_sem=down_recv.at[k, slot],
                device_id={"tp": to},
                device_id_type=MESH,
            )

        def slot_columns(slot):
            return pl.ds(pl.multiple_of(slot * half_rows, LANES), half_rows)

        def make_columns(hop):
            for direction in range(2):
                block = origin(hop, direction)
                owner = block // group
                slot = (block % group) * 2 + direction
                rows = pl.ds(direction * half_rows, half_rows)
                part2_send[owner, :, slot_columns(slot)] = dot_nt(
                    hid[...], down_all[block, rows]
                ).astype(jnp.bfloat16)

                @pl.when(owner != tp)
                def send_away():
                    down_copy((owner + n_tp - tp) % n_tp, slot, owner, slot_columns(slot)).start()

        made = 0
        while queue[1] < len(queue[0]):
            array, piece, hop = queue[0][queue[1]]
            advance(1)
            if piece == splits - 1:
                made_to = hop
                while made < made_to:
                    make_columns(made)
                    made += 1
        while made < n_sp - 1:
            make_columns(made)
            made += 1
        last_hop(2)
        make_columns(n_sp - 1)
        mixer = part2_send[tp].astype(jnp.float32)
        for k in range(1, n_tp):
            for slot in range(2 * group):
                down_copy(k, slot, (tp + k) % n_tp, slot_columns(slot)).wait_recv()
            mixer = mixer + part2_recv[k].astype(jnp.float32)
    else:
        advance(len(queue[0]))
        last_hop(2)
        copies = exchange(3, lambda to: part2_send.at[to], lambda k: part2_recv.at[k])
        for k in range(1, n_tp + 1):
            to = (tp + k) % n_tp
            part2_send[to] = dot_nt(
                hidden, down_all[pl.ds(to * group, group)].reshape(depth, hidden_width)
            ).astype(jnp.bfloat16)
            if k < n_tp:
                copies[k - 1].start()
        mixer = part2_send[tp].astype(jnp.float32)
        for k in range(1, n_tp):
            copies[k - 1].wait_recv()
            mixer = mixer + part2_recv[k].astype(jnp.float32)
        pending.extend(copies)
    final = DEEP_ALPHA * rows_all[tp].astype(jnp.float32) + HALF_STEP * mixer
    out_ref[...] = normed(final, gain_out_ref, 4, stat2_send, stat2_recv, lambda: None)
    for copy in pending:
        copy.wait_send()
    if half_rows % LANES == 0:
        for k in range(1, n_tp):
            for slot in range(2 * group):
                down_copy(k, slot, (tp + k) % n_tp, slot_columns(slot)).wait_send()


def attend_loop(attend, head, at, state):
    return attend(head, at, state)


def flip(value, mask):
    result = value
    bit = 1
    while bit <= mask:
        if mask & bit:
            result = result + bit - 2 * bit * ((value // bit) % 2)
        bit *= 2
    return result


class Semaphores:
    def __init__(self, refs):
        self.refs, self.base, self.used = refs, {}, 0

    def at(self, name, count=1, index=0):
        if name not in self.base:
            self.base[name] = self.used
            self.used += count
        return self.refs.at[self.base[name] + index]


def paired_kernel(
    n_sp,
    n_tp,
    pieces,
    q_in,
    lat_ref,
    rope_in,
    wk_in,
    wv_in,
    wo_ref,
    resid_in,
    gain_mix_in,
    gain_out_in,
    wg_ref,
    wu_ref,
    wd_ref,
    out_ref,
    q_ref,
    rope_ref,
    wk_ref,
    wv_ref,
    resid_ref,
    gain_mix_ref,
    gain_out_ref,
    lat_all,
    keys,
    rotary,
    values,
    q_all,
    heads_all,
    wo_all,
    wide_all,
    down_own,
    down_all,
    rows_all,
    hid,
    summed,
    core_send,
    core_recv,
    far_send,
    far_recv,
    pair_send,
    pair_recv,
    first_send,
    first_recv,
    last_send,
    last_recv,
    total_sum,
    stat_send,
    stat_recv,
    local_sem,
    remote_sem,
):
    sp = lax.axis_index("sp")
    tp = lax.axis_index("tp")
    n_hi = n_sp // 2
    z, x = sp // 2, sp % 2
    half = z % 2
    edge = half == (z // 2) % 2
    inner = jnp.logical_not(edge)
    n_rows = q_ref.shape[0]
    head_count = wk_ref.shape[1] // NOPE
    rank = wk_ref.shape[0]
    lat_rows = lat_all.shape[2]
    n_cols = out_ref.shape[1]
    group = n_sp // n_tp
    depth = wg_ref.shape[0]
    width = wg_ref.shape[1] // 2
    piece_cols = wd_ref.shape[1] // pieces
    local_sems = Semaphores(local_sem)
    remote_sems = Semaphores(remote_sem)

    order = [(1, flip(z, 1))]
    for m in range(2, n_hi, 2):
        low, high = flip(z, m), flip(z, m + 1)
        order.append((jnp.where(edge, m, m + 1), jnp.where(edge, low, high)))
        order.append((jnp.where(edge, m + 1, m), jnp.where(edge, high, low)))
    near, rest = list(range(1, len(order), 2)), list(range(2, len(order), 2))

    def sp_of(place, side):
        return 2 * place + side

    def remote(source, target, device, sent, name, count=1, index=0):
        return pltpu.make_async_remote_copy(
            src_ref=source,
            dst_ref=target,
            send_sem=remote_sems.at(("sent", sent)),
            recv_sem=remote_sems.at(name, count, index),
            device_id=device,
            device_id_type=MESH,
        )

    other_x = 1 - x
    partner, across, corner = flip(tp, 1), flip(tp, 2), flip(tp, 3)
    to_x = {"sp": sp_of(z, other_x)}
    to_pair = {"sp": sp_of(flip(z, 1), x)}
    to_core = {"tp": partner}
    to_across = {"tp": across}

    barrier = pltpu.get_barrier_semaphore()
    peers = [{"sp": sp_of(flip(z, k), x)} for k in range(1, n_hi)] + [to_x]
    peers += [{"tp": flip(tp, j)} for j in range(1, n_tp)]
    for device in peers:
        pl.semaphore_signal(barrier, inc=1, device_id=device, device_id_type=MESH)

    def local(source, target, name):
        return pltpu.make_async_copy(source, target, local_sems.at(name))

    inputs = {
        "rope": local(rope_in, rope_ref, "rope"),
        "q": local(q_in, q_ref, "q"),
        "wk": local(wk_in, wk_ref, "wk"),
        "wv": local(wv_in, wv_ref, "wv"),
        "resid": local(resid_in, resid_ref, "resid"),
        "mix": local(gain_mix_in, gain_mix_ref, "mix"),
        "out": local(gain_out_in, gain_out_ref, "out"),
    }

    wide_rows = depth // pieces

    def wide_source(array, which, piece):
        columns = pl.ds(pl.multiple_of(which * width, LANES), width)
        return (wg_ref, wu_ref)[array].at[pl.ds(piece * wide_rows, wide_rows), columns]

    def wide_block(array, place, side, piece):
        rows = pl.ds(piece * wide_rows, wide_rows)
        return wide_all.at[sp_of(place, side), rows, pl.ds(array * width, width)]

    def down_rows(which, piece):
        rows = pl.ds(pl.multiple_of(which * width, 16), width)
        return wd_ref.at[rows, pl.ds(piece * piece_cols, piece_cols)]

    def down_block(place, side, piece):
        return down_all.at[place * pieces + piece, side]

    def weight_source(array, which, piece):
        if array == 2:
            return down_own.at[which, piece]
        return wide_source(array, which, piece)

    def weight_block(array, place, side, piece):
        if array == 2:
            return down_block(place, side, piece)
        return wide_block(array, place, side, piece)

    def sent_of(array):
        return "down" if array == 2 else "wide"

    def parts_of(array, ref):
        if array < 2:
            return [ref]
        return [ref.at[pl.ds(part * width // 2, width // 2)] for part in range(2)]

    def weight_out(array, k, piece):
        place = flip(z, k)
        sources = parts_of(array, weight_source(array, place % 2, piece))
        targets = parts_of(array, weight_block(array, z, x, piece))
        for part, (source, target) in enumerate(zip(sources, targets)):
            remote(
                source,
                target,
                {"sp": sp_of(place, x)},
                sent_of(array),
                ("wz", array, piece, part),
                n_hi - 1,
                k - 1,
            ).start()

    def weight_side(array, k, place, piece, source=None):
        block = weight_block(array, place, x, piece)
        name = ("wx", piece) if array == 2 else "wx"
        count, index = (n_hi, k) if array == 2 else (1, 0)
        source = block if source is None else source
        remote(source, block, to_x, sent_of(array), name, count, index).start()

    def weight_own(array, piece):
        weight_side(array, 0, z, piece, weight_source(array, half, piece))

    def relay(array, at, piece):
        k, place = order[at]
        name = ("wx", piece) if array == 2 else "wx"
        count, index = (n_hi, k) if array == 2 else (1, 0)
        for part, block in enumerate(parts_of(array, weight_block(array, place, x, piece))):
            remote(
                block,
                block,
                to_x,
                sent_of(array),
                ("wz", array, piece, part),
                n_hi - 1,
                k - 1,
            ).wait_recv()
            remote(block, block, to_x, sent_of(array), name, count, index).start()

    def relay_all(array, at):
        for piece in range(pieces):
            relay(array, at, piece)

    lat_own = local(lat_ref, lat_all.at[sp, :, :, pl.ds(0, rank)], "lat")
    inputs["rope"].start()
    lat_own.start()
    for name in ("q", "wk", "wv", "resid", "mix", "out"):
        inputs[name].start()
    staged = []
    for piece in range(pieces):
        for which in range(2):
            name = ("staged", which, piece)
            staged.append(local(down_rows(which, piece), down_own.at[which, piece], name))
            staged[-1].start()
        for array in range(2):
            local(
                weight_source(array, half, piece), weight_block(array, z, x, piece), "wide"
            ).start()
    down_mine = []
    for piece in range(pieces):
        down_mine.append(
            local(down_rows(half, piece), down_block(z, x, piece), ("down", piece))
        )
        down_mine[-1].start()

    def wo_columns(which):
        return wo_ref.at[:, pl.ds(pl.multiple_of(which * n_cols, LANES), n_cols)]

    wo_own = local(wo_columns(tp), wo_all.at[tp], "wo")
    wo_own.start()
    cosine, sine = rotary_tables(sp * n_rows, n_rows)
    inputs["rope"].wait()
    turned_in = jnp.concatenate(
        [rope_ref[...].astype(jnp.float32), jnp.zeros((LANES - ROPE, n_rows), jnp.float32)],
        axis=0,
    )
    key_rot = rotate(jnp.transpose(turned_in)[:, :ROPE], cosine, sine)
    key_rot.append(jnp.zeros((n_rows, LANES - ROPE), jnp.float32))
    lat_all[sp, :, :, pl.ds(rank, LANES)] = (
        jnp.concatenate(key_rot, axis=1).astype(jnp.bfloat16).reshape(n_tp, lat_rows, LANES)
    )

    def prepare_queries(head):
        base = head * (NOPE + ROPE)
        wide_q = q_ref[...].astype(jnp.float32)
        nope = wide_q[:, base : base + NOPE]
        other = jnp.zeros((n_rows, NOPE), jnp.float32)
        turned = rotate(wide_q[:, base + NOPE : base + NOPE + ROPE], cosine, sine)
        parts = [nope, other] if head % 2 == 0 else [other, nope]
        parts = parts + turned + [jnp.zeros((n_rows, LANES - ROPE), jnp.float32)]
        q_all[head] = jnp.concatenate(parts, axis=1).astype(jnp.bfloat16)

    pl.semaphore_wait(barrier, len(peers))
    lat_own.wait()
    for copy in staged:
        copy.wait()

    def lat_copy(name, k, place, side, quarter, device):
        block = lat_all.at[sp_of(place, side), quarter]
        return remote(block, block, device, "lat", ("lat", name), n_hi, k)

    def lat_core(place, side, quarter):
        block = lat_all.at[sp_of(place, side), quarter]
        remote(block, block, to_core, "lat", "latc").start()

    def lat_z_in(at):
        k, place = order[at]
        lat_copy("z", k, place, x, tp, to_x).wait_recv()
        lat_copy("x", k, place, x, tp, to_x).start()
        lat_copy("y", k, place, x, tp, to_across).start()
        lat_core(place, x, tp)

    def lat_x_in(at):
        k, place = (0, z) if at is None else order[at]
        lat_copy("x", k, place, other_x, tp, to_x).wait_recv()
        lat_copy("yd", k, place, other_x, tp, to_across).start()
        lat_core(place, other_x, tp)

    def lat_y_in(at):
        k, place = order[at]
        lat_copy("y", k, place, x, across, to_across).wait_recv()
        lat_core(place, x, across)

    def lat_yd_in(at):
        k, place = (0, z) if at is None else order[at]
        lat_copy("yd", k, place, other_x, across, to_across).wait_recv()
        lat_core(place, other_x, across)

    for k in range(1, n_hi):
        block = lat_all.at[sp, tp]
        remote(
            block, block, {"sp": sp_of(flip(z, k), x)}, "lat", ("lat", "z"), n_hi, k
        ).start()
    lat_copy("x", 0, z, x, tp, to_x).start()
    weight_own(0, 0)

    far = list(range(2, n_hi))

    def send_near(arrays):
        for array in arrays:
            for piece in range(pieces):
                weight_out(array, 1, piece)

    def send_far(array, which):
        for piece in which:
            for k in far:
                weight_out(array, k, piece)

    every = range(pieces)
    early, late = range(pieces // 2), range(pieces // 2, pieces)

    @pl.when(edge)
    def outer_first():
        send_near((0, 1))
        send_far(0, every)
        send_far(1, early)

    @pl.when(inner)
    def inner_first():
        send_near((0, 1, 2))
        send_far(0, every)
        send_far(1, every)

    inputs["q"].wait()
    prepare_queries(0)
    lat_x_in(None)
    lat_z_in(0)

    prepare_queries(1)
    for piece in range(1, pieces):
        weight_own(0, piece)
    for at in near:
        lat_z_in(at)
    lat_yd_in(None)
    lat_x_in(0)
    lat_y_in(0)
    for at in rest:
        lat_z_in(at)
    for piece in range(pieces):
        weight_own(1, piece)
    for piece in range(pieces):
        weight_own(2, piece)
    for head in range(2, head_count):
        prepare_queries(head)
    for at in near:
        lat_x_in(at)
        lat_y_in(at)
    lat_yd_in(0)
    for at in rest:
        lat_x_in(at)
        lat_y_in(at)
    for j in (2, 3, 1):
        to = flip(tp, j)
        remote(wo_columns(to), wo_all.at[tp], {"tp": to}, "wo", "wo").start()
    for at in near + rest:
        lat_yd_in(at)
    relay_all(0, 0)
    whole = lat_all.at[pl.ds(0, n_sp - 1), pl.ds(0, 2)]
    remote(whole, whole, to_core, "lat", "latc").wait_recv()

    half_blocks = n_sp // 2

    def project(step):
        rows = half_blocks * n_rows
        blocks = pl.ds(step * half_blocks, half_blocks)
        lat = lat_all[blocks, :, :, pl.ds(0, rank)].reshape(rows, rank)
        rotary[pl.ds(step * rows, rows)] = lat_all[blocks, :, :, pl.ds(rank, LANES)].reshape(
            rows, LANES
        )
        keys[pl.ds(step * rows, rows)] = dot(lat, wk_ref[...]).astype(jnp.bfloat16)
        values[pl.ds(step * rows, rows)] = dot(lat, wv_ref[...]).astype(jnp.bfloat16)

    inputs["wk"].wait()
    inputs["wv"].wait()
    for step in range(n_sp // half_blocks):
        project(step)

    score_scale = (NOPE + ROPE) ** (-0.5)
    lane = lax.broadcasted_iota(jnp.int32, (n_rows, LANES), 1)

    for head in range(head_count):
        pair = slice(head // 2 * LANES, (head // 2 + 1) * LANES)
        whole_keys = jnp.concatenate([keys[:, pair], rotary[...]], axis=1)
        scores = dot_nt(q_all[head], whole_keys) * score_scale
        top = jnp.max(scores, axis=1, keepdims=True)
        probs = jnp.exp(scores - top)
        sums = jnp.sum(probs, axis=1, keepdims=True)
        result = dot(probs.astype(jnp.bfloat16), values[:, pair]) / sums
        if head % 2 == 0:
            held = result
        else:
            heads_all[tp, :, pair] = jnp.where(lane < VDIM, held, result).astype(jnp.bfloat16)
            block = heads_all.at[tp, :, pl.ds(head // 2 * LANES, LANES)]
            for j in (2, 3, 1):
                remote(block, block, {"tp": flip(tp, j)}, "heads", "heads").start()
        if head == head_count // 2 - 1:
            relay_all(1, 0)
    for at in near:
        relay_all(0, at)
    for name in ("resid", "mix", "out"):
        inputs[name].wait()
    mixed = DEEP_ALPHA * resid_ref[...].astype(jnp.float32)
    wo_own.wait()
    mixed = mixed + dot(heads_all[tp], wo_all[tp])
    others = pl.ds(0, n_tp - 1)
    remote(wo_all.at[others], wo_all.at[others], to_core, "wo", "wo").wait_recv()
    remote(heads_all.at[others], heads_all.at[others], to_core, "heads", "heads").wait_recv()
    for j in (1, 2, 3):
        sender = flip(tp, j)
        mixed = mixed + dot(heads_all[sender], wo_all[sender])

    width_total = n_cols * n_tp

    def normed(rows_in, gain_ref, stage, between):
        sums = jnp.sum(rows_in, axis=1, keepdims=True)
        squares = jnp.sum(rows_in * rows_in, axis=1, keepdims=True)
        mine = jnp.transpose(jnp.where(lane < 4, sums, squares))[:8]
        stat_send[stage] = mine
        for j in (2, 3, 1):
            remote(
                stat_send.at[stage],
                stat_recv.at[stage, j - 1],
                {"tp": flip(tp, j)},
                ("stat", stage),
                ("stat", stage),
            ).start()
        between()
        arrived = stat_recv.at[stage]
        remote(arrived, arrived, to_core, ("stat", stage), ("stat", stage)).wait_recv()
        for j in (1, 2, 3):
            mine = mine + stat_recv[stage, j - 1]
        whole = jnp.transpose(mine) / width_total
        row_mean = whole[:, :1]
        variance = whole[:, 4:5] - row_mean * row_mean
        return (
            (rows_in - row_mean) * lax.rsqrt(variance + NORM_EPSILON) * gain_ref[...]
        ).astype(jnp.bfloat16)

    def more_wide():
        for at in rest:
            relay_all(0, at)

    hidden_in = normed(mixed, gain_mix_ref, 0, more_wide)
    mine = pl.ds(pl.multiple_of(half * n_rows, 16), n_rows)
    theirs = pl.ds(pl.multiple_of((1 - half) * n_rows, 16), n_rows)
    rows_all[tp, mine] = hidden_in

    def rows_copy(name, owner, rows, device):
        block = rows_all.at[owner, rows]
        return remote(block, block, device, "rows", ("rows", name))

    def rows_core(owner, rows):
        block = rows_all.at[owner, rows]
        remote(block, block, to_core, "rowsc", "rowsc").start()

    rows_copy("y", tp, mine, to_across).start()
    rows_copy("z", tp, mine, to_pair).start()
    rows_core(tp, mine)

    @pl.when(edge)
    def outer_last():
        send_far(1, late)
        send_near((2,))
        send_far(2, every)

    @pl.when(inner)
    def inner_last():
        send_far(2, every)

    for at in near:
        relay_all(1, at)
    for at in rest:
        for piece in early:
            relay(1, at, piece)
    rows_copy("z", tp, theirs, to_pair).wait_recv()
    rows_copy("yz", tp, theirs, to_across).start()
    rows_core(tp, theirs)
    rows_copy("y", across, mine, to_across).wait_recv()
    rows_core(across, mine)
    for at in rest:
        for piece in late:
            relay(1, at, piece)
    rows_copy("yz", across, theirs, to_across).wait_recv()
    rows_core(across, theirs)
    relay_all(2, 0)
    for at in near:
        for piece in early:
            relay(2, at, piece)
    both = rows_all.at[pl.ds(0, 2)]
    remote(both, both, to_core, "rowsc", "rowsc").wait_recv()
    local(wg_ref, wide_all.at[0], "wide").wait()
    arrived = wide_all.at[pl.ds(0, n_hi)]
    remote(arrived, arrived, to_x, "wide", "wx").wait_recv()

    total = None
    for t in range(n_tp):
        term = dot(
            rows_all[t], wide_all[t * group : (t + 1) * group].reshape(group * depth, 2 * width)
        )
        total = term if total is None else total + term
    gate_sum, up_sum = total[:, :width], total[:, width:]
    hid[...] = (gate_sum / (1.0 + jnp.exp(-gate_sum)) * up_sum).astype(jnp.bfloat16)
    for copy in down_mine:
        copy.wait()

    def facts(at, piece):
        k, place = (0, z) if at is None else order[at]
        unit = place * pieces + piece
        return k, place, unit, tp % 2 == place % 2, tp // 2 == place // 2

    def core_copy(place, unit, piece):
        return remote(
            core_send.at[unit],
            core_recv.at[unit],
            to_core,
            "core",
            "core",
            n_tp // 2 * pieces,
            place // 2 * pieces + piece,
        )

    def far_copy(piece):
        return remote(
            far_send.at[piece], far_recv.at[piece], to_across, "far", "far", pieces, piece
        )

    def pair_copy(piece):
        return remote(
            pair_send.at[piece], pair_recv.at[piece], to_pair, "pair", "pair", pieces, piece
        )

    def pair_first_copy(piece):
        source, target = first_send.at[piece], first_recv.at[piece]
        return remote(source, target, to_pair, "first", "first", pieces, piece)

    def far_last_copy(piece):
        source, target = last_send.at[piece], last_recv.at[piece]
        return remote(source, target, to_across, "last", "last", pieces, piece)

    def make_block(at, piece):
        k, place, unit, same_core, same_chip = facts(at, piece)
        block = down_block(place, other_x, piece)
        remote(block, block, to_x, "down", ("wx", piece), n_hi, k).wait_recv()
        columns = jnp.concatenate([down_all[unit, 0], down_all[unit, 1]], axis=1)
        product = dot(hid[...], columns)

        @pl.when(same_core)
        def keep():
            summed[unit] = product

        @pl.when(jnp.logical_not(same_core))
        def give():
            core_send[unit] = product.astype(jnp.bfloat16)
            core_copy(place, unit, piece).start()

    def add_core(at, piece):
        k, place, unit, same_core, same_chip = facts(at, piece)

        @pl.when(same_core)
        def add():
            core_copy(place, unit, piece).wait_recv()
            both = summed[unit] + core_recv[unit].astype(jnp.float32)

            @pl.when(same_chip)
            def keep():
                summed[unit] = both

            @pl.when(jnp.logical_not(same_chip))
            def give():
                far_send[piece] = both.astype(jnp.bfloat16)
                far_copy(piece).start()

    def add_far(at, piece):
        k, place, unit, same_core, same_chip = facts(at, piece)

        @pl.when(place == tp)
        def add():
            far_copy(piece).wait_recv()
            summed[unit, mine] = summed[unit, mine] + far_recv[piece, mine].astype(jnp.float32)
            pair_send[piece] = (
                summed[unit, theirs] + far_recv[piece, theirs].astype(jnp.float32)
            ).astype(jnp.bfloat16)
            pair_copy(piece).start()

    def pair_first(at, piece):
        k, place, unit, same_core, same_chip = facts(at, piece)

        @pl.when(same_core)
        def add():
            core_copy(place, unit, piece).wait_recv()
            first_send[piece] = (
                summed[unit, theirs] + core_recv[unit, theirs].astype(jnp.float32)
            ).astype(jnp.bfloat16)
            pair_first_copy(piece).start()

    def pair_added(at, piece):
        k, place, unit, same_core, same_chip = facts(at, piece)

        @pl.when(same_core)
        def add():
            pair_first_copy(piece).wait_recv()
            both = summed[unit, mine] + core_recv[unit, mine].astype(jnp.float32)
            both = both + first_recv[piece].astype(jnp.float32)

            @pl.when(same_chip)
            def keep():
                total_sum[piece] = both

            @pl.when(jnp.logical_not(same_chip))
            def give():
                last_send[piece] = both.astype(jnp.bfloat16)
                far_last_copy(piece).start()

    def finish_far(at, piece):
        k, place, unit, same_core, same_chip = facts(at, piece)

        @pl.when(place == tp)
        def add():
            far_last_copy(piece).wait_recv()
            total_sum[piece] = total_sum[piece] + last_recv[piece].astype(jnp.float32)

    def finish_pair(at, piece):
        k, place, unit, same_core, same_chip = facts(at, piece)

        @pl.when(place == tp)
        def add():
            pair_copy(piece).wait_recv()
            total_sum[piece] = summed[unit, mine] + pair_recv[piece].astype(jnp.float32)

    def each(apply, ats, which):
        for piece in which:
            for at in ats:
                apply(at, piece)

    close = [None, 0]
    each(make_block, close, every)
    each(functools.partial(relay, 2), rest, early)
    each(add_core, close, every)
    each(make_block, near, early)
    each(functools.partial(relay, 2), rest, late)
    each(make_block, rest, early)
    each(functools.partial(relay, 2), near, late)
    each(pair_first, near + rest, early)
    each(make_block, rest, late)
    each(make_block, near, late)
    each(pair_first, rest + near, late)
    each(add_far, close, every)
    each(pair_added, near + rest, early)
    each(pair_added, rest + near, late)
    each(finish_pair, close, every)
    each(finish_far, near + rest, every)
    final = [total_sum[piece] for piece in range(pieces)]
    sides = []
    for side in range(2):
        for piece in range(pieces):
            sides.append(final[piece][:, side * piece_cols : (side + 1) * piece_cols])
    mixer = jnp.concatenate(sides, axis=1)
    last_in = DEEP_ALPHA * rows_all[tp, mine].astype(jnp.float32) + HALF_STEP * mixer
    out_ref[...] = normed(last_in, gain_out_ref, 1, lambda: None)

    def all_sent(sent, name, whole):
        remote(whole, whole, to_core, sent, name).wait_send()

    all_sent("lat", "latc", lat_all.at[pl.ds(0, n_sp - 1)])
    all_sent("wide", "wx", wide_all.at[pl.ds(0, n_sp - 1)])
    all_sent("down", "wx", down_all.at[pl.ds(0, (n_sp - 1) * pieces // 2)])
    all_sent("wo", "wo", wo_all.at[others])
    all_sent("heads", "heads", heads_all.at[others])
    all_sent("rows", ("rows", "z"), rows_all.at[others, pl.ds(0, n_rows)])
    all_sent("rowsc", "rowsc", both)
    for stage in range(2):
        all_sent(("stat", stage), ("stat", stage), stat_recv.at[stage])
    all_sent("core", "core", core_send.at[pl.ds(0, n_hi * pieces // 2)])
    all_sent("first", "first", first_send)
    home = tp // 2 == z // 2

    @pl.when(home)
    def sent_home():
        all_sent("pair", "pair", pair_send)
        all_sent("last", "last", last_send)

    @pl.when(jnp.logical_not(home))
    def sent_away():
        all_sent("far", "far", far_send)


def paired_call(n_sp, n_tp, operands):
    queries, latents, rope_key, w_key, w_value, w_out, resid, gain_mix = operands[:8]
    w_gate, w_up, w_down, gain_out = operands[8:]
    rows = queries.shape[0]
    head_count = w_key.shape[1] // NOPE
    rank = latents.shape[1]
    cols = resid.shape[1]
    depth, hidden_width = w_gate.shape
    width = hidden_width // 2
    pieces = 2
    n_hi = n_sp // 2
    unit_cols = 2 * w_down.shape[1] // pieces
    total_rows = n_sp * rows
    bf16 = jnp.bfloat16
    f32 = jnp.float32
    vmem = pl.BlockSpec(memory_space=pltpu.VMEM)
    anywhere = pl.BlockSpec(memory_space=pl.ANY)
    dma = pltpu.SemaphoreType.DMA
    signals = 4 * n_hi + 4 * (n_hi - 1) * pieces + n_hi * pieces
    signals += (n_tp // 2 + 4) * pieces + 24
    return pl.pallas_call(
        functools.partial(paired_kernel, n_sp, n_tp, pieces),
        out_shape=pltpu.VMEM((rows, cols), bf16),
        in_specs=[anywhere] * 12,
        out_specs=vmem,
        scratch_shapes=[
            pltpu.VMEM(queries.shape, bf16),
            pltpu.VMEM((rope_key.shape[1], rows), bf16),
            pltpu.VMEM(w_key.shape, bf16),
            pltpu.VMEM(w_value.shape, bf16),
            pltpu.VMEM(resid.shape, bf16),
            pltpu.VMEM((1, cols), f32),
            pltpu.VMEM((1, cols), f32),
            pltpu.VMEM((n_sp, n_tp, rows // n_tp, rank + LANES), bf16),
            pltpu.VMEM((total_rows, head_count * NOPE), bf16),
            pltpu.VMEM((total_rows, LANES), bf16),
            pltpu.VMEM((total_rows, head_count * VDIM), bf16),
            pltpu.VMEM((head_count, rows, 2 * LANES), bf16),
            pltpu.VMEM((n_tp, rows, head_count * VDIM), bf16),
            pltpu.VMEM((n_tp, head_count * VDIM, cols), bf16),
            pltpu.VMEM((n_sp, depth, 2 * width), bf16),
            pltpu.VMEM((2, pieces, width, unit_cols // 2), bf16),
            pltpu.VMEM((n_hi * pieces, 2, width, unit_cols // 2), bf16),
            pltpu.VMEM((n_tp, 2 * rows, cols), bf16),
            pltpu.VMEM((2 * rows, width), bf16),
            pltpu.VMEM((n_hi * pieces, 2 * rows, unit_cols), f32),
            pltpu.VMEM((n_hi * pieces, 2 * rows, unit_cols), bf16),
            pltpu.VMEM((n_hi * pieces, 2 * rows, unit_cols), bf16),
            pltpu.VMEM((pieces, 2 * rows, unit_cols), bf16),
            pltpu.VMEM((pieces, 2 * rows, unit_cols), bf16),
            pltpu.VMEM((pieces, rows, unit_cols), bf16),
            pltpu.VMEM((pieces, rows, unit_cols), bf16),
            pltpu.VMEM((pieces, rows, unit_cols), bf16),
            pltpu.VMEM((pieces, rows, unit_cols), bf16),
            pltpu.VMEM((pieces, rows, unit_cols), bf16),
            pltpu.VMEM((pieces, rows, unit_cols), bf16),
            pltpu.VMEM((pieces, rows, unit_cols), f32),
            pltpu.VMEM((2, 8, rows), f32),
            pltpu.VMEM((2, n_tp - 1, 8, rows), f32),
            dma((10 + 3 * pieces,)),
            dma((signals,)),
        ],
        compiler_params=pltpu.CompilerParams(
            collective_id=1, has_side_effects=True, vmem_limit_bytes=66000000
        ),
    )(
        queries,
        latents.reshape(n_tp, rows // n_tp, rank),
        rope_key.T,
        w_key,
        w_value,
        w_out,
        resid,
        gain_mix.reshape(1, -1),
        gain_out.reshape(1, -1),
        w_gate,
        w_up,
        w_down,
    )


def fits_pairs(n_sp, n_tp, operands):
    queries, w_key, w_gate, w_down = operands[0], operands[3], operands[8], operands[10]
    return (
        n_tp == 4
        and n_sp == 2 * n_tp
        and queries.shape[0] % 64 == 0
        and n_sp * queries.shape[0] <= 1536
        and (w_key.shape[1] // NOPE) % 2 == 0
        and w_gate.shape[1] % (2 * LANES) == 0
        and w_gate.shape[0] % 32 == 0
        and w_down.shape[1] % (2 * LANES) == 0
    )


def local(
    queries,
    latents,
    rope_key,
    w_key,
    w_value,
    w_out,
    resid,
    gain_mix,
    w_gate,
    w_up,
    w_down,
    gain_out,
):
    n_sp = lax.axis_size("sp")
    n_tp = lax.axis_size("tp")
    operands = (queries, latents, rope_key, w_key, w_value, w_out, resid, gain_mix)
    operands += (w_gate, w_up, w_down, gain_out)
    if fits_pairs(n_sp, n_tp, operands):
        return paired_call(n_sp, n_tp, operands)
    rows = queries.shape[0]
    head_count = w_key.shape[1] // NOPE
    rank = latents.shape[1]
    cols = resid.shape[1]
    hidden_width = w_gate.shape[1]
    weight_rows = w_gate.shape[0]
    lat_wide = rank + LANES
    splits = 2 if weight_rows % 64 == 0 else 1
    bf16 = jnp.bfloat16
    total_rows = n_sp * rows
    vmem = pl.BlockSpec(memory_space=pltpu.VMEM)
    anywhere = pl.BlockSpec(memory_space=pl.ANY)
    dma = pltpu.SemaphoreType.DMA
    return pl.pallas_call(
        functools.partial(layer_kernel, n_sp, n_tp, splits),
        out_shape=jax.ShapeDtypeStruct((rows, cols), bf16),
        in_specs=[vmem, anywhere] + [vmem] * 7 + [anywhere] * 2 + [vmem],
        out_specs=vmem,
        scratch_shapes=[
            pltpu.VMEM((n_sp, 4, rows // 4, lat_wide), bf16),
            pltpu.VMEM((total_rows, head_count * NOPE), bf16),
            pltpu.VMEM((total_rows, LANES), bf16),
            pltpu.VMEM((total_rows, head_count * VDIM), bf16),
            pltpu.VMEM((n_sp, weight_rows, hidden_width), bf16),
            pltpu.VMEM((n_sp, weight_rows, hidden_width), bf16),
            pltpu.VMEM((n_sp, weight_rows, hidden_width), bf16),
            pltpu.VMEM((head_count, rows, 2 * LANES), bf16),
            pltpu.VMEM((rows, head_count * VDIM), bf16),
            pltpu.VMEM((n_tp, rows, cols), bf16),
            pltpu.VMEM((n_tp, rows, cols), bf16),
            pltpu.VMEM((8, rows), jnp.float32),
            pltpu.VMEM((n_tp, 8, rows), jnp.float32),
            pltpu.VMEM((n_tp, rows, cols), bf16),
            pltpu.VMEM((n_tp, rows, cols), bf16),
            pltpu.VMEM((n_tp, rows, cols), bf16),
            pltpu.VMEM((8, rows), jnp.float32),
            pltpu.VMEM((n_tp, 8, rows), jnp.float32),
            pltpu.VMEM((rows, hidden_width), bf16),
            dma((4,)),
            dma((2,)),
            dma((2, n_sp - 1)),
            dma((2,)),
            dma((2, n_sp - 1)),
            dma((3, splits, 2)),
            dma((3, splits, 2, n_sp - 1)),
            dma((5, n_tp)),
            dma((5, n_tp)),
            dma((n_tp, 2 * (n_sp // n_tp))),
            dma((n_tp, 2 * (n_sp // n_tp))),
        ],
        compiler_params=pltpu.CompilerParams(
            collective_id=0, has_side_effects=True, vmem_limit_bytes=66000000
        ),
    )(
        queries,
        latents.reshape(4, rows // 4, rank),
        rope_key,
        w_key,
        w_value,
        w_out,
        resid,
        gain_mix.reshape(1, -1),
        gain_out.reshape(1, -1),
        w_gate,
        w_up,
        w_down,
    )


def solution(mesh):
    placed = (
        P("sp", "tp"),
        P("sp", None),
        P("sp", None),
        P(None, "tp"),
        P(None, "tp"),
        P("tp", None),
        P("sp", "tp"),
        P("tp"),
        P("sp", "tp"),
        P("sp", "tp"),
        P("tp", "sp"),
        P("tp"),
    )
    return jax.shard_map(
        local, mesh=mesh, in_specs=placed, out_specs=P("sp", "tp"), check_vma=False
    )
```

```python
import functools

import jax
import jax.numpy as jnp
from jax import lax
from jax.experimental import pallas as pl
from jax.experimental.pallas import tpu as pltpu
from jax.sharding import PartitionSpec as P

NOPE = 64
ROPE = 32
VDIM = 64
GRID_W = 64
LANES = 128

ROTARY_BASE = 10000.0
NORM_EPSILON = 1e-06
DEEP_ALPHA = 8.0**0.25
HALF_STEP = 0.5
MESH = pl.DeviceIdType.MESH


def rotary_tables(first, rows):
    at = first + lax.broadcasted_iota(jnp.int32, (rows, LANES), 0)
    column = lax.broadcasted_iota(jnp.int32, (rows, LANES), 1)
    freq_count = ROPE // 4
    grid_row = (at // GRID_W).astype(jnp.float32)
    grid_col = (at % GRID_W).astype(jnp.float32)
    spot = jnp.where(column % (2 * freq_count) < freq_count, grid_row, grid_col)
    inverse = jnp.ones((rows, LANES), jnp.float32)
    for k in range(1, freq_count):
        inverse = jnp.where(column % freq_count == k, ROTARY_BASE ** (-k / freq_count), inverse)
    angles = spot * inverse
    return (jnp.cos(angles)[:, : ROPE // 2], jnp.sin(angles)[:, : ROPE // 2])


def rotate(vectors, cosine, sine):
    half_width = ROPE // 2
    leading = vectors[:, :half_width]
    trailing = vectors[:, half_width:]
    return [leading * cosine - trailing * sine, leading * sine + trailing * cosine]


def ring_device(place, count):
    return jnp.where(place < count // 2, 2 * place, 2 * (count - 1 - place) + 1)


def ring_place(index, count):
    return jnp.where(index % 2 == 0, index // 2, count - 1 - index // 2)


def dot(left, right):
    return jnp.dot(left, right, preferred_element_type=jnp.float32)


def dot_nt(left, right):
    return lax.dot_general(
        left, right, (((1,), (1,)), ((), ())), preferred_element_type=jnp.float32
    )


def layer_kernel(
    n_sp,
    n_tp,
    splits,
    q_ref,
    lat_ref,
    rope_ref,
    wk_ref,
    wv_ref,
    wo_ref,
    resid_ref,
    gain_mix_ref,
    gain_out_ref,
    wg_ref,
    wu_ref,
    wd_ref,
    out_ref,
    lat_all,
    keys,
    rotary,
    values,
    gate_all,
    up_all,
    down_all,
    q_all,
    heads,
    part_send,
    part_recv,
    stat_send,
    stat_recv,
    rows_all,
    part2_send,
    part2_recv,
    stat2_send,
    stat2_recv,
    hid,
    local_sem,
    lat_send,
    lat_recv,
    share_send,
    share_recv,
    ring_send,
    ring_recv,
    tp_send,
    tp_recv,
    down_send,
    down_recv,
):
    sp = lax.axis_index("sp")
    tp = lax.axis_index("tp")
    place = ring_place(sp, n_sp)
    ahead = ring_device((place + 1) % n_sp, n_sp)
    behind = ring_device((place + n_sp - 1) % n_sp, n_sp)
    targets = (ahead, behind)
    partner = tp + 1 - 2 * (tp % 2)
    core = tp % 2
    n_rows = q_ref.shape[0]
    head_count = wk_ref.shape[1] // NOPE
    rank = wk_ref.shape[0]
    lat_rows = lat_all.shape[2]
    n_cols = out_ref.shape[1]

    barrier = pltpu.get_barrier_semaphore()
    for device in targets:
        pl.semaphore_signal(barrier, inc=1, device_id={"sp": device}, device_id_type=MESH)
    for step in range(1, n_tp):
        pl.semaphore_signal(
            barrier, inc=1, device_id={"tp": (tp + step) % n_tp}, device_id_type=MESH
        )

    own = []
    lat_own = pltpu.make_async_copy(
        lat_ref, lat_all.at[sp, :, :, pl.ds(0, rank)], local_sem.at[0]
    )
    lat_own.start()
    weights = (gate_all, up_all, down_all)
    for i, source in enumerate((wg_ref, wu_ref)):
        copy = pltpu.make_async_copy(source, weights[i].at[sp], local_sem.at[i + 1])
        copy.start()
        own.append(copy)
    cosine, sine = rotary_tables(sp * n_rows, n_rows)
    key_rot = rotate(rope_ref[...].astype(jnp.float32), cosine, sine)
    key_rot.append(jnp.zeros((n_rows, LANES - ROPE), jnp.float32))
    lat_all[sp, :, :, pl.ds(rank, LANES)] = (
        jnp.concatenate(key_rot, axis=1).astype(jnp.bfloat16).reshape(4, lat_rows, LANES)
    )

    def prepare_queries(head):
        base = head * (NOPE + ROPE)
        wide_q = q_ref[...].astype(jnp.float32)
        nope = wide_q[:, base : base + NOPE]
        other = jnp.zeros((n_rows, NOPE), jnp.float32)
        rotary = rotate(wide_q[:, base + NOPE : base + NOPE + ROPE], cosine, sine)
        parts = [nope, other] if head % 2 == 0 else [other, nope]
        parts = parts + rotary + [jnp.zeros((n_rows, LANES - ROPE), jnp.float32)]
        q_all[head] = jnp.concatenate(parts, axis=1).astype(jnp.bfloat16)

    def prepare_down():
        count = wd_ref.shape[1]
        across = lax.broadcasted_iota(jnp.int32, (count, count), 1)
        diagonal = (lax.broadcasted_iota(jnp.int32, (count, count), 0) == across).astype(
            jnp.float32
        ).astype(jnp.bfloat16)
        down_all[sp] = dot_nt(diagonal, wd_ref[...]).astype(jnp.bfloat16)

    preparing = [functools.partial(prepare_queries, head) for head in range(head_count)]
    preparing.append(prepare_down)
    pl.semaphore_wait(barrier, 2 + n_tp - 1)

    def origin(hop, direction):
        if direction == 0:
            return ring_device((place + n_sp - hop) % n_sp, n_sp)
        return ring_device((place + hop) % n_sp, n_sp)

    def lat_copy(hop, direction):
        block = lat_all.at[origin(hop - 1, direction), core * 2 + direction]
        return pltpu.make_async_remote_copy(
            src_ref=block,
            dst_ref=block,
            send_sem=lat_send.at[direction],
            recv_sem=lat_recv.at[direction, hop - 1],
            device_id={"sp": targets[direction]},
            device_id_type=MESH,
        )

    def lat_arrival(hop, direction):
        block = lat_all.at[origin(hop, direction), core * 2 + direction]
        return pltpu.make_async_remote_copy(
            src_ref=block,
            dst_ref=block,
            send_sem=lat_send.at[direction],
            recv_sem=lat_recv.at[direction, hop - 1],
            device_id={"sp": targets[direction]},
            device_id_type=MESH,
        )

    def share_copy(hop, direction, which):
        block = lat_all.at[origin(hop, direction), which * 2 + direction]
        return pltpu.make_async_remote_copy(
            src_ref=block,
            dst_ref=block,
            send_sem=share_send.at[direction],
            recv_sem=share_recv.at[direction, hop - 1],
            device_id={"tp": partner},
            device_id_type=MESH,
        )

    piece_rows = wg_ref.shape[0] // (2 * splits)

    def ring_copy(array, piece, hop, direction, arriving):
        block = origin(hop if arriving else hop - 1, direction)
        rows = pl.ds((direction * splits + piece) * piece_rows, piece_rows)
        ref = weights[array].at[block, rows]
        return pltpu.make_async_remote_copy(
            src_ref=ref,
            dst_ref=ref,
            send_sem=ring_send.at[array, piece, direction],
            recv_sem=ring_recv.at[array, piece, direction, hop - 1],
            device_id={"sp": targets[direction]},
            device_id_type=MESH,
        )

    started = set()

    def ring_step(array, piece, hop):
        if hop == 1 and array < 2 and array not in started:
            own[array].wait()
            started.add(array)
        for direction in range(2):
            if hop > 1:
                ring_copy(array, piece, hop - 1, direction, True).wait_recv()
                ring_copy(array, piece, hop - 1, direction, False).wait_send()
            if hop < n_sp:
                ring_copy(array, piece, hop, direction, False).start()

    first = [
        (array, piece, hop)
        for hop in range(1, n_sp)
        for array in range(2)
        for piece in range(splits)
    ]
    second = [(2, piece, hop) for hop in range(1, n_sp) for piece in range(splits)]
    queue = [first + second, 0]

    def advance(count):
        steps, at = queue
        for step in steps[at : at + count]:
            ring_step(*step)
        queue[1] = min(at + count, len(steps))

    unit = max(1, len(first) // 28)

    lat_own.wait()
    for hop in range(1, n_sp + 1):
        for direction in range(2):
            if hop > 1:
                lat_arrival(hop - 1, direction).wait_recv()
                lat_copy(hop - 1, direction).wait_send()
            if hop < n_sp:
                lat_copy(hop, direction).start()
            if hop > 2:
                share_copy(hop - 2, direction, core).wait_send()
            if hop > 1:
                share_copy(hop - 1, direction, core).start()
        if hop < n_sp and queue[1] < 7 * unit:
            advance(1)
        if preparing:
            preparing.pop(0)()
    while preparing:
        preparing.pop(0)()
    for direction in range(2):
        share_copy(n_sp - 1, direction, core).wait_send()
        for hop in range(1, n_sp):
            share_copy(hop, direction, 1 - core).wait_recv()

    total_rows = n_sp * n_rows
    lat_wide = lat_all.shape[3]
    chunk_blocks = max(1, min(n_sp, 1536 // n_rows))
    chunks = n_sp // chunk_blocks
    chunk = chunk_blocks * n_rows
    half_blocks = max(1, chunk_blocks // 2)

    def project(step):
        rows = half_blocks * n_rows
        blocks = pl.ds(step * half_blocks, half_blocks)
        lat = lat_all[blocks, :, :, pl.ds(0, rank)].reshape(rows, rank)
        rotary[pl.ds(step * rows, rows)] = lat_all[blocks, :, :, pl.ds(rank, LANES)].reshape(
            rows, LANES
        )
        keys[pl.ds(step * rows, rows)] = dot(lat, wk_ref[...]).astype(jnp.bfloat16)
        values[pl.ds(step * rows, rows)] = dot(lat, wv_ref[...]).astype(jnp.bfloat16)

    if chunks == 1:
        for step in range(n_sp // half_blocks):
            project(step)
            advance(unit)
    else:
        pl.loop(0, n_sp // half_blocks)(project)
        advance(2 * unit)

    score_scale = (NOPE + ROPE) ** (-0.5)
    lane = lax.broadcasted_iota(jnp.int32, (n_rows, LANES), 1)

    def attend(head, at, state):
        maxima, totals, running = state
        rows = pl.ds(at * chunk, chunk)
        pair = slice(head // 2 * LANES, (head // 2 + 1) * LANES)
        whole_keys = jnp.concatenate([keys[rows, pair], rotary[rows]], axis=1)
        scores = dot_nt(q_all[head], whole_keys) * score_scale
        top = jnp.max(scores, axis=1, keepdims=True)
        if maxima is not None:
            top = jnp.maximum(maxima, top)
        probs = jnp.exp(scores - top)
        sums = jnp.sum(probs, axis=1, keepdims=True)
        update = dot(probs.astype(jnp.bfloat16), values[rows, pair])
        if maxima is not None:
            factor = jnp.exp(maxima - top)
            sums = totals * factor + sums
            update = running * factor + update
        return (top, sums, update)

    for head in range(head_count):
        state = attend(head, 0, (None, None, None))
        if chunks > 1:
            state = lax.fori_loop(1, chunks, functools.partial(attend_loop, attend, head), state)
        result = state[2] / state[1]
        pair = slice(head // 2 * LANES, (head // 2 + 1) * LANES)
        if head % 2 == 0:
            heads[:, pair] = result.astype(jnp.bfloat16)
        else:
            heads[:, pair] = jnp.where(
                lane < VDIM, heads[:, pair].astype(jnp.float32), result
            ).astype(jnp.bfloat16)
        advance(unit)

    def tp_copy(stage, slot_source, slot_target, to, slot_semaphore):
        return pltpu.make_async_remote_copy(
            src_ref=slot_source,
            dst_ref=slot_target,
            send_sem=tp_send.at[stage, slot_semaphore],
            recv_sem=tp_recv.at[stage, slot_semaphore],
            device_id={"tp": to},
            device_id_type=MESH,
        )

    def exchange(stage, source_of, target_of):
        copies = []
        for k in range(1, n_tp):
            to = (tp + k) % n_tp
            copies.append(tp_copy(stage, source_of(to), target_of(k), to, k))
        return copies

    copies = exchange(0, lambda to: part_send.at[to], lambda k: part_recv.at[k])
    for k in range(1, n_tp + 1):
        to = (tp + k) % n_tp
        part_send[to] = dot(
            heads[...], wo_ref[:, pl.ds(pl.multiple_of(to * n_cols, LANES), n_cols)]
        ).astype(jnp.bfloat16)
        if k < n_tp:
            copies[k - 1].start()
    advance(4 * unit)
    mixed = DEEP_ALPHA * resid_ref[...].astype(jnp.float32) + part_send[tp].astype(jnp.float32)
    for k in range(1, n_tp):
        copies[k - 1].wait_recv()
        mixed = mixed + part_recv[k].astype(jnp.float32)
    pending = list(copies)

    width_total = n_cols * n_tp

    def normed(rows_in, gain_ref, stage, send, recv, between):
        sums = jnp.sum(rows_in, axis=1, keepdims=True)
        squares = jnp.sum(rows_in * rows_in, axis=1, keepdims=True)
        mine = jnp.transpose(jnp.where(lane < 4, sums, squares))[:8]
        send[...] = mine
        copies = exchange(stage, lambda to: send, lambda k: recv.at[k])
        for copy in copies:
            copy.start()
        between()
        for k in range(1, n_tp):
            copies[k - 1].wait_recv()
            mine = mine + recv[k]
        pending.extend(copies)
        whole = jnp.transpose(mine) / width_total
        row_mean = whole[:, :1]
        variance = whole[:, 4:5] - row_mean * row_mean
        return (
            (rows_in - row_mean) * lax.rsqrt(variance + NORM_EPSILON) * gain_ref[...]
        ).astype(jnp.bfloat16)

    hidden_in = normed(
        mixed, gain_mix_ref, 1, stat_send, stat_recv, lambda: advance(2 * unit)
    )
    rows_all[tp] = hidden_in
    copies = exchange(2, lambda to: rows_all.at[tp], lambda k: rows_all.at[tp])
    for copy in copies:
        copy.start()
    pending.extend(copies)
    advance(4 * unit)
    for k in range(1, n_tp):
        sender = (tp + n_tp - k) % n_tp
        tp_copy(2, rows_all.at[sender], rows_all.at[sender], sender, k).wait_recv()

    advance(len(first) - queue[1])
    advance(splits)

    def last_hop(array):
        for piece in range(splits):
            for direction in range(2):
                ring_copy(array, piece, n_sp - 1, direction, True).wait_recv()
                ring_copy(array, piece, n_sp - 1, direction, False).wait_send()

    last_hop(0)
    group = n_sp // n_tp
    depth = group * wg_ref.shape[0]
    hidden_width = wg_ref.shape[1]

    def wide(weight):
        total = None
        for t in range(n_tp):
            term = dot(
                rows_all[t],
                weight[t * group : (t + 1) * group].reshape(depth, hidden_width),
            )
            total = term if total is None else total + term
            advance(1)
        return total

    gate_sum = wide(gate_all)
    last_hop(1)
    up_sum = wide(up_all)
    hidden = (gate_sum / (1.0 + jnp.exp(-gate_sum)) * up_sum).astype(jnp.bfloat16)
    advance(1)

    half_rows = piece_rows * splits
    if half_rows % LANES == 0:
        hid[...] = hidden

        def down_copy(k, slot, to, columns):
            ref = part2_send.at[to, :, columns]
            return pltpu.make_async_remote_copy(
                src_ref=ref,
                dst_ref=part2_recv.at[k, :, columns],
                send_sem=down_send.at[k, slot],
                recv_sem=down_recv.at[k, slot],
                device_id={"tp": to},
                device_id_type=MESH,
            )

        def slot_columns(slot):
            return pl.ds(pl.multiple_of(slot * half_rows, LANES), half_rows)

        def make_columns(hop):
            for direction in range(2):
                block = origin(hop, direction)
                owner = block // group
                slot = (block % group) * 2 + direction
                rows = pl.ds(direction * half_rows, half_rows)
                part2_send[owner, :, slot_columns(slot)] = dot_nt(
                    hid[...], down_all[block, rows]
                ).astype(jnp.bfloat16)

                @pl.when(owner != tp)
                def send_away():
                    down_copy((owner + n_tp - tp) % n_tp, slot, owner, slot_columns(slot)).start()

        made = 0
        while queue[1] < len(queue[0]):
            array, piece, hop = queue[0][queue[1]]
            advance(1)
            if piece == splits - 1:
                made_to = hop
                while made < made_to:
                    make_columns(made)
                    made += 1
        while made < n_sp - 1:
            make_columns(made)
            made += 1
        last_hop(2)
        make_columns(n_sp - 1)
        mixer = part2_send[tp].astype(jnp.float32)
        for k in range(1, n_tp):
            for slot in range(2 * group):
                down_copy(k, slot, (tp + k) % n_tp, slot_columns(slot)).wait_recv()
            mixer = mixer + part2_recv[k].astype(jnp.float32)
    else:
        advance(len(queue[0]))
        last_hop(2)
        copies = exchange(3, lambda to: part2_send.at[to], lambda k: part2_recv.at[k])
        for k in range(1, n_tp + 1):
            to = (tp + k) % n_tp
            part2_send[to] = dot_nt(
                hidden, down_all[pl.ds(to * group, group)].reshape(depth, hidden_width)
            ).astype(jnp.bfloat16)
            if k < n_tp:
                copies[k - 1].start()
        mixer = part2_send[tp].astype(jnp.float32)
        for k in range(1, n_tp):
            copies[k - 1].wait_recv()
            mixer = mixer + part2_recv[k].astype(jnp.float32)
        pending.extend(copies)
    final = DEEP_ALPHA * rows_all[tp].astype(jnp.float32) + HALF_STEP * mixer
    out_ref[...] = normed(final, gain_out_ref, 4, stat2_send, stat2_recv, lambda: None)
    for copy in pending:
        copy.wait_send()
    if half_rows % LANES == 0:
        for k in range(1, n_tp):
            for slot in range(2 * group):
                down_copy(k, slot, (tp + k) % n_tp, slot_columns(slot)).wait_send()


def attend_loop(attend, head, at, state):
    return attend(head, at, state)


def flip(value, mask):
    result = value
    bit = 1
    while bit <= mask:
        if mask & bit:
            result = result + bit - 2 * bit * ((value // bit) % 2)
        bit *= 2
    return result


class Semaphores:
    def __init__(self, refs):
        self.refs, self.base, self.used = refs, {}, 0

    def at(self, name, count=1, index=0):
        if name not in self.base:
            self.base[name] = self.used
            self.used += count
        return self.refs.at[self.base[name] + index]


def paired_kernel(
    n_sp,
    n_tp,
    pieces,
    q_in,
    lat_ref,
    rope_in,
    wk_in,
    wv_in,
    wo_ref,
    resid_in,
    gain_mix_in,
    gain_out_in,
    wg_ref,
    wu_ref,
    wd_ref,
    out_ref,
    q_ref,
    rope_ref,
    wk_ref,
    wv_ref,
    resid_ref,
    gain_mix_ref,
    gain_out_ref,
    lat_all,
    keys,
    rotary,
    values,
    q_all,
    heads_all,
    wo_all,
    wide_all,
    down_own,
    down_all,
    rows_all,
    hid,
    summed,
    core_send,
    core_recv,
    far_send,
    far_recv,
    pair_send,
    pair_recv,
    first_send,
    first_recv,
    last_send,
    last_recv,
    total_sum,
    stat_send,
    stat_recv,
    local_sem,
    remote_sem,
):
    sp = lax.axis_index("sp")
    tp = lax.axis_index("tp")
    n_hi = n_sp // 2
    z, x = sp // 2, sp % 2
    half = z % 2
    edge = half == (z // 2) % 2
    inner = jnp.logical_not(edge)
    n_rows = q_ref.shape[0]
    head_count = wk_ref.shape[1] // NOPE
    rank = wk_ref.shape[0]
    lat_rows = lat_all.shape[2]
    n_cols = out_ref.shape[1]
    group = n_sp // n_tp
    depth = wg_ref.shape[0]
    width = wg_ref.shape[1] // 2
    piece_cols = wd_ref.shape[1] // pieces
    local_sems = Semaphores(local_sem)
    remote_sems = Semaphores(remote_sem)

    order = [(1, flip(z, 1))]
    for m in range(2, n_hi, 2):
        low, high = flip(z, m), flip(z, m + 1)
        order.append((jnp.where(edge, m, m + 1), jnp.where(edge, low, high)))
        order.append((jnp.where(edge, m + 1, m), jnp.where(edge, high, low)))
    near, rest = list(range(1, len(order), 2)), list(range(2, len(order), 2))

    def sp_of(place, side):
        return 2 * place + side

    def remote(source, target, device, sent, name, count=1, index=0):
        return pltpu.make_async_remote_copy(
            src_ref=source,
            dst_ref=target,
            send_sem=remote_sems.at(("sent", sent)),
            recv_sem=remote_sems.at(name, count, index),
            device_id=device,
            device_id_type=MESH,
        )

    other_x = 1 - x
    partner, across, corner = flip(tp, 1), flip(tp, 2), flip(tp, 3)
    to_x = {"sp": sp_of(z, other_x)}
    to_pair = {"sp": sp_of(flip(z, 1), x)}
    to_core = {"tp": partner}
    to_across = {"tp": across}

    barrier = pltpu.get_barrier_semaphore()
    peers = [{"sp": sp_of(flip(z, k), x)} for k in range(1, n_hi)] + [to_x]
    peers += [{"tp": flip(tp, j)} for j in range(1, n_tp)]
    for device in peers:
        pl.semaphore_signal(barrier, inc=1, device_id=device, device_id_type=MESH)

    def local(source, target, name):
        return pltpu.make_async_copy(source, target, local_sems.at(name))

    inputs = {
        "rope": local(rope_in, rope_ref, "rope"),
        "q": local(q_in, q_ref, "q"),
        "wk": local(wk_in, wk_ref, "wk"),
        "wv": local(wv_in, wv_ref, "wv"),
        "resid": local(resid_in, resid_ref, "resid"),
        "mix": local(gain_mix_in, gain_mix_ref, "mix"),
        "out": local(gain_out_in, gain_out_ref, "out"),
    }

    wide_rows = depth // pieces

    def wide_source(array, which, piece):
        columns = pl.ds(pl.multiple_of(which * width, LANES), width)
        return (wg_ref, wu_ref)[array].at[pl.ds(piece * wide_rows, wide_rows), columns]

    def wide_block(array, place, side, piece):
        rows = pl.ds(piece * wide_rows, wide_rows)
        return wide_all.at[sp_of(place, side), rows, pl.ds(array * width, width)]

    def down_rows(which, piece):
        rows = pl.ds(pl.multiple_of(which * width, 16), width)
        return wd_ref.at[rows, pl.ds(piece * piece_cols, piece_cols)]

    def down_block(place, side, piece):
        return down_all.at[place * pieces + piece, side]

    def weight_source(array, which, piece):
        if array == 2:
            return down_own.at[which, piece]
        return wide_source(array, which, piece)

    def weight_block(array, place, side, piece):
        if array == 2:
            return down_block(place, side, piece)
        return wide_block(array, place, side, piece)

    def sent_of(array):
        return "down" if array == 2 else "wide"

    def parts_of(array, ref):
        if array < 2:
            return [ref]
        return [ref.at[pl.ds(part * width // 2, width // 2)] for part in range(2)]

    def weight_out(array, k, piece):
        place = flip(z, k)
        sources = parts_of(array, weight_source(array, place % 2, piece))
        targets = parts_of(array, weight_block(array, z, x, piece))
        for part, (source, target) in enumerate(zip(sources, targets)):
            remote(
                source,
                target,
                {"sp": sp_of(place, x)},
                sent_of(array),
                ("wz", array, piece, part),
                n_hi - 1,
                k - 1,
            ).start()

    def weight_side(array, k, place, piece, source=None):
        block = weight_block(array, place, x, piece)
        name = ("wx", piece) if array == 2 else "wx"
        count, index = (n_hi, k) if array == 2 else (1, 0)
        source = block if source is None else source
        remote(source, block, to_x, sent_of(array), name, count, index).start()

    def weight_own(array, piece):
        weight_side(array, 0, z, piece, weight_source(array, half, piece))

    def relay(array, at, piece):
        k, place = order[at]
        name = ("wx", piece) if array == 2 else "wx"
        count, index = (n_hi, k) if array == 2 else (1, 0)
        for part, block in enumerate(parts_of(array, weight_block(array, place, x, piece))):
            remote(
                block,
                block,
                to_x,
                sent_of(array),
                ("wz", array, piece, part),
                n_hi - 1,
                k - 1,
            ).wait_recv()
            remote(block, block, to_x, sent_of(array), name, count, index).start()

    def relay_all(array, at):
        for piece in range(pieces):
            relay(array, at, piece)

    lat_own = local(lat_ref, lat_all.at[sp, :, :, pl.ds(0, rank)], "lat")
    inputs["rope"].start()
    lat_own.start()
    for name in ("q", "wk", "wv", "resid", "mix", "out"):
        inputs[name].start()
    staged = []
    for piece in range(pieces):
        for which in range(2):
            name = ("staged", which, piece)
            staged.append(local(down_rows(which, piece), down_own.at[which, piece], name))
            staged[-1].start()
        for array in range(2):
            local(
                weight_source(array, half, piece), weight_block(array, z, x, piece), "wide"
            ).start()
    down_mine = []
    for piece in range(pieces):
        down_mine.append(
            local(down_rows(half, piece), down_block(z, x, piece), ("down", piece))
        )
        down_mine[-1].start()

    def wo_columns(which):
        return wo_ref.at[:, pl.ds(pl.multiple_of(which * n_cols, LANES), n_cols)]

    wo_own = local(wo_columns(tp), wo_all.at[tp], "wo")
    wo_own.start()
    cosine, sine = rotary_tables(sp * n_rows, n_rows)
    inputs["rope"].wait()
    turned_in = jnp.concatenate(
        [rope_ref[...].astype(jnp.float32), jnp.zeros((LANES - ROPE, n_rows), jnp.float32)],
        axis=0,
    )
    key_rot = rotate(jnp.transpose(turned_in)[:, :ROPE], cosine, sine)
    key_rot.append(jnp.zeros((n_rows, LANES - ROPE), jnp.float32))
    lat_all[sp, :, :, pl.ds(rank, LANES)] = (
        jnp.concatenate(key_rot, axis=1).astype(jnp.bfloat16).reshape(n_tp, lat_rows, LANES)
    )

    def prepare_queries(head):
        base = head * (NOPE + ROPE)
        wide_q = q_ref[...].astype(jnp.float32)
        nope = wide_q[:, base : base + NOPE]
        other = jnp.zeros((n_rows, NOPE), jnp.float32)
        turned = rotate(wide_q[:, base + NOPE : base + NOPE + ROPE], cosine, sine)
        parts = [nope, other] if head % 2 == 0 else [other, nope]
        parts = parts + turned + [jnp.zeros((n_rows, LANES - ROPE), jnp.float32)]
        q_all[head] = jnp.concatenate(parts, axis=1).astype(jnp.bfloat16)

    pl.semaphore_wait(barrier, len(peers))
    lat_own.wait()
    for copy in staged:
        copy.wait()

    def lat_copy(name, k, place, side, quarter, device):
        block = lat_all.at[sp_of(place, side), quarter]
        return remote(block, block, device, "lat", ("lat", name), n_hi, k)

    def lat_core(place, side, quarter):
        block = lat_all.at[sp_of(place, side), quarter]
        remote(block, block, to_core, "lat", "latc").start()

    def lat_z_in(at):
        k, place = order[at]
        lat_copy("z", k, place, x, tp, to_x).wait_recv()
        lat_copy("x", k, place, x, tp, to_x).start()
        lat_copy("y", k, place, x, tp, to_across).start()
        lat_core(place, x, tp)

    def lat_x_in(at):
        k, place = (0, z) if at is None else order[at]
        lat_copy("x", k, place, other_x, tp, to_x).wait_recv()
        lat_copy("yd", k, place, other_x, tp, to_across).start()
        lat_core(place, other_x, tp)

    def lat_y_in(at):
        k, place = order[at]
        lat_copy("y", k, place, x, across, to_across).wait_recv()
        lat_core(place, x, across)

    def lat_yd_in(at):
        k, place = (0, z) if at is None else order[at]
        lat_copy("yd", k, place, other_x, across, to_across).wait_recv()
        lat_core(place, other_x, across)

    for k in range(1, n_hi):
        block = lat_all.at[sp, tp]
        remote(
            block, block, {"sp": sp_of(flip(z, k), x)}, "lat", ("lat", "z"), n_hi, k
        ).start()
    lat_copy("x", 0, z, x, tp, to_x).start()
    weight_own(0, 0)

    far = list(range(2, n_hi))

    def send_near(arrays):
        for array in arrays:
            for piece in range(pieces):
                weight_out(array, 1, piece)

    def send_far(array, which):
        for piece in which:
            for k in far:
                weight_out(array, k, piece)

    every = range(pieces)
    early, late = range(pieces // 2), range(pieces // 2, pieces)

    @pl.when(edge)
    def outer_first():
        send_near((0, 1))
        send_far(0, every)
        send_far(1, early)

    @pl.when(inner)
    def inner_first():
        send_near((0, 1, 2))
        send_far(0, every)
        send_far(1, every)

    inputs["q"].wait()
    prepare_queries(0)
    lat_x_in(None)
    lat_z_in(0)

    prepare_queries(1)
    for piece in range(1, pieces):
        weight_own(0, piece)
    for at in near:
        lat_z_in(at)
    lat_yd_in(None)
    lat_x_in(0)
    lat_y_in(0)
    for at in rest:
        lat_z_in(at)
    for piece in range(pieces):
        weight_own(1, piece)
    for piece in range(pieces):
        weight_own(2, piece)
    for head in range(2, head_count):
        prepare_queries(head)
    for at in near:
        lat_x_in(at)
        lat_y_in(at)
    lat_yd_in(0)
    for at in rest:
        lat_x_in(at)
        lat_y_in(at)
    for j in (2, 3, 1):
        to = flip(tp, j)
        remote(wo_columns(to), wo_all.at[tp], {"tp": to}, "wo", "wo").start()
    for at in near + rest:
        lat_yd_in(at)
    relay_all(0, 0)
    whole = lat_all.at[pl.ds(0, n_sp - 1), pl.ds(0, 2)]
    remote(whole, whole, to_core, "lat", "latc").wait_recv()

    half_blocks = n_sp // 2

    def project(step):
        rows = half_blocks * n_rows
        blocks = pl.ds(step * half_blocks, half_blocks)
        lat = lat_all[blocks, :, :, pl.ds(0, rank)].reshape(rows, rank)
        rotary[pl.ds(step * rows, rows)] = lat_all[blocks, :, :, pl.ds(rank, LANES)].reshape(
            rows, LANES
        )
        keys[pl.ds(step * rows, rows)] = dot(lat, wk_ref[...]).astype(jnp.bfloat16)
        values[pl.ds(step * rows, rows)] = dot(lat, wv_ref[...]).astype(jnp.bfloat16)

    inputs["wk"].wait()
    inputs["wv"].wait()
    for step in range(n_sp // half_blocks):
        project(step)

    score_scale = (NOPE + ROPE) ** (-0.5)
    lane = lax.broadcasted_iota(jnp.int32, (n_rows, LANES), 1)

    for head in range(head_count):
        pair = slice(head // 2 * LANES, (head // 2 + 1) * LANES)
        whole_keys = jnp.concatenate([keys[:, pair], rotary[...]], axis=1)
        scores = dot_nt(q_all[head], whole_keys) * score_scale
        top = jnp.max(scores, axis=1, keepdims=True)
        probs = jnp.exp(scores - top)
        sums = jnp.sum(probs, axis=1, keepdims=True)
        result = dot(probs.astype(jnp.bfloat16), values[:, pair]) / sums
        if head % 2 == 0:
            held = result
        else:
            heads_all[tp, :, pair] = jnp.where(lane < VDIM, held, result).astype(jnp.bfloat16)
            block = heads_all.at[tp, :, pl.ds(head // 2 * LANES, LANES)]
            for j in (2, 3, 1):
                remote(block, block, {"tp": flip(tp, j)}, "heads", "heads").start()
        if head == head_count // 2 - 1:
            relay_all(1, 0)
    for at in near:
        relay_all(0, at)
    for name in ("resid", "mix", "out"):
        inputs[name].wait()
    mixed = DEEP_ALPHA * resid_ref[...].astype(jnp.float32)
    wo_own.wait()
    mixed = mixed + dot(heads_all[tp], wo_all[tp])
    others = pl.ds(0, n_tp - 1)
    remote(wo_all.at[others], wo_all.at[others], to_core, "wo", "wo").wait_recv()
    remote(heads_all.at[others], heads_all.at[others], to_core, "heads", "heads").wait_recv()
    for j in (1, 2, 3):
        sender = flip(tp, j)
        mixed = mixed + dot(heads_all[sender], wo_all[sender])

    width_total = n_cols * n_tp

    def normed(rows_in, gain_ref, stage, between):
        sums = jnp.sum(rows_in, axis=1, keepdims=True)
        squares = jnp.sum(rows_in * rows_in, axis=1, keepdims=True)
        mine = jnp.transpose(jnp.where(lane < 4, sums, squares))[:8]
        stat_send[stage] = mine
        for j in (2, 3, 1):
            remote(
                stat_send.at[stage],
                stat_recv.at[stage, j - 1],
                {"tp": flip(tp, j)},
                ("stat", stage),
                ("stat", stage),
            ).start()
        between()
        arrived = stat_recv.at[stage]
        remote(arrived, arrived, to_core, ("stat", stage), ("stat", stage)).wait_recv()
        for j in (1, 2, 3):
            mine = mine + stat_recv[stage, j - 1]
        whole = jnp.transpose(mine) / width_total
        row_mean = whole[:, :1]
        variance = whole[:, 4:5] - row_mean * row_mean
        return (
            (rows_in - row_mean) * lax.rsqrt(variance + NORM_EPSILON) * gain_ref[...]
        ).astype(jnp.bfloat16)

    def more_wide():
        for at in rest:
            relay_all(0, at)

    hidden_in = normed(mixed, gain_mix_ref, 0, more_wide)
    mine = pl.ds(pl.multiple_of(half * n_rows, 16), n_rows)
    theirs = pl.ds(pl.multiple_of((1 - half) * n_rows, 16), n_rows)
    rows_all[tp, mine] = hidden_in

    def rows_copy(name, owner, rows, device):
        block = rows_all.at[owner, rows]
        return remote(block, block, device, "rows", ("rows", name))

    def rows_core(owner, rows):
        block = rows_all.at[owner, rows]
        remote(block, block, to_core, "rowsc", "rowsc").start()

    rows_copy("y", tp, mine, to_across).start()
    rows_copy("z", tp, mine, to_pair).start()
    rows_core(tp, mine)

    @pl.when(edge)
    def outer_last():
        send_far(1, late)
        send_near((2,))
        send_far(2, every)

    @pl.when(inner)
    def inner_last():
        send_far(2, every)

    for at in near:
        relay_all(1, at)
    for at in rest:
        for piece in early:
            relay(1, at, piece)
    rows_copy("z", tp, theirs, to_pair).wait_recv()
    rows_copy("yz", tp, theirs, to_across).start()
    rows_core(tp, theirs)
    rows_copy("y", across, mine, to_across).wait_recv()
    rows_core(across, mine)
    for at in rest:
        for piece in late:
            relay(1, at, piece)

    @pl.when(edge)
    def outer_first_down():
        relay_all(2, 0)
        for at in near:
            for piece in early:
                relay(2, at, piece)

    rows_copy("yz", across, theirs, to_across).wait_recv()
    rows_core(across, theirs)

    @pl.when(inner)
    def inner_first_down():
        relay_all(2, 0)

    @pl.when(inner)
    def inner_near_down():
        for at in near:
            for piece in early:
                relay(2, at, piece)

    both = rows_all.at[pl.ds(0, 2)]
    remote(both, both, to_core, "rowsc", "rowsc").wait_recv()
    local(wg_ref, wide_all.at[0], "wide").wait()
    arrived = wide_all.at[pl.ds(0, n_hi)]
    remote(arrived, arrived, to_x, "wide", "wx").wait_recv()

    total = None
    for t in range(n_tp):
        term = dot(
            rows_all[t], wide_all[t * group : (t + 1) * group].reshape(group * depth, 2 * width)
        )
        total = term if total is None else total + term
    gate_sum, up_sum = total[:, :width], total[:, width:]
    hid[...] = (gate_sum / (1.0 + jnp.exp(-gate_sum)) * up_sum).astype(jnp.bfloat16)
    for copy in down_mine:
        copy.wait()

    def facts(at, piece):
        k, place = (0, z) if at is None else order[at]
        unit = place * pieces + piece
        return k, place, unit, tp % 2 == place % 2, tp // 2 == place // 2

    def core_copy(place, unit, piece):
        return remote(
            core_send.at[unit],
            core_recv.at[unit],
            to_core,
            "core",
            "core",
            n_tp // 2 * pieces,
            place // 2 * pieces + piece,
        )

    def far_copy(piece):
        return remote(
            far_send.at[piece], far_recv.at[piece], to_across, "far", "far", pieces, piece
        )

    def pair_copy(piece):
        return remote(
            pair_send.at[piece], pair_recv.at[piece], to_pair, "pair", "pair", pieces, piece
        )

    def pair_first_copy(piece):
        source, target = first_send.at[piece], first_recv.at[piece]
        return remote(source, target, to_pair, "first", "first", pieces + 1, piece)

    def far_last_copy(piece):
        source, target = last_send.at[piece], last_recv.at[piece]
        return remote(source, target, to_across, "last", "last", pieces + 1, piece)

    def make_block(at, piece):
        k, place, unit, same_core, same_chip = facts(at, piece)
        block = down_block(place, other_x, piece)
        remote(block, block, to_x, "down", ("wx", piece), n_hi, k).wait_recv()
        columns = jnp.concatenate([down_all[unit, 0], down_all[unit, 1]], axis=1)
        product = dot(hid[...], columns)

        @pl.when(same_core)
        def keep():
            summed[unit] = product

        @pl.when(jnp.logical_not(same_core))
        def give():
            core_send[unit] = product.astype(jnp.bfloat16)
            core_copy(place, unit, piece).start()

    def add_core(at, piece):
        k, place, unit, same_core, same_chip = facts(at, piece)

        @pl.when(same_core)
        def add():
            core_copy(place, unit, piece).wait_recv()
            both = summed[unit] + core_recv[unit].astype(jnp.float32)

            @pl.when(same_chip)
            def keep():
                summed[unit] = both

            @pl.when(jnp.logical_not(same_chip))
            def give():
                far_send[piece] = both.astype(jnp.bfloat16)
                far_copy(piece).start()

    def add_far(at, piece):
        k, place, unit, same_core, same_chip = facts(at, piece)

        @pl.when(place == tp)
        def add():
            far_copy(piece).wait_recv()
            summed[unit, mine] = summed[unit, mine] + far_recv[piece, mine].astype(jnp.float32)
            pair_send[piece] = (
                summed[unit, theirs] + far_recv[piece, theirs].astype(jnp.float32)
            ).astype(jnp.bfloat16)
            pair_copy(piece).start()

    def slot_of(at, piece):
        return pieces if at is None or at == 0 else piece

    def pair_first(at, piece):
        k, place, unit, same_core, same_chip = facts(at, piece)
        slot = slot_of(at, piece)

        @pl.when(same_core)
        def add():
            core_copy(place, unit, piece).wait_recv()
            first_send[slot] = (
                summed[unit, theirs] + core_recv[unit, theirs].astype(jnp.float32)
            ).astype(jnp.bfloat16)
            pair_first_copy(slot).start()

    def pair_added(at, piece):
        k, place, unit, same_core, same_chip = facts(at, piece)
        slot = slot_of(at, piece)

        @pl.when(same_core)
        def add():
            pair_first_copy(slot).wait_recv()
            both = summed[unit, mine] + core_recv[unit, mine].astype(jnp.float32)
            both = both + first_recv[slot].astype(jnp.float32)

            @pl.when(same_chip)
            def keep():
                total_sum[slot] = both

            @pl.when(jnp.logical_not(same_chip))
            def give():
                last_send[slot] = both.astype(jnp.bfloat16)
                far_last_copy(slot).start()

    def finish_far(at, piece):
        k, place, unit, same_core, same_chip = facts(at, piece)
        slot = slot_of(at, piece)

        @pl.when(place == tp)
        def add():
            far_last_copy(slot).wait_recv()
            total_sum[piece] = total_sum[slot] + last_recv[slot].astype(jnp.float32)

    def finish_pair(at, piece):
        k, place, unit, same_core, same_chip = facts(at, piece)

        @pl.when(place == tp)
        def add():
            pair_copy(piece).wait_recv()
            total_sum[piece] = summed[unit, mine] + pair_recv[piece].astype(jnp.float32)

    def each(apply, ats, which):
        for piece in which:
            for at in ats:
                apply(at, piece)

    close = [None, 0]
    each(make_block, close, every)
    each(functools.partial(relay, 2), rest, early)
    each(add_core, close, early)
    each(pair_first, close, late)
    each(make_block, near, early)
    each(functools.partial(relay, 2), rest, late)
    each(make_block, rest, early)
    each(functools.partial(relay, 2), near, late)
    each(pair_first, near + rest, early)
    each(make_block, rest, late)
    each(pair_added, close, late)
    each(make_block, near, late)
    each(pair_first, rest + near, late)
    each(add_far, close, early)
    each(pair_added, near + rest, early)
    each(pair_added, rest + near, late)
    each(finish_far, close, late)
    each(finish_pair, close, early)
    each(finish_far, near + rest, every)
    final = [total_sum[piece] for piece in range(pieces)]
    sides = []
    for side in range(2):
        for piece in range(pieces):
            sides.append(final[piece][:, side * piece_cols : (side + 1) * piece_cols])
    mixer = jnp.concatenate(sides, axis=1)
    last_in = DEEP_ALPHA * rows_all[tp, mine].astype(jnp.float32) + HALF_STEP * mixer
    out_ref[...] = normed(last_in, gain_out_ref, 1, lambda: None)

    def all_sent(sent, name, whole):
        remote(whole, whole, to_core, sent, name).wait_send()

    all_sent("lat", "latc", lat_all.at[pl.ds(0, n_sp - 1)])
    all_sent("wide", "wx", wide_all.at[pl.ds(0, n_sp - 1)])
    all_sent("down", "wx", down_all.at[pl.ds(0, (n_sp - 1) * pieces // 2)])
    all_sent("wo", "wo", wo_all.at[others])
    all_sent("heads", "heads", heads_all.at[others])
    all_sent("rows", ("rows", "z"), rows_all.at[others, pl.ds(0, n_rows)])
    all_sent("rowsc", "rowsc", both)
    for stage in range(2):
        all_sent(("stat", stage), ("stat", stage), stat_recv.at[stage])
    all_sent("core", "core", core_send.at[pl.ds(0, n_hi * pieces // 2)])
    all_sent("first", "first", first_send)
    home = tp // 2 == z // 2
    early_rows = pl.ds(0, pieces // 2)

    @pl.when(home)
    def sent_home():
        all_sent("pair", "pair", pair_send.at[early_rows])
        all_sent("last", "last", last_send.at[pl.ds(0, pieces)])

    @pl.when(jnp.logical_not(home))
    def sent_away():
        all_sent("far", "far", far_send.at[early_rows])
        all_sent("last", "last", last_send.at[early_rows])


def paired_call(n_sp, n_tp, operands):
    queries, latents, rope_key, w_key, w_value, w_out, resid, gain_mix = operands[:8]
    w_gate, w_up, w_down, gain_out = operands[8:]
    rows = queries.shape[0]
    head_count = w_key.shape[1] // NOPE
    rank = latents.shape[1]
    cols = resid.shape[1]
    depth, hidden_width = w_gate.shape
    width = hidden_width // 2
    pieces = 2
    n_hi = n_sp // 2
    unit_cols = 2 * w_down.shape[1] // pieces
    total_rows = n_sp * rows
    bf16 = jnp.bfloat16
    f32 = jnp.float32
    vmem = pl.BlockSpec(memory_space=pltpu.VMEM)
    anywhere = pl.BlockSpec(memory_space=pl.ANY)
    dma = pltpu.SemaphoreType.DMA
    signals = 4 * n_hi + 4 * (n_hi - 1) * pieces + n_hi * pieces
    signals += (n_tp // 2 + 4) * pieces + 26
    return pl.pallas_call(
        functools.partial(paired_kernel, n_sp, n_tp, pieces),
        out_shape=pltpu.VMEM((rows, cols), bf16),
        in_specs=[anywhere] * 12,
        out_specs=vmem,
        scratch_shapes=[
            pltpu.VMEM(queries.shape, bf16),
            pltpu.VMEM((rope_key.shape[1], rows), bf16),
            pltpu.VMEM(w_key.shape, bf16),
            pltpu.VMEM(w_value.shape, bf16),
            pltpu.VMEM(resid.shape, bf16),
            pltpu.VMEM((1, cols), f32),
            pltpu.VMEM((1, cols), f32),
            pltpu.VMEM((n_sp, n_tp, rows // n_tp, rank + LANES), bf16),
            pltpu.VMEM((total_rows, head_count * NOPE), bf16),
            pltpu.VMEM((total_rows, LANES), bf16),
            pltpu.VMEM((total_rows, head_count * VDIM), bf16),
            pltpu.VMEM((head_count, rows, 2 * LANES), bf16),
            pltpu.VMEM((n_tp, rows, head_count * VDIM), bf16),
            pltpu.VMEM((n_tp, head_count * VDIM, cols), bf16),
            pltpu.VMEM((n_sp, depth, 2 * width), bf16),
            pltpu.VMEM((2, pieces, width, unit_cols // 2), bf16),
            pltpu.VMEM((n_hi * pieces, 2, width, unit_cols // 2), bf16),
            pltpu.VMEM((n_tp, 2 * rows, cols), bf16),
            pltpu.VMEM((2 * rows, width), bf16),
            pltpu.VMEM((n_hi * pieces, 2 * rows, unit_cols), f32),
            pltpu.VMEM((n_hi * pieces, 2 * rows, unit_cols), bf16),
            pltpu.VMEM((n_hi * pieces, 2 * rows, unit_cols), bf16),
            pltpu.VMEM((pieces, 2 * rows, unit_cols), bf16),
            pltpu.VMEM((pieces, 2 * rows, unit_cols), bf16),
            pltpu.VMEM((pieces, rows, unit_cols), bf16),
            pltpu.VMEM((pieces, rows, unit_cols), bf16),
            pltpu.VMEM((pieces + 1, rows, unit_cols), bf16),
            pltpu.VMEM((pieces + 1, rows, unit_cols), bf16),
            pltpu.VMEM((pieces + 1, rows, unit_cols), bf16),
            pltpu.VMEM((pieces + 1, rows, unit_cols), bf16),
            pltpu.VMEM((pieces + 1, rows, unit_cols), f32),
            pltpu.VMEM((2, 8, rows), f32),
            pltpu.VMEM((2, n_tp - 1, 8, rows), f32),
            dma((10 + 3 * pieces,)),
            dma((signals,)),
        ],
        compiler_params=pltpu.CompilerParams(
            collective_id=1, has_side_effects=True, vmem_limit_bytes=66000000
        ),
    )(
        queries,
        latents.reshape(n_tp, rows // n_tp, rank),
        rope_key.T,
        w_key,
        w_value,
        w_out,
        resid,
        gain_mix.reshape(1, -1),
        gain_out.reshape(1, -1),
        w_gate,
        w_up,
        w_down,
    )


def fits_pairs(n_sp, n_tp, operands):
    queries, w_key, w_gate, w_down = operands[0], operands[3], operands[8], operands[10]
    return (
        n_tp == 4
        and n_sp == 2 * n_tp
        and queries.shape[0] % 64 == 0
        and n_sp * queries.shape[0] <= 1536
        and (w_key.shape[1] // NOPE) % 2 == 0
        and w_gate.shape[1] % (2 * LANES) == 0
        and w_gate.shape[0] % 32 == 0
        and w_down.shape[1] % (2 * LANES) == 0
    )


def local(
    queries,
    latents,
    rope_key,
    w_key,
    w_value,
    w_out,
    resid,
    gain_mix,
    w_gate,
    w_up,
    w_down,
    gain_out,
):
    n_sp = lax.axis_size("sp")
    n_tp = lax.axis_size("tp")
    operands = (queries, latents, rope_key, w_key, w_value, w_out, resid, gain_mix)
    operands += (w_gate, w_up, w_down, gain_out)
    if fits_pairs(n_sp, n_tp, operands):
        return paired_call(n_sp, n_tp, operands)
    rows = queries.shape[0]
    head_count = w_key.shape[1] // NOPE
    rank = latents.shape[1]
    cols = resid.shape[1]
    hidden_width = w_gate.shape[1]
    weight_rows = w_gate.shape[0]
    lat_wide = rank + LANES
    splits = 2 if weight_rows % 64 == 0 else 1
    bf16 = jnp.bfloat16
    total_rows = n_sp * rows
    vmem = pl.BlockSpec(memory_space=pltpu.VMEM)
    anywhere = pl.BlockSpec(memory_space=pl.ANY)
    dma = pltpu.SemaphoreType.DMA
    return pl.pallas_call(
        functools.partial(layer_kernel, n_sp, n_tp, splits),
        out_shape=jax.ShapeDtypeStruct((rows, cols), bf16),
        in_specs=[vmem, anywhere] + [vmem] * 7 + [anywhere] * 2 + [vmem],
        out_specs=vmem,
        scratch_shapes=[
            pltpu.VMEM((n_sp, 4, rows // 4, lat_wide), bf16),
            pltpu.VMEM((total_rows, head_count * NOPE), bf16),
            pltpu.VMEM((total_rows, LANES), bf16),
            pltpu.VMEM((total_rows, head_count * VDIM), bf16),
            pltpu.VMEM((n_sp, weight_rows, hidden_width), bf16),
            pltpu.VMEM((n_sp, weight_rows, hidden_width), bf16),
            pltpu.VMEM((n_sp, weight_rows, hidden_width), bf16),
            pltpu.VMEM((head_count, rows, 2 * LANES), bf16),
            pltpu.VMEM((rows, head_count * VDIM), bf16),
            pltpu.VMEM((n_tp, rows, cols), bf16),
            pltpu.VMEM((n_tp, rows, cols), bf16),
            pltpu.VMEM((8, rows), jnp.float32),
            pltpu.VMEM((n_tp, 8, rows), jnp.float32),
            pltpu.VMEM((n_tp, rows, cols), bf16),
            pltpu.VMEM((n_tp, rows, cols), bf16),
            pltpu.VMEM((n_tp, rows, cols), bf16),
            pltpu.VMEM((8, rows), jnp.float32),
            pltpu.VMEM((n_tp, 8, rows), jnp.float32),
            pltpu.VMEM((rows, hidden_width), bf16),
            dma((4,)),
            dma((2,)),
            dma((2, n_sp - 1)),
            dma((2,)),
            dma((2, n_sp - 1)),
            dma((3, splits, 2)),
            dma((3, splits, 2, n_sp - 1)),
            dma((5, n_tp)),
            dma((5, n_tp)),
            dma((n_tp, 2 * (n_sp // n_tp))),
            dma((n_tp, 2 * (n_sp // n_tp))),
        ],
        compiler_params=pltpu.CompilerParams(
            collective_id=0, has_side_effects=True, vmem_limit_bytes=66000000
        ),
    )(
        queries,
        latents.reshape(4, rows // 4, rank),
        rope_key,
        w_key,
        w_value,
        w_out,
        resid,
        gain_mix.reshape(1, -1),
        gain_out.reshape(1, -1),
        w_gate,
        w_up,
        w_down,
    )


def solution(mesh):
    placed = (
        P("sp", "tp"),
        P("sp", None),
        P("sp", None),
        P(None, "tp"),
        P(None, "tp"),
        P("tp", None),
        P("sp", "tp"),
        P("tp"),
        P("sp", "tp"),
        P("sp", "tp"),
        P("tp", "sp"),
        P("tp"),
    )
    return jax.shard_map(
        local, mesh=mesh, in_specs=placed, out_specs=P("sp", "tp"), check_vma=False
    )
```

```python
import functools

import jax
import jax.numpy as jnp
from jax import lax
from jax.experimental import pallas as pl
from jax.experimental.pallas import tpu as pltpu
from jax.sharding import PartitionSpec as P

NOPE = 64
ROPE = 32
VDIM = 64
GRID_W = 64
LANES = 128

ROTARY_BASE = 10000.0
NORM_EPSILON = 1e-06
DEEP_ALPHA = 8.0**0.25
HALF_STEP = 0.5
MESH = pl.DeviceIdType.MESH


def rotary_tables(first, rows):
    at = first + lax.broadcasted_iota(jnp.int32, (rows, LANES), 0)
    column = lax.broadcasted_iota(jnp.int32, (rows, LANES), 1)
    freq_count = ROPE // 4
    grid_row = (at // GRID_W).astype(jnp.float32)
    grid_col = (at % GRID_W).astype(jnp.float32)
    spot = jnp.where(column % (2 * freq_count) < freq_count, grid_row, grid_col)
    inverse = jnp.ones((rows, LANES), jnp.float32)
    for k in range(1, freq_count):
        inverse = jnp.where(column % freq_count == k, ROTARY_BASE ** (-k / freq_count), inverse)
    angles = spot * inverse
    return (jnp.cos(angles)[:, : ROPE // 2], jnp.sin(angles)[:, : ROPE // 2])


def rotate(vectors, cosine, sine):
    half_width = ROPE // 2
    leading = vectors[:, :half_width]
    trailing = vectors[:, half_width:]
    return [leading * cosine - trailing * sine, leading * sine + trailing * cosine]


def ring_device(place, count):
    return jnp.where(place < count // 2, 2 * place, 2 * (count - 1 - place) + 1)


def ring_place(index, count):
    return jnp.where(index % 2 == 0, index // 2, count - 1 - index // 2)


def dot(left, right):
    return jnp.dot(left, right, preferred_element_type=jnp.float32)


def dot_nt(left, right):
    return lax.dot_general(
        left, right, (((1,), (1,)), ((), ())), preferred_element_type=jnp.float32
    )


def layer_kernel(
    n_sp,
    n_tp,
    splits,
    q_ref,
    lat_ref,
    rope_ref,
    wk_ref,
    wv_ref,
    wo_ref,
    resid_ref,
    gain_mix_ref,
    gain_out_ref,
    wg_ref,
    wu_ref,
    wd_ref,
    out_ref,
    lat_all,
    keys,
    rotary,
    values,
    gate_all,
    up_all,
    down_all,
    q_all,
    heads,
    part_send,
    part_recv,
    stat_send,
    stat_recv,
    rows_all,
    part2_send,
    part2_recv,
    stat2_send,
    stat2_recv,
    hid,
    local_sem,
    lat_send,
    lat_recv,
    share_send,
    share_recv,
    ring_send,
    ring_recv,
    tp_send,
    tp_recv,
    down_send,
    down_recv,
):
    sp = lax.axis_index("sp")
    tp = lax.axis_index("tp")
    place = ring_place(sp, n_sp)
    ahead = ring_device((place + 1) % n_sp, n_sp)
    behind = ring_device((place + n_sp - 1) % n_sp, n_sp)
    targets = (ahead, behind)
    partner = tp + 1 - 2 * (tp % 2)
    core = tp % 2
    n_rows = q_ref.shape[0]
    head_count = wk_ref.shape[1] // NOPE
    rank = wk_ref.shape[0]
    lat_rows = lat_all.shape[2]
    n_cols = out_ref.shape[1]

    barrier = pltpu.get_barrier_semaphore()
    for device in targets:
        pl.semaphore_signal(barrier, inc=1, device_id={"sp": device}, device_id_type=MESH)
    for step in range(1, n_tp):
        pl.semaphore_signal(
            barrier, inc=1, device_id={"tp": (tp + step) % n_tp}, device_id_type=MESH
        )

    own = []
    lat_own = pltpu.make_async_copy(
        lat_ref, lat_all.at[sp, :, :, pl.ds(0, rank)], local_sem.at[0]
    )
    lat_own.start()
    weights = (gate_all, up_all, down_all)
    for i, source in enumerate((wg_ref, wu_ref)):
        copy = pltpu.make_async_copy(source, weights[i].at[sp], local_sem.at[i + 1])
        copy.start()
        own.append(copy)
    cosine, sine = rotary_tables(sp * n_rows, n_rows)
    key_rot = rotate(rope_ref[...].astype(jnp.float32), cosine, sine)
    key_rot.append(jnp.zeros((n_rows, LANES - ROPE), jnp.float32))
    lat_all[sp, :, :, pl.ds(rank, LANES)] = (
        jnp.concatenate(key_rot, axis=1).astype(jnp.bfloat16).reshape(4, lat_rows, LANES)
    )

    def prepare_queries(head):
        base = head * (NOPE + ROPE)
        wide_q = q_ref[...].astype(jnp.float32)
        nope = wide_q[:, base : base + NOPE]
        other = jnp.zeros((n_rows, NOPE), jnp.float32)
        rotary = rotate(wide_q[:, base + NOPE : base + NOPE + ROPE], cosine, sine)
        parts = [nope, other] if head % 2 == 0 else [other, nope]
        parts = parts + rotary + [jnp.zeros((n_rows, LANES - ROPE), jnp.float32)]
        q_all[head] = jnp.concatenate(parts, axis=1).astype(jnp.bfloat16)

    def prepare_down():
        count = wd_ref.shape[1]
        across = lax.broadcasted_iota(jnp.int32, (count, count), 1)
        diagonal = (lax.broadcasted_iota(jnp.int32, (count, count), 0) == across).astype(
            jnp.float32
        ).astype(jnp.bfloat16)
        down_all[sp] = dot_nt(diagonal, wd_ref[...]).astype(jnp.bfloat16)

    preparing = [functools.partial(prepare_queries, head) for head in range(head_count)]
    preparing.append(prepare_down)
    pl.semaphore_wait(barrier, 2 + n_tp - 1)

    def origin(hop, direction):
        if direction == 0:
            return ring_device((place + n_sp - hop) % n_sp, n_sp)
        return ring_device((place + hop) % n_sp, n_sp)

    def lat_copy(hop, direction):
        block = lat_all.at[origin(hop - 1, direction), core * 2 + direction]
        return pltpu.make_async_remote_copy(
            src_ref=block,
            dst_ref=block,
            send_sem=lat_send.at[direction],
            recv_sem=lat_recv.at[direction, hop - 1],
            device_id={"sp": targets[direction]},
            device_id_type=MESH,
        )

    def lat_arrival(hop, direction):
        block = lat_all.at[origin(hop, direction), core * 2 + direction]
        return pltpu.make_async_remote_copy(
            src_ref=block,
            dst_ref=block,
            send_sem=lat_send.at[direction],
            recv_sem=lat_recv.at[direction, hop - 1],
            device_id={"sp": targets[direction]},
            device_id_type=MESH,
        )

    def share_copy(hop, direction, which):
        block = lat_all.at[origin(hop, direction), which * 2 + direction]
        return pltpu.make_async_remote_copy(
            src_ref=block,
            dst_ref=block,
            send_sem=share_send.at[direction],
            recv_sem=share_recv.at[direction, hop - 1],
            device_id={"tp": partner},
            device_id_type=MESH,
        )

    piece_rows = wg_ref.shape[0] // (2 * splits)

    def ring_copy(array, piece, hop, direction, arriving):
        block = origin(hop if arriving else hop - 1, direction)
        rows = pl.ds((direction * splits + piece) * piece_rows, piece_rows)
        ref = weights[array].at[block, rows]
        return pltpu.make_async_remote_copy(
            src_ref=ref,
            dst_ref=ref,
            send_sem=ring_send.at[array, piece, direction],
            recv_sem=ring_recv.at[array, piece, direction, hop - 1],
            device_id={"sp": targets[direction]},
            device_id_type=MESH,
        )

    started = set()

    def ring_step(array, piece, hop):
        if hop == 1 and array < 2 and array not in started:
            own[array].wait()
            started.add(array)
        for direction in range(2):
            if hop > 1:
                ring_copy(array, piece, hop - 1, direction, True).wait_recv()
                ring_copy(array, piece, hop - 1, direction, False).wait_send()
            if hop < n_sp:
                ring_copy(array, piece, hop, direction, False).start()

    first = [
        (array, piece, hop)
        for hop in range(1, n_sp)
        for array in range(2)
        for piece in range(splits)
    ]
    second = [(2, piece, hop) for hop in range(1, n_sp) for piece in range(splits)]
    queue = [first + second, 0]

    def advance(count):
        steps, at = queue
        for step in steps[at : at + count]:
            ring_step(*step)
        queue[1] = min(at + count, len(steps))

    unit = max(1, len(first) // 28)

    lat_own.wait()
    for hop in range(1, n_sp + 1):
        for direction in range(2):
            if hop > 1:
                lat_arrival(hop - 1, direction).wait_recv()
                lat_copy(hop - 1, direction).wait_send()
            if hop < n_sp:
                lat_copy(hop, direction).start()
            if hop > 2:
                share_copy(hop - 2, direction, core).wait_send()
            if hop > 1:
                share_copy(hop - 1, direction, core).start()
        if hop < n_sp and queue[1] < 7 * unit:
            advance(1)
        if preparing:
            preparing.pop(0)()
    while preparing:
        preparing.pop(0)()
    for direction in range(2):
        share_copy(n_sp - 1, direction, core).wait_send()
        for hop in range(1, n_sp):
            share_copy(hop, direction, 1 - core).wait_recv()

    total_rows = n_sp * n_rows
    lat_wide = lat_all.shape[3]
    chunk_blocks = max(1, min(n_sp, 1536 // n_rows))
    chunks = n_sp // chunk_blocks
    chunk = chunk_blocks * n_rows
    half_blocks = max(1, chunk_blocks // 2)

    def project(step):
        rows = half_blocks * n_rows
        blocks = pl.ds(step * half_blocks, half_blocks)
        lat = lat_all[blocks, :, :, pl.ds(0, rank)].reshape(rows, rank)
        rotary[pl.ds(step * rows, rows)] = lat_all[blocks, :, :, pl.ds(rank, LANES)].reshape(
            rows, LANES
        )
        keys[pl.ds(step * rows, rows)] = dot(lat, wk_ref[...]).astype(jnp.bfloat16)
        values[pl.ds(step * rows, rows)] = dot(lat, wv_ref[...]).astype(jnp.bfloat16)

    if chunks == 1:
        for step in range(n_sp // half_blocks):
            project(step)
            advance(unit)
    else:
        pl.loop(0, n_sp // half_blocks)(project)
        advance(2 * unit)

    score_scale = (NOPE + ROPE) ** (-0.5)
    lane = lax.broadcasted_iota(jnp.int32, (n_rows, LANES), 1)

    def attend(head, at, state):
        maxima, totals, running = state
        rows = pl.ds(at * chunk, chunk)
        pair = slice(head // 2 * LANES, (head // 2 + 1) * LANES)
        whole_keys = jnp.concatenate([keys[rows, pair], rotary[rows]], axis=1)
        scores = dot_nt(q_all[head], whole_keys) * score_scale
        top = jnp.max(scores, axis=1, keepdims=True)
        if maxima is not None:
            top = jnp.maximum(maxima, top)
        probs = jnp.exp(scores - top)
        sums = jnp.sum(probs, axis=1, keepdims=True)
        update = dot(probs.astype(jnp.bfloat16), values[rows, pair])
        if maxima is not None:
            factor = jnp.exp(maxima - top)
            sums = totals * factor + sums
            update = running * factor + update
        return (top, sums, update)

    for head in range(head_count):
        state = attend(head, 0, (None, None, None))
        if chunks > 1:
            state = lax.fori_loop(1, chunks, functools.partial(attend_loop, attend, head), state)
        result = state[2] / state[1]
        pair = slice(head // 2 * LANES, (head // 2 + 1) * LANES)
        if head % 2 == 0:
            heads[:, pair] = result.astype(jnp.bfloat16)
        else:
            heads[:, pair] = jnp.where(
                lane < VDIM, heads[:, pair].astype(jnp.float32), result
            ).astype(jnp.bfloat16)
        advance(unit)

    def tp_copy(stage, slot_source, slot_target, to, slot_semaphore):
        return pltpu.make_async_remote_copy(
            src_ref=slot_source,
            dst_ref=slot_target,
            send_sem=tp_send.at[stage, slot_semaphore],
            recv_sem=tp_recv.at[stage, slot_semaphore],
            device_id={"tp": to},
            device_id_type=MESH,
        )

    def exchange(stage, source_of, target_of):
        copies = []
        for k in range(1, n_tp):
            to = (tp + k) % n_tp
            copies.append(tp_copy(stage, source_of(to), target_of(k), to, k))
        return copies

    copies = exchange(0, lambda to: part_send.at[to], lambda k: part_recv.at[k])
    for k in range(1, n_tp + 1):
        to = (tp + k) % n_tp
        part_send[to] = dot(
            heads[...], wo_ref[:, pl.ds(pl.multiple_of(to * n_cols, LANES), n_cols)]
        ).astype(jnp.bfloat16)
        if k < n_tp:
            copies[k - 1].start()
    advance(4 * unit)
    mixed = DEEP_ALPHA * resid_ref[...].astype(jnp.float32) + part_send[tp].astype(jnp.float32)
    for k in range(1, n_tp):
        copies[k - 1].wait_recv()
        mixed = mixed + part_recv[k].astype(jnp.float32)
    pending = list(copies)

    width_total = n_cols * n_tp

    def normed(rows_in, gain_ref, stage, send, recv, between):
        sums = jnp.sum(rows_in, axis=1, keepdims=True)
        squares = jnp.sum(rows_in * rows_in, axis=1, keepdims=True)
        mine = jnp.transpose(jnp.where(lane < 4, sums, squares))[:8]
        send[...] = mine
        copies = exchange(stage, lambda to: send, lambda k: recv.at[k])
        for copy in copies:
            copy.start()
        between()
        for k in range(1, n_tp):
            copies[k - 1].wait_recv()
            mine = mine + recv[k]
        pending.extend(copies)
        whole = jnp.transpose(mine) / width_total
        row_mean = whole[:, :1]
        variance = whole[:, 4:5] - row_mean * row_mean
        return (
            (rows_in - row_mean) * lax.rsqrt(variance + NORM_EPSILON) * gain_ref[...]
        ).astype(jnp.bfloat16)

    hidden_in = normed(
        mixed, gain_mix_ref, 1, stat_send, stat_recv, lambda: advance(2 * unit)
    )
    rows_all[tp] = hidden_in
    copies = exchange(2, lambda to: rows_all.at[tp], lambda k: rows_all.at[tp])
    for copy in copies:
        copy.start()
    pending.extend(copies)
    advance(4 * unit)
    for k in range(1, n_tp):
        sender = (tp + n_tp - k) % n_tp
        tp_copy(2, rows_all.at[sender], rows_all.at[sender], sender, k).wait_recv()

    advance(len(first) - queue[1])
    advance(splits)

    def last_hop(array):
        for piece in range(splits):
            for direction in range(2):
                ring_copy(array, piece, n_sp - 1, direction, True).wait_recv()
                ring_copy(array, piece, n_sp - 1, direction, False).wait_send()

    last_hop(0)
    group = n_sp // n_tp
    depth = group * wg_ref.shape[0]
    hidden_width = wg_ref.shape[1]

    def wide(weight):
        total = None
        for t in range(n_tp):
            term = dot(
                rows_all[t],
                weight[t * group : (t + 1) * group].reshape(depth, hidden_width),
            )
            total = term if total is None else total + term
            advance(1)
        return total

    gate_sum = wide(gate_all)
    last_hop(1)
    up_sum = wide(up_all)
    hidden = (gate_sum / (1.0 + jnp.exp(-gate_sum)) * up_sum).astype(jnp.bfloat16)
    advance(1)

    half_rows = piece_rows * splits
    if half_rows % LANES == 0:
        hid[...] = hidden

        def down_copy(k, slot, to, columns):
            ref = part2_send.at[to, :, columns]
            return pltpu.make_async_remote_copy(
                src_ref=ref,
                dst_ref=part2_recv.at[k, :, columns],
                send_sem=down_send.at[k, slot],
                recv_sem=down_recv.at[k, slot],
                device_id={"tp": to},
                device_id_type=MESH,
            )

        def slot_columns(slot):
            return pl.ds(pl.multiple_of(slot * half_rows, LANES), half_rows)

        def make_columns(hop):
            for direction in range(2):
                block = origin(hop, direction)
                owner = block // group
                slot = (block % group) * 2 + direction
                rows = pl.ds(direction * half_rows, half_rows)
                part2_send[owner, :, slot_columns(slot)] = dot_nt(
                    hid[...], down_all[block, rows]
                ).astype(jnp.bfloat16)

                @pl.when(owner != tp)
                def send_away():
                    down_copy((owner + n_tp - tp) % n_tp, slot, owner, slot_columns(slot)).start()

        made = 0
        while queue[1] < len(queue[0]):
            array, piece, hop = queue[0][queue[1]]
            advance(1)
            if piece == splits - 1:
                made_to = hop
                while made < made_to:
                    make_columns(made)
                    made += 1
        while made < n_sp - 1:
            make_columns(made)
            made += 1
        last_hop(2)
        make_columns(n_sp - 1)
        mixer = part2_send[tp].astype(jnp.float32)
        for k in range(1, n_tp):
            for slot in range(2 * group):
                down_copy(k, slot, (tp + k) % n_tp, slot_columns(slot)).wait_recv()
            mixer = mixer + part2_recv[k].astype(jnp.float32)
    else:
        advance(len(queue[0]))
        last_hop(2)
        copies = exchange(3, lambda to: part2_send.at[to], lambda k: part2_recv.at[k])
        for k in range(1, n_tp + 1):
            to = (tp + k) % n_tp
            part2_send[to] = dot_nt(
                hidden, down_all[pl.ds(to * group, group)].reshape(depth, hidden_width)
            ).astype(jnp.bfloat16)
            if k < n_tp:
                copies[k - 1].start()
        mixer = part2_send[tp].astype(jnp.float32)
        for k in range(1, n_tp):
            copies[k - 1].wait_recv()
            mixer = mixer + part2_recv[k].astype(jnp.float32)
        pending.extend(copies)
    final = DEEP_ALPHA * rows_all[tp].astype(jnp.float32) + HALF_STEP * mixer
    out_ref[...] = normed(final, gain_out_ref, 4, stat2_send, stat2_recv, lambda: None)
    for copy in pending:
        copy.wait_send()
    if half_rows % LANES == 0:
        for k in range(1, n_tp):
            for slot in range(2 * group):
                down_copy(k, slot, (tp + k) % n_tp, slot_columns(slot)).wait_send()


def attend_loop(attend, head, at, state):
    return attend(head, at, state)


def flip(value, mask):
    result = value
    bit = 1
    while bit <= mask:
        if mask & bit:
            result = result + bit - 2 * bit * ((value // bit) % 2)
        bit *= 2
    return result


class Semaphores:
    def __init__(self, refs):
        self.refs, self.base, self.used = refs, {}, 0

    def at(self, name, count=1, index=0):
        if name not in self.base:
            self.base[name] = self.used
            self.used += count
        return self.refs.at[self.base[name] + index]


def paired_kernel(
    n_sp,
    n_tp,
    pieces,
    q_in,
    lat_ref,
    rope_in,
    wk_in,
    wv_in,
    wo_ref,
    resid_in,
    gain_mix_in,
    gain_out_in,
    wg_ref,
    wu_ref,
    wd_ref,
    out_ref,
    q_ref,
    rope_ref,
    wk_ref,
    wv_ref,
    resid_ref,
    gain_mix_ref,
    gain_out_ref,
    lat_all,
    keys,
    rotary,
    values,
    q_all,
    heads_all,
    wo_all,
    wide_all,
    down_own,
    down_all,
    rows_all,
    hid,
    summed,
    core_send,
    core_recv,
    far_send,
    far_recv,
    pair_send,
    pair_recv,
    first_send,
    first_recv,
    last_send,
    last_recv,
    total_sum,
    stat_send,
    stat_recv,
    local_sem,
    remote_sem,
):
    sp = lax.axis_index("sp")
    tp = lax.axis_index("tp")
    n_hi = n_sp // 2
    z, x = sp // 2, sp % 2
    half = z % 2
    edge = half == (z // 2) % 2
    inner = jnp.logical_not(edge)
    n_rows = q_ref.shape[0]
    head_count = wk_ref.shape[1] // NOPE
    rank = wk_ref.shape[0]
    lat_rows = lat_all.shape[2]
    n_cols = out_ref.shape[1]
    group = n_sp // n_tp
    depth = wg_ref.shape[0]
    width = wg_ref.shape[1] // 2
    piece_cols = wd_ref.shape[1] // pieces
    local_sems = Semaphores(local_sem)
    remote_sems = Semaphores(remote_sem)

    order = [(1, flip(z, 1))]
    for m in range(2, n_hi, 2):
        low, high = flip(z, m), flip(z, m + 1)
        order.append((jnp.where(edge, m, m + 1), jnp.where(edge, low, high)))
        order.append((jnp.where(edge, m + 1, m), jnp.where(edge, high, low)))
    near, rest = list(range(1, len(order), 2)), list(range(2, len(order), 2))

    def sp_of(place, side):
        return 2 * place + side

    def remote(source, target, device, sent, name, count=1, index=0):
        return pltpu.make_async_remote_copy(
            src_ref=source,
            dst_ref=target,
            send_sem=remote_sems.at(("sent", sent)),
            recv_sem=remote_sems.at(name, count, index),
            device_id=device,
            device_id_type=MESH,
        )

    other_x = 1 - x
    partner, across, corner = flip(tp, 1), flip(tp, 2), flip(tp, 3)
    to_x = {"sp": sp_of(z, other_x)}
    to_pair = {"sp": sp_of(flip(z, 1), x)}
    to_core = {"tp": partner}
    to_across = {"tp": across}

    barrier = pltpu.get_barrier_semaphore()
    peers = [{"sp": sp_of(flip(z, k), x)} for k in range(1, n_hi)] + [to_x]
    peers += [{"tp": flip(tp, j)} for j in range(1, n_tp)]
    for device in peers:
        pl.semaphore_signal(barrier, inc=1, device_id=device, device_id_type=MESH)

    def local(source, target, name):
        return pltpu.make_async_copy(source, target, local_sems.at(name))

    inputs = {
        "rope": local(rope_in, rope_ref, "rope"),
        "q": local(q_in, q_ref, "q"),
        "wk": local(wk_in, wk_ref, "wk"),
        "wv": local(wv_in, wv_ref, "wv"),
        "resid": local(resid_in, resid_ref, "resid"),
        "mix": local(gain_mix_in, gain_mix_ref, "mix"),
        "out": local(gain_out_in, gain_out_ref, "out"),
    }

    wide_rows = depth // pieces

    def wide_source(array, which, piece):
        columns = pl.ds(pl.multiple_of(which * width, LANES), width)
        return (wg_ref, wu_ref)[array].at[pl.ds(piece * wide_rows, wide_rows), columns]

    def wide_block(array, place, side, piece):
        rows = pl.ds(piece * wide_rows, wide_rows)
        return wide_all.at[sp_of(place, side), rows, pl.ds(array * width, width)]

    def down_rows(which, piece):
        rows = pl.ds(pl.multiple_of(which * width, 16), width)
        return wd_ref.at[rows, pl.ds(piece * piece_cols, piece_cols)]

    def down_block(place, side, piece):
        return down_all.at[place * pieces + piece, side]

    def weight_source(array, which, piece):
        if array == 2:
            return down_own.at[which, piece]
        return wide_source(array, which, piece)

    def weight_block(array, place, side, piece):
        if array == 2:
            return down_block(place, side, piece)
        return wide_block(array, place, side, piece)

    def sent_of(array):
        return "down" if array == 2 else "wide"

    def parts_of(array, ref):
        if array < 2:
            return [ref]
        return [ref.at[pl.ds(part * width // 2, width // 2)] for part in range(2)]

    def weight_out(array, k, piece):
        place = flip(z, k)
        sources = parts_of(array, weight_source(array, place % 2, piece))
        targets = parts_of(array, weight_block(array, z, x, piece))
        for part, (source, target) in enumerate(zip(sources, targets)):
            remote(
                source,
                target,
                {"sp": sp_of(place, x)},
                sent_of(array),
                ("wz", array, piece, part),
                n_hi - 1,
                k - 1,
            ).start()

    def weight_side(array, k, place, piece, source=None):
        block = weight_block(array, place, x, piece)
        name = ("wx", piece) if array == 2 else "wx"
        count, index = (n_hi, k) if array == 2 else (1, 0)
        source = block if source is None else source
        remote(source, block, to_x, sent_of(array), name, count, index).start()

    def weight_own(array, piece):
        weight_side(array, 0, z, piece, weight_source(array, half, piece))

    def relay(array, at, piece):
        k, place = order[at]
        name = ("wx", piece) if array == 2 else "wx"
        count, index = (n_hi, k) if array == 2 else (1, 0)
        for part, block in enumerate(parts_of(array, weight_block(array, place, x, piece))):
            remote(
                block,
                block,
                to_x,
                sent_of(array),
                ("wz", array, piece, part),
                n_hi - 1,
                k - 1,
            ).wait_recv()
            remote(block, block, to_x, sent_of(array), name, count, index).start()

    def relay_all(array, at):
        for piece in range(pieces):
            relay(array, at, piece)

    lat_own = local(lat_ref, lat_all.at[sp, :, :, pl.ds(0, rank)], "lat")
    inputs["rope"].start()
    lat_own.start()
    for name in ("q", "wk", "wv", "resid", "mix", "out"):
        inputs[name].start()
    staged = []
    for piece in range(pieces):
        for which in range(2):
            name = ("staged", which, piece)
            staged.append(local(down_rows(which, piece), down_own.at[which, piece], name))
            staged[-1].start()
        for array in range(2):
            local(
                weight_source(array, half, piece), weight_block(array, z, x, piece), "wide"
            ).start()
    down_mine = []
    for piece in range(pieces):
        down_mine.append(
            local(down_rows(half, piece), down_block(z, x, piece), ("down", piece))
        )
        down_mine[-1].start()

    def wo_columns(which):
        return wo_ref.at[:, pl.ds(pl.multiple_of(which * n_cols, LANES), n_cols)]

    wo_own = local(wo_columns(tp), wo_all.at[tp], "wo")
    wo_own.start()
    cosine, sine = rotary_tables(sp * n_rows, n_rows)
    inputs["rope"].wait()
    turned_in = jnp.concatenate(
        [rope_ref[...].astype(jnp.float32), jnp.zeros((LANES - ROPE, n_rows), jnp.float32)],
        axis=0,
    )
    key_rot = rotate(jnp.transpose(turned_in)[:, :ROPE], cosine, sine)
    key_rot.append(jnp.zeros((n_rows, LANES - ROPE), jnp.float32))
    lat_all[sp, :, :, pl.ds(rank, LANES)] = (
        jnp.concatenate(key_rot, axis=1).astype(jnp.bfloat16).reshape(n_tp, lat_rows, LANES)
    )

    def prepare_queries(head):
        base = head * (NOPE + ROPE)
        wide_q = q_ref[...].astype(jnp.float32)
        nope = wide_q[:, base : base + NOPE]
        other = jnp.zeros((n_rows, NOPE), jnp.float32)
        turned = rotate(wide_q[:, base + NOPE : base + NOPE + ROPE], cosine, sine)
        parts = [nope, other] if head % 2 == 0 else [other, nope]
        parts = parts + turned + [jnp.zeros((n_rows, LANES - ROPE), jnp.float32)]
        q_all[head] = jnp.concatenate(parts, axis=1).astype(jnp.bfloat16)

    pl.semaphore_wait(barrier, len(peers))
    lat_own.wait()
    for copy in staged:
        copy.wait()

    def lat_copy(name, k, place, side, quarter, device):
        block = lat_all.at[sp_of(place, side), quarter]
        return remote(block, block, device, "lat", ("lat", name), n_hi, k)

    def lat_core(place, side, quarter):
        block = lat_all.at[sp_of(place, side), quarter]
        remote(block, block, to_core, "lat", "latc").start()

    def lat_z_in(at):
        k, place = order[at]
        lat_copy("z", k, place, x, tp, to_x).wait_recv()
        lat_copy("x", k, place, x, tp, to_x).start()
        lat_copy("y", k, place, x, tp, to_across).start()
        lat_core(place, x, tp)

    def lat_x_in(at):
        k, place = (0, z) if at is None else order[at]
        lat_copy("x", k, place, other_x, tp, to_x).wait_recv()
        lat_copy("yd", k, place, other_x, tp, to_across).start()
        lat_core(place, other_x, tp)

    def lat_y_in(at):
        k, place = order[at]
        lat_copy("y", k, place, x, across, to_across).wait_recv()
        lat_core(place, x, across)

    def lat_yd_in(at):
        k, place = (0, z) if at is None else order[at]
        lat_copy("yd", k, place, other_x, across, to_across).wait_recv()
        lat_core(place, other_x, across)

    for k in range(1, n_hi):
        block = lat_all.at[sp, tp]
        remote(
            block, block, {"sp": sp_of(flip(z, k), x)}, "lat", ("lat", "z"), n_hi, k
        ).start()
    lat_copy("x", 0, z, x, tp, to_x).start()
    weight_own(0, 0)

    far = list(range(2, n_hi))

    def send_near(arrays):
        for array in arrays:
            for piece in range(pieces):
                weight_out(array, 1, piece)

    def send_far(array, which):
        for piece in which:
            for k in far:
                weight_out(array, k, piece)

    every = range(pieces)
    early, late = range(pieces // 2), range(pieces // 2, pieces)

    @pl.when(edge)
    def outer_first():
        send_near((0, 1))
        send_far(0, every)
        send_far(1, early)

    @pl.when(inner)
    def inner_first():
        send_near((0, 1, 2))
        send_far(0, every)
        send_far(1, every)

    inputs["q"].wait()
    prepare_queries(0)
    lat_x_in(None)
    lat_z_in(0)

    prepare_queries(1)
    for piece in range(1, pieces):
        weight_own(0, piece)
    for at in near:
        lat_z_in(at)
    lat_yd_in(None)
    lat_x_in(0)
    lat_y_in(0)
    for at in rest:
        lat_z_in(at)
    for piece in range(pieces):
        weight_own(1, piece)
    for piece in range(pieces):
        weight_own(2, piece)
    for head in range(2, head_count):
        prepare_queries(head)
    for at in near:
        lat_x_in(at)
        lat_y_in(at)
    lat_yd_in(0)
    for at in rest:
        lat_x_in(at)
        lat_y_in(at)
    for j in (2, 3, 1):
        to = flip(tp, j)
        remote(wo_columns(to), wo_all.at[tp], {"tp": to}, "wo", "wo").start()
    for at in near + rest:
        lat_yd_in(at)
    relay_all(0, 0)
    whole = lat_all.at[pl.ds(0, n_sp - 1), pl.ds(0, 2)]
    remote(whole, whole, to_core, "lat", "latc").wait_recv()

    half_blocks = n_sp // 2

    def project(step):
        rows = half_blocks * n_rows
        blocks = pl.ds(step * half_blocks, half_blocks)
        lat = lat_all[blocks, :, :, pl.ds(0, rank)].reshape(rows, rank)
        rotary[pl.ds(step * rows, rows)] = lat_all[blocks, :, :, pl.ds(rank, LANES)].reshape(
            rows, LANES
        )
        keys[pl.ds(step * rows, rows)] = dot(lat, wk_ref[...]).astype(jnp.bfloat16)
        values[pl.ds(step * rows, rows)] = dot(lat, wv_ref[...]).astype(jnp.bfloat16)

    inputs["wk"].wait()
    inputs["wv"].wait()
    for step in range(n_sp // half_blocks):
        project(step)

    score_scale = (NOPE + ROPE) ** (-0.5)
    lane = lax.broadcasted_iota(jnp.int32, (n_rows, LANES), 1)

    for head in range(head_count):
        pair = slice(head // 2 * LANES, (head // 2 + 1) * LANES)
        whole_keys = jnp.concatenate([keys[:, pair], rotary[...]], axis=1)
        scores = dot_nt(q_all[head], whole_keys) * score_scale
        top = jnp.max(scores, axis=1, keepdims=True)
        probs = jnp.exp(scores - top)
        sums = jnp.sum(probs, axis=1, keepdims=True)
        result = dot(probs.astype(jnp.bfloat16), values[:, pair]) / sums
        if head % 2 == 0:
            held = result
        else:
            heads_all[tp, :, pair] = jnp.where(lane < VDIM, held, result).astype(jnp.bfloat16)
            block = heads_all.at[tp, :, pl.ds(head // 2 * LANES, LANES)]
            for j in (2, 3, 1):
                remote(block, block, {"tp": flip(tp, j)}, "heads", "heads").start()
        if head == head_count // 2 - 1:
            relay_all(1, 0)
    for at in near:
        relay_all(0, at)
    for name in ("resid", "mix", "out"):
        inputs[name].wait()
    mixed = DEEP_ALPHA * resid_ref[...].astype(jnp.float32)
    wo_own.wait()
    mixed = mixed + dot(heads_all[tp], wo_all[tp])
    others = pl.ds(0, n_tp - 1)
    remote(wo_all.at[others], wo_all.at[others], to_core, "wo", "wo").wait_recv()
    remote(heads_all.at[others], heads_all.at[others], to_core, "heads", "heads").wait_recv()
    for j in (1, 2, 3):
        sender = flip(tp, j)
        mixed = mixed + dot(heads_all[sender], wo_all[sender])

    width_total = n_cols * n_tp

    def normed(rows_in, gain_ref, stage, between):
        sums = jnp.sum(rows_in, axis=1, keepdims=True)
        squares = jnp.sum(rows_in * rows_in, axis=1, keepdims=True)
        mine = jnp.transpose(jnp.where(lane < 4, sums, squares))[:8]
        stat_send[stage] = mine
        for j in (2, 3, 1):
            remote(
                stat_send.at[stage],
                stat_recv.at[stage, j - 1],
                {"tp": flip(tp, j)},
                ("stat", stage),
                ("stat", stage),
            ).start()
        between()
        arrived = stat_recv.at[stage]
        remote(arrived, arrived, to_core, ("stat", stage), ("stat", stage)).wait_recv()
        for j in (1, 2, 3):
            mine = mine + stat_recv[stage, j - 1]
        whole = jnp.transpose(mine) / width_total
        row_mean = whole[:, :1]
        variance = whole[:, 4:5] - row_mean * row_mean
        return (
            (rows_in - row_mean) * lax.rsqrt(variance + NORM_EPSILON) * gain_ref[...]
        ).astype(jnp.bfloat16)

    def more_wide():
        for at in rest:
            relay_all(0, at)

    hidden_in = normed(mixed, gain_mix_ref, 0, more_wide)
    mine = pl.ds(pl.multiple_of(half * n_rows, 16), n_rows)
    theirs = pl.ds(pl.multiple_of((1 - half) * n_rows, 16), n_rows)
    rows_all[tp, mine] = hidden_in

    def rows_copy(name, owner, rows, device):
        block = rows_all.at[owner, rows]
        return remote(block, block, device, "rows", ("rows", name))

    def rows_core(owner, rows):
        block = rows_all.at[owner, rows]
        remote(block, block, to_core, "rowsc", "rowsc").start()

    rows_copy("y", tp, mine, to_across).start()
    rows_copy("z", tp, mine, to_pair).start()
    rows_core(tp, mine)

    @pl.when(edge)
    def outer_last():
        send_far(1, late)
        send_near((2,))
        send_far(2, every)

    @pl.when(inner)
    def inner_last():
        send_far(2, every)

    for at in near:
        relay_all(1, at)
    for at in rest:
        for piece in early:
            relay(1, at, piece)
    rows_copy("z", tp, theirs, to_pair).wait_recv()
    rows_copy("yz", tp, theirs, to_across).start()
    rows_core(tp, theirs)
    rows_copy("y", across, mine, to_across).wait_recv()
    rows_core(across, mine)
    for at in rest:
        for piece in late:
            relay(1, at, piece)

    @pl.when(edge)
    def outer_first_down():
        relay_all(2, 0)
        for at in near:
            for piece in early:
                relay(2, at, piece)

    rows_copy("yz", across, theirs, to_across).wait_recv()
    rows_core(across, theirs)

    @pl.when(inner)
    def inner_first_down():
        relay_all(2, 0)

    @pl.when(inner)
    def inner_near_down():
        for at in near:
            for piece in early:
                relay(2, at, piece)

    both = rows_all.at[pl.ds(0, 2)]
    remote(both, both, to_core, "rowsc", "rowsc").wait_recv()
    local(wg_ref, wide_all.at[0], "wide").wait()
    arrived = wide_all.at[pl.ds(0, n_hi)]
    remote(arrived, arrived, to_x, "wide", "wx").wait_recv()

    total = None
    for t in range(n_tp):
        term = dot(
            rows_all[t], wide_all[t * group : (t + 1) * group].reshape(group * depth, 2 * width)
        )
        total = term if total is None else total + term
    gate_sum, up_sum = total[:, :width], total[:, width:]
    hid[...] = (gate_sum / (1.0 + jnp.exp(-gate_sum)) * up_sum).astype(jnp.bfloat16)
    for copy in down_mine:
        copy.wait()

    def facts(at, piece):
        k, place = (0, z) if at is None else order[at]
        unit = place * pieces + piece
        return k, place, unit, tp % 2 == place % 2, tp // 2 == place // 2

    def core_copy(place, unit, piece):
        return remote(
            core_send.at[unit],
            core_recv.at[unit],
            to_core,
            "core",
            "core",
            n_tp // 2 * pieces,
            place // 2 * pieces + piece,
        )

    def far_copy(piece):
        return remote(
            far_send.at[piece], far_recv.at[piece], to_across, "far", "far", pieces, piece
        )

    def pair_copy(piece):
        return remote(
            pair_send.at[piece], pair_recv.at[piece], to_pair, "pair", "pair", pieces, piece
        )

    def pair_first_copy(piece):
        source, target = first_send.at[piece], first_recv.at[piece]
        return remote(source, target, to_pair, "first", "first", pieces + 1, piece)

    def far_last_copy(piece):
        source, target = last_send.at[piece], last_recv.at[piece]
        return remote(source, target, to_across, "last", "last", pieces + 1, piece)

    def make_block(at, piece):
        k, place, unit, same_core, same_chip = facts(at, piece)
        block = down_block(place, other_x, piece)
        remote(block, block, to_x, "down", ("wx", piece), n_hi, k).wait_recv()
        columns = jnp.concatenate([down_all[unit, 0], down_all[unit, 1]], axis=1)
        product = dot(hid[...], columns)

        @pl.when(same_core)
        def keep():
            summed[unit] = product

        @pl.when(jnp.logical_not(same_core))
        def give():
            core_send[unit] = product.astype(jnp.bfloat16)
            core_copy(place, unit, piece).start()

    def add_core(at, piece):
        k, place, unit, same_core, same_chip = facts(at, piece)

        @pl.when(same_core)
        def add():
            core_copy(place, unit, piece).wait_recv()
            both = summed[unit] + core_recv[unit].astype(jnp.float32)

            @pl.when(same_chip)
            def keep():
                summed[unit] = both

            @pl.when(jnp.logical_not(same_chip))
            def give():
                far_send[piece] = both.astype(jnp.bfloat16)
                far_copy(piece).start()

    def add_far(at, piece):
        k, place, unit, same_core, same_chip = facts(at, piece)

        @pl.when(place == tp)
        def add():
            far_copy(piece).wait_recv()
            summed[unit, mine] = summed[unit, mine] + far_recv[piece, mine].astype(jnp.float32)
            pair_send[piece] = (
                summed[unit, theirs] + far_recv[piece, theirs].astype(jnp.float32)
            ).astype(jnp.bfloat16)
            pair_copy(piece).start()

    def slot_of(at, piece):
        return pieces if at is None or at == 0 else piece

    def pair_first(at, piece):
        k, place, unit, same_core, same_chip = facts(at, piece)
        slot = slot_of(at, piece)

        @pl.when(same_core)
        def add():
            core_copy(place, unit, piece).wait_recv()
            first_send[slot] = (
                summed[unit, theirs] + core_recv[unit, theirs].astype(jnp.float32)
            ).astype(jnp.bfloat16)
            pair_first_copy(slot).start()

    def pair_added(at, piece):
        k, place, unit, same_core, same_chip = facts(at, piece)
        slot = slot_of(at, piece)

        @pl.when(same_core)
        def add():
            pair_first_copy(slot).wait_recv()
            both = summed[unit, mine] + core_recv[unit, mine].astype(jnp.float32)
            both = both + first_recv[slot].astype(jnp.float32)

            @pl.when(same_chip)
            def keep():
                total_sum[slot] = both

            @pl.when(jnp.logical_not(same_chip))
            def give():
                last_send[slot] = both.astype(jnp.bfloat16)
                far_last_copy(slot).start()

    def finish_far(at, piece):
        k, place, unit, same_core, same_chip = facts(at, piece)
        slot = slot_of(at, piece)

        @pl.when(place == tp)
        def add():
            far_last_copy(slot).wait_recv()
            total_sum[piece] = total_sum[slot] + last_recv[slot].astype(jnp.float32)

    def finish_pair(at, piece):
        k, place, unit, same_core, same_chip = facts(at, piece)

        @pl.when(place == tp)
        def add():
            pair_copy(piece).wait_recv()
            total_sum[piece] = summed[unit, mine] + pair_recv[piece].astype(jnp.float32)

    def each(apply, ats, which):
        for piece in which:
            for at in ats:
                apply(at, piece)

    close = [None, 0]
    each(make_block, close, every)
    each(functools.partial(relay, 2), rest, early)
    each(add_core, close, early)
    each(pair_first, close, late)
    each(make_block, near, early)
    each(functools.partial(relay, 2), rest, late)
    each(make_block, rest, early)
    each(functools.partial(relay, 2), near, late)
    each(pair_first, near + rest, early)
    each(make_block, rest, late)
    each(pair_added, close, late)
    each(make_block, near, late)
    each(pair_first, rest + near, late)
    each(pair_added, near + rest, early)
    each(add_far, close, early)
    each(pair_added, rest + near, late)
    each(finish_far, close, late)
    each(finish_pair, close, early)
    each(finish_far, near + rest, every)
    final = [total_sum[piece] for piece in range(pieces)]
    sides = []
    for side in range(2):
        for piece in range(pieces):
            sides.append(final[piece][:, side * piece_cols : (side + 1) * piece_cols])
    mixer = jnp.concatenate(sides, axis=1)
    last_in = DEEP_ALPHA * rows_all[tp, mine].astype(jnp.float32) + HALF_STEP * mixer
    out_ref[...] = normed(last_in, gain_out_ref, 1, lambda: None)

    def all_sent(sent, name, whole):
        remote(whole, whole, to_core, sent, name).wait_send()

    all_sent("lat", "latc", lat_all.at[pl.ds(0, n_sp - 1)])
    all_sent("wide", "wx", wide_all.at[pl.ds(0, n_sp - 1)])
    all_sent("down", "wx", down_all.at[pl.ds(0, (n_sp - 1) * pieces // 2)])
    all_sent("wo", "wo", wo_all.at[others])
    all_sent("heads", "heads", heads_all.at[others])
    all_sent("rows", ("rows", "z"), rows_all.at[others, pl.ds(0, n_rows)])
    all_sent("rowsc", "rowsc", both)
    for stage in range(2):
        all_sent(("stat", stage), ("stat", stage), stat_recv.at[stage])
    all_sent("core", "core", core_send.at[pl.ds(0, n_hi * pieces // 2)])
    all_sent("first", "first", first_send)
    home = tp // 2 == z // 2
    early_rows = pl.ds(0, pieces // 2)

    @pl.when(home)
    def sent_home():
        all_sent("pair", "pair", pair_send.at[early_rows])
        all_sent("last", "last", last_send.at[pl.ds(0, pieces)])

    @pl.when(jnp.logical_not(home))
    def sent_away():
        all_sent("far", "far", far_send.at[early_rows])
        all_sent("last", "last", last_send.at[early_rows])


def paired_call(n_sp, n_tp, operands):
    queries, latents, rope_key, w_key, w_value, w_out, resid, gain_mix = operands[:8]
    w_gate, w_up, w_down, gain_out = operands[8:]
    rows = queries.shape[0]
    head_count = w_key.shape[1] // NOPE
    rank = latents.shape[1]
    cols = resid.shape[1]
    depth, hidden_width = w_gate.shape
    width = hidden_width // 2
    pieces = 2
    n_hi = n_sp // 2
    unit_cols = 2 * w_down.shape[1] // pieces
    total_rows = n_sp * rows
    bf16 = jnp.bfloat16
    f32 = jnp.float32
    vmem = pl.BlockSpec(memory_space=pltpu.VMEM)
    anywhere = pl.BlockSpec(memory_space=pl.ANY)
    dma = pltpu.SemaphoreType.DMA
    signals = 4 * n_hi + 4 * (n_hi - 1) * pieces + n_hi * pieces
    signals += (n_tp // 2 + 4) * pieces + 26
    return pl.pallas_call(
        functools.partial(paired_kernel, n_sp, n_tp, pieces),
        out_shape=pltpu.VMEM((rows, cols), bf16),
        in_specs=[anywhere] * 12,
        out_specs=vmem,
        scratch_shapes=[
            pltpu.VMEM(queries.shape, bf16),
            pltpu.VMEM((rope_key.shape[1], rows), bf16),
            pltpu.VMEM(w_key.shape, bf16),
            pltpu.VMEM(w_value.shape, bf16),
            pltpu.VMEM(resid.shape, bf16),
            pltpu.VMEM((1, cols), f32),
            pltpu.VMEM((1, cols), f32),
            pltpu.VMEM((n_sp, n_tp, rows // n_tp, rank + LANES), bf16),
            pltpu.VMEM((total_rows, head_count * NOPE), bf16),
            pltpu.VMEM((total_rows, LANES), bf16),
            pltpu.VMEM((total_rows, head_count * VDIM), bf16),
            pltpu.VMEM((head_count, rows, 2 * LANES), bf16),
            pltpu.VMEM((n_tp, rows, head_count * VDIM), bf16),
            pltpu.VMEM((n_tp, head_count * VDIM, cols), bf16),
            pltpu.VMEM((n_sp, depth, 2 * width), bf16),
            pltpu.VMEM((2, pieces, width, unit_cols // 2), bf16),
            pltpu.VMEM((n_hi * pieces, 2, width, unit_cols // 2), bf16),
            pltpu.VMEM((n_tp, 2 * rows, cols), bf16),
            pltpu.VMEM((2 * rows, width), bf16),
            pltpu.VMEM((n_hi * pieces, 2 * rows, unit_cols), f32),
            pltpu.VMEM((n_hi * pieces, 2 * rows, unit_cols), bf16),
            pltpu.VMEM((n_hi * pieces, 2 * rows, unit_cols), bf16),
            pltpu.VMEM((pieces, 2 * rows, unit_cols), bf16),
            pltpu.VMEM((pieces, 2 * rows, unit_cols), bf16),
            pltpu.VMEM((pieces, rows, unit_cols), bf16),
            pltpu.VMEM((pieces, rows, unit_cols), bf16),
            pltpu.VMEM((pieces + 1, rows, unit_cols), bf16),
            pltpu.VMEM((pieces + 1, rows, unit_cols), bf16),
            pltpu.VMEM((pieces + 1, rows, unit_cols), bf16),
            pltpu.VMEM((pieces + 1, rows, unit_cols), bf16),
            pltpu.VMEM((pieces + 1, rows, unit_cols), f32),
            pltpu.VMEM((2, 8, rows), f32),
            pltpu.VMEM((2, n_tp - 1, 8, rows), f32),
            dma((10 + 3 * pieces,)),
            dma((signals,)),
        ],
        compiler_params=pltpu.CompilerParams(
            collective_id=1, has_side_effects=True, vmem_limit_bytes=66000000
        ),
    )(
        queries,
        latents.reshape(n_tp, rows // n_tp, rank),
        rope_key.T,
        w_key,
        w_value,
        w_out,
        resid,
        gain_mix.reshape(1, -1),
        gain_out.reshape(1, -1),
        w_gate,
        w_up,
        w_down,
    )


def fits_pairs(n_sp, n_tp, operands):
    queries, w_key, w_gate, w_down = operands[0], operands[3], operands[8], operands[10]
    return (
        n_tp == 4
        and n_sp == 2 * n_tp
        and queries.shape[0] % 64 == 0
        and n_sp * queries.shape[0] <= 1536
        and (w_key.shape[1] // NOPE) % 2 == 0
        and w_gate.shape[1] % (2 * LANES) == 0
        and w_gate.shape[0] % 32 == 0
        and w_down.shape[1] % (2 * LANES) == 0
    )


def local(
    queries,
    latents,
    rope_key,
    w_key,
    w_value,
    w_out,
    resid,
    gain_mix,
    w_gate,
    w_up,
    w_down,
    gain_out,
):
    n_sp = lax.axis_size("sp")
    n_tp = lax.axis_size("tp")
    operands = (queries, latents, rope_key, w_key, w_value, w_out, resid, gain_mix)
    operands += (w_gate, w_up, w_down, gain_out)
    if fits_pairs(n_sp, n_tp, operands):
        return paired_call(n_sp, n_tp, operands)
    rows = queries.shape[0]
    head_count = w_key.shape[1] // NOPE
    rank = latents.shape[1]
    cols = resid.shape[1]
    hidden_width = w_gate.shape[1]
    weight_rows = w_gate.shape[0]
    lat_wide = rank + LANES
    splits = 2 if weight_rows % 64 == 0 else 1
    bf16 = jnp.bfloat16
    total_rows = n_sp * rows
    vmem = pl.BlockSpec(memory_space=pltpu.VMEM)
    anywhere = pl.BlockSpec(memory_space=pl.ANY)
    dma = pltpu.SemaphoreType.DMA
    return pl.pallas_call(
        functools.partial(layer_kernel, n_sp, n_tp, splits),
        out_shape=jax.ShapeDtypeStruct((rows, cols), bf16),
        in_specs=[vmem, anywhere] + [vmem] * 7 + [anywhere] * 2 + [vmem],
        out_specs=vmem,
        scratch_shapes=[
            pltpu.VMEM((n_sp, 4, rows // 4, lat_wide), bf16),
            pltpu.VMEM((total_rows, head_count * NOPE), bf16),
            pltpu.VMEM((total_rows, LANES), bf16),
            pltpu.VMEM((total_rows, head_count * VDIM), bf16),
            pltpu.VMEM((n_sp, weight_rows, hidden_width), bf16),
            pltpu.VMEM((n_sp, weight_rows, hidden_width), bf16),
            pltpu.VMEM((n_sp, weight_rows, hidden_width), bf16),
            pltpu.VMEM((head_count, rows, 2 * LANES), bf16),
            pltpu.VMEM((rows, head_count * VDIM), bf16),
            pltpu.VMEM((n_tp, rows, cols), bf16),
            pltpu.VMEM((n_tp, rows, cols), bf16),
            pltpu.VMEM((8, rows), jnp.float32),
            pltpu.VMEM((n_tp, 8, rows), jnp.float32),
            pltpu.VMEM((n_tp, rows, cols), bf16),
            pltpu.VMEM((n_tp, rows, cols), bf16),
            pltpu.VMEM((n_tp, rows, cols), bf16),
            pltpu.VMEM((8, rows), jnp.float32),
            pltpu.VMEM((n_tp, 8, rows), jnp.float32),
            pltpu.VMEM((rows, hidden_width), bf16),
            dma((4,)),
            dma((2,)),
            dma((2, n_sp - 1)),
            dma((2,)),
            dma((2, n_sp - 1)),
            dma((3, splits, 2)),
            dma((3, splits, 2, n_sp - 1)),
            dma((5, n_tp)),
            dma((5, n_tp)),
            dma((n_tp, 2 * (n_sp // n_tp))),
            dma((n_tp, 2 * (n_sp // n_tp))),
        ],
        compiler_params=pltpu.CompilerParams(
            collective_id=0, has_side_effects=True, vmem_limit_bytes=66000000
        ),
    )(
        queries,
        latents.reshape(4, rows // 4, rank),
        rope_key,
        w_key,
        w_value,
        w_out,
        resid,
        gain_mix.reshape(1, -1),
        gain_out.reshape(1, -1),
        w_gate,
        w_up,
        w_down,
    )


def solution(mesh):
    placed = (
        P("sp", "tp"),
        P("sp", None),
        P("sp", None),
        P(None, "tp"),
        P(None, "tp"),
        P("tp", None),
        P("sp", "tp"),
        P("tp"),
        P("sp", "tp"),
        P("sp", "tp"),
        P("tp", "sp"),
        P("tp"),
    )
    return jax.shard_map(
        local, mesh=mesh, in_specs=placed, out_specs=P("sp", "tp"), check_vma=False
    )
```
